32 devices in a mesh: fs: 8 (over z, x), tp: 4 (over y, core).
Axes of the slice: x: 2, y: 2, z: 4, core: 2. Of those that a mesh axis runs over, the one named last changes fastest.
Arguments:
- later_rows: bfloat16 [4096, 2048], P(('fs', 'tp')), may hold values from -6 to 6
- earlier_rows: bfloat16 [4096, 2048], P(('fs', 'tp')), may hold values from -6 to 6
- cotangent: bfloat16 [4096, 2048], P(('fs', 'tp')), may hold values from -6 to 6
- up_weight: bfloat16 [2048, 4096], P('fs', 'tp'), may hold values from -0.125 to 0.125
- down_weight: bfloat16 [2048, 4096], P('fs', 'tp'), may hold values from -0.09375 to 0.09375
- up_total: float32 [2048, 4096], P('fs', 'tp'), may hold values from -6 to 6
- down_total: float32 [2048, 4096], P('fs', 'tp'), may hold values from -6 to 6
Outputs:
- later_out: bfloat16 [4096, 2048], P(('fs', 'tp'))
- earlier_grad: bfloat16 [4096, 2048], P(('fs', 'tp'))
- up_updated: float32 [2048, 4096], P('fs', 'tp')
- down_updated: float32 [2048, 4096], P('fs', 'tp')
The draws below stay inside these ranges and needn't reach their ends.
All inputs are finite; a program needn't handle non-finite values.
Results may differ from the reference program's by a relative error of at most 0.015.
Values may be sent and summed in bfloat16 or wider, within the bound.
A program may use at most 128 MiB of HBM per device.

```python
import math
import jax
import jax.numpy as jnp
from jax import lax

D = 2048
FF = 4096
TOKENS = 4096
FF_TP = 1024
N_TP = 4


def spiked(drawn, rng, source, target, shards_of, factor):
    def block_of(position):
        return (jnp.arange(drawn.shape[position]) // (drawn.shape[position] // shards_of)).reshape((-1,) + (1,) * (drawn.ndim - 1 - position))

    one_side = jax.random.permutation(rng, shards_of)[block_of(target)]
    far = (block_of(target) + shards_of // 2) % shards_of
    return jnp.where((block_of(source) == one_side) | (block_of(source) == far), factor * drawn, drawn)


def steps_of(rng, dims, split, low, largest):
    def one(axis_at, parts):
        steps = jax.random.uniform(jax.random.fold_in(jax.random.fold_in(rng, 6), axis_at), (parts,), jnp.float32, low / len(split), largest / len(split))
        return jnp.repeat(jnp.exp(steps), dims[axis_at] // parts).reshape((-1,) + (1,) * (len(dims) - axis_at - 1))

    level = one(*split[0])
    for cut in split[1:]:
        level = level * one(*cut)
    return level


def scatter_about(key, extent, width, reach, shards=(), kind=jnp.bfloat16):
    loudness = steps_of(key, extent, shards, -0.22, 0.18) if shards else 1.0
    array = jax.random.normal(key, extent, jnp.float32) * width * loudness
    return jnp.minimum(jnp.maximum(array, -reach), reach).astype(kind)


def noise_with(stream_key, dims, width, reach, shards, heavy, kind=jnp.bfloat16):
    entries = width * jax.random.normal(stream_key, dims, jnp.float32)
    if shards:
        entries = entries * steps_of(stream_key, dims, shards, -0.22, 0.18)
    return jnp.clip(spiked(entries, jax.random.fold_in(stream_key, 3), *heavy), -reach, reach).astype(kind)


def setup_inputs(seed: int = 0) -> dict:
    keys = jax.random.split(jax.random.key(seed), 8)
    return {
        "later_rows": scatter_about(keys[0], (TOKENS, D), 1.0, 6.0, ((0, 32),)),
        "earlier_rows": scatter_about(keys[1], (TOKENS, D), 1.0, 6.0, ((0, 32),)),
        "cotangent": noise_with(keys[2], (TOKENS, D), 1.0, 6.0, ((0, 32),), (0, 1, 32, 2.75)),
        "up_weight": scatter_about(keys[3], (D, FF), D ** -0.5, 0.125, ((0, 8), (1, 4))),
        "down_weight": scatter_about(keys[4], (D, FF), FF ** -0.5, 0.09375, ((0, 8), (1, 4))),
        "up_total": scatter_about(keys[5], (D, FF), 1.0, 6.0, ((0, 8), (1, 4)), jnp.float32),
        "down_total": scatter_about(keys[6], (D, FF), 1.0, 6.0, ((0, 8), (1, 4)), jnp.float32),
    }


def blocked_sum(left, right):

    def one_block(carry, index):
        start = (index * FF_TP).astype(jnp.int32)
        left_block = lax.dynamic_slice_in_dim(left, start, FF_TP, 1)
        right_block = lax.dynamic_slice_in_dim(right, start, FF_TP, 1)
        partial_value = lax.dot_general(left_block, right_block, (((1,), (1,)), ((), ())), preferred_element_type=jnp.float32)
        rounded = lax.optimization_barrier(partial_value.astype(jnp.bfloat16))
        return (carry + rounded.astype(jnp.float32), None)
    init = jnp.zeros((left.shape[0], right.shape[0]), jnp.float32)
    total, _ = lax.scan(one_block, init, jnp.arange(N_TP, dtype=jnp.int32))
    return total

def reference(later_rows, earlier_rows, cotangent, up_weight, down_weight, up_total, down_total):
    later_pre = jnp.dot(later_rows, up_weight, preferred_element_type=jnp.float32)
    later_relu = jnp.maximum(later_pre, 0.0)
    later_hidden = (later_relu * later_relu).astype(jnp.bfloat16)
    later_out = blocked_sum(later_hidden, down_weight).astype(jnp.bfloat16)
    earlier_pre = jnp.dot(earlier_rows, up_weight, preferred_element_type=jnp.float32)
    earlier_relu = jnp.maximum(earlier_pre, 0.0)
    earlier_hidden = (earlier_relu * earlier_relu).astype(jnp.bfloat16)
    hidden_grad = jnp.dot(cotangent, down_weight, preferred_element_type=jnp.float32)
    pre_grad = (2.0 * earlier_relu * hidden_grad).astype(jnp.bfloat16)
    earlier_grad = blocked_sum(pre_grad, up_weight).astype(jnp.bfloat16)
    factor = 1.0 / math.sqrt(TOKENS)
    up_term = jnp.dot(earlier_rows.T, pre_grad, preferred_element_type=jnp.float32)
    down_term = jnp.dot(cotangent.T, earlier_hidden, preferred_element_type=jnp.float32)
    up_updated = up_total + up_term * factor
    down_updated = down_total + down_term * factor
    return (later_out, earlier_grad, up_updated, down_updated)
```

```python
import functools
import math

import jax
import jax.numpy as jnp
from jax import lax
from jax.experimental import pallas as pl
from jax.experimental.pallas import tpu as pltpu
from jax.sharding import PartitionSpec as P

MESH = pl.DeviceIdType.MESH
BF16 = jnp.bfloat16
F32 = jnp.float32


def columns_of(n):
    best = 1
    for x in range(1, n + 1):
        if n % x == 0 and 2 * x * x <= n and (n // x) % 2 == 0:
            best = x
    return best


def ring_to_fs(p, n, x_size):
    if x_size == 1:
        return p
    z_size, wide = n // x_size, x_size - 1
    body = z_size * wide
    z, r = p // wide, p % wide
    x = 1 + jnp.where(z % 2 == 0, r, wide - 1 - r)
    back = z_size - 1 - (p - body)
    return jnp.where(p < body, z * x_size + x, back * x_size)


def fs_to_ring(f, n, x_size):
    if x_size == 1:
        return f
    z_size, wide = n // x_size, x_size - 1
    z, x = f // x_size, f % x_size
    r = jnp.where(z % 2 == 0, x - 1, x_size - 1 - x)
    return jnp.where(x == 0, z_size * wide + z_size - 1 - z, z * wide + r)


def kernel(n, m, parts,
           later_ref, earlier_ref, cot_ref, up_ref, down_ref,
           later_out, earlier_out, up_out, down_out,
           tok, wts, acc, hid, grads, rbuf, part, dbuf, ybuf,
           ty_s, ty_r, td_s, td_r, w_s, w_r, g_s, g_r, od_s, od_r, oy_s, oy_r):
    rows_dev, depth = later_ref.shape
    blk, width = up_ref.shape
    rows = rows_dev * m
    half, y_size = n // 2, m // 2
    aligned = blk % 128 == 0
    wide_q = width // parts
    fs, tp = lax.axis_index("fs"), lax.axis_index("tp")
    x_size = columns_of(n)
    pos = fs_to_ring(fs, n, x_size)
    y, c = tp // 2, tp % 2

    def at_ring(p):
        return ring_to_fs((p + 2 * n) % n, n, x_size)

    right = {"fs": at_ring(pos + 1), "tp": tp}
    left = {"fs": at_ring(pos - 1), "tp": tp}
    mate = {"fs": fs, "tp": y * 2 + 1 - c}
    y_next = {"fs": fs, "tp": ((y + 1) % y_size) * 2 + c}
    y_prev = {"fs": fs, "tp": ((y + y_size - 1) % y_size) * 2 + c}

    barrier = pltpu.get_barrier_semaphore()
    for other in (right, left, mate, y_next, y_prev):
        pl.semaphore_signal(barrier, inc=1, device_id=other, device_id_type=MESH)
    pl.semaphore_wait(barrier, 5)

    def remote(src, dst, send, recv, to):
        return pltpu.make_async_remote_copy(
            src_ref=src, dst_ref=dst, send_sem=send, recv_sem=recv, device_id=to, device_id_type=MESH)

    def trows(a, t):
        return tok.at[a, pl.ds(pl.multiple_of(t * rows_dev, rows_dev), rows_dev), :]

    own_w, own_t = (up_ref, down_ref), (earlier_ref, cot_ref, later_ref)

    arr_of, sign_of = (0, 1, 1, 0), (1, -1, 1, -1)

    def cut(q):
        return pl.ds(q * wide_q, wide_q)

    def w_copy(k, s, q, first=False):
        f = at_ring(pos - sign_of[k] * s)
        there = wts.at[arr_of[k], pl.ds(pl.multiple_of(f * blk, blk), blk), cut(q)]
        src = own_w[arr_of[k]].at[:, cut(q)] if first else there
        return remote(src, there, w_s.at[k, s, q], w_r.at[k, s, q], right if sign_of[k] > 0 else left)

    def ty_copy(a, s, first=False):
        t = ((y + y_size - s) % y_size) * 2 + c
        return remote(own_t[a] if first else trows(a, t), trows(a, t), ty_s.at[a, s], ty_r.at[a, s], y_next)

    def td_copy(a, s, first=False):
        t = ((y + y_size - s) % y_size) * 2 + c
        return remote(own_t[a] if first else trows(a, t), trows(a, t), td_s.at[a, s], td_r.at[a, s], mate)

    every = tuple((k, q) for pair in ((0, 1), (2, 3)) for q in range(parts) for k in pair)
    longs = tuple((k, q) for k, q in every if k < 2)
    for k, q in every:
        w_copy(k, 0, q, True).start()
    for a in range(3):
        if y_size > 1:
            ty_copy(a, 0, True).start()
    for a in range(3):
        td_copy(a, 0, True).start()

    def put(dst, dst_row, src, count):
        step = math.gcd(count, 64)

        @pl.loop(0, count // step)
        def _(i):
            o = pl.multiple_of(i * step, step)
            dst[pl.ds(pl.multiple_of(dst_row + o, step), step), :] = src[pl.ds(o, step), :]

    for a in range(2):
        put(wts.at[a], fs * blk, own_w[a], blk)
    for a in range(3):
        put(tok.at[a], tp * rows_dev, own_t[a], rows_dev)

    tile = math.gcd(wide_q, 256)

    def multiply(a, w, rows_w, clear, q=None):
        first, count = (0, width) if q is None else (q * wide_q, wide_q)

        @pl.loop(0, count // tile)
        def _(j):
            o = pl.ds(pl.multiple_of(first + j * tile, tile), tile)
            got = jnp.dot(tok[a, :, rows_w], wts[w, rows_w, o], preferred_element_type=F32)
            if clear:
                acc[a, :, o] = got
            else:
                acc[a, :, o] += got

    def use(w, f, clear=False, q=None):
        if not aligned:
            return
        o = pl.ds(pl.multiple_of(f * blk, blk), blk)
        for a in ((0, 2) if w == 0 else (1,)):
            multiply(a, w, o, clear, q)

    def forward(s, present, go):
        for k, q in present:
            w_copy(k, s - 1, q).wait_recv()
            if (k, q) in go:
                w_copy(k, s, q).start()

    def use_step(s):
        for k in range(4):
            use(arr_of[k], at_ring(pos - sign_of[k] * s))

    forward(1, every, every if half > 2 else longs)
    for s in range(1, y_size):
        for a in range(3):
            ty_copy(a, s - 1).wait_recv()
            if s < y_size - 1:
                ty_copy(a, s).start()
            td_copy(a, s).start()
    for s in range(y_size):
        for a in range(3):
            td_copy(a, s).wait_recv()
    for w in range(2):
        use(w, fs, True)
    if half > 3:
        @pl.loop(2, half - 1)
        def _(s):
            forward(s, every, every)
            use_step(s - 1)
    if half > 2:
        forward(half - 1, every, longs)
        use_step(half - 2)
    use_step(half - 1)

    step_r = math.gcd(rows, 32)

    def activate(q):
        @pl.loop(0, rows // step_r)
        def _(i):
            o = pl.ds(pl.multiple_of(i * step_r, step_r), step_r)
            relu = jnp.maximum(acc[0, o, cut(q)], 0.0)
            hid[0, o, cut(q)] = (2.0 * relu * acc[1, o, cut(q)]).astype(BF16)
            hid[1, o, cut(q)] = (relu * relu).astype(BF16)

    def term(a, row, size, q=None):
        first, count = (0, width) if q is None else (q * wide_q, wide_q)

        @pl.loop(0, count // tile)
        def _(j):
            o = pl.ds(pl.multiple_of(first + j * tile, tile), tile)
            grads[a, pl.ds(row, size), o] = lax.dot_general(
                tok[a, :, pl.ds(row, size)], hid[a, :, o], (((0,), (0,)), ((), ())),
                preferred_element_type=F32).astype(BF16)

    def block_term(a, p, q=None):
        term(a, pl.multiple_of(at_ring(p) * blk, blk), blk, q)

    def g_copy(k, s, q):
        d = half - (k >= 2) - s
        f = at_ring(pos + sign_of[k] * d)
        src = grads.at[arr_of[k], pl.ds(pl.multiple_of(f * blk, blk), blk), cut(q)]
        return remote(src, rbuf.at[k, s, :, cut(q)], g_s.at[k, s, q], g_r.at[k, s, q],
                      right if sign_of[k] > 0 else left)

    def add_rows(dst, dst_row, src, count, columns=slice(None)):
        step = math.gcd(count, 32)

        @pl.loop(0, count // step)
        def _(i):
            o = pl.multiple_of(i * step, step)
            at = pl.ds(pl.multiple_of(dst_row + o, step), step)
            total = dst[at, columns].astype(F32) + src[pl.ds(o, step), columns].astype(F32)
            dst[at, columns] = total.astype(BF16)

    def g_step(s, which):
        for k, q in which:
            g_copy(k, s - 1, q).wait_recv()
            f = at_ring(pos + sign_of[k] * (half - (k >= 2) - s))
            add_rows(grads.at[arr_of[k]], f * blk, rbuf.at[k, s - 1], blk, cut(q))
            g_copy(k, s, q).start()

    wide = math.gcd(depth, 256)
    for q in range(parts):
        for k in (0, 1):
            w_copy(k, half - 1, q).wait_recv()
            use(arr_of[k], at_ring(pos - sign_of[k] * half), q=q)
        if not aligned:
            full = pl.ds(0, depth)
            for a, w in ((0, 0), (1, 1), (2, 0)):
                multiply(a, w, full, True, q)
        activate(q)
        if not aligned:
            for a in range(2):
                @pl.loop(0, depth // wide)
                def _(i):
                    term(a, pl.multiple_of(i * wide, wide), wide, q)
        for k in (0, 1):
            if aligned:
                block_term(arr_of[k], pos + sign_of[k] * half, q)
            g_copy(k, 0, q).start()
    for k in (2, 3):
        if aligned:
            block_term(arr_of[k], pos + sign_of[k] * (half - 1))
        for q in range(parts):
            g_copy(k, 0, q).start()
    if aligned:
        if half > 1:
            @pl.loop(0, half - 1)
            def _(i):
                d = half - 1 - i
                block_term(0, pos + d)
                block_term(1, pos - d)
        if half > 2:
            @pl.loop(0, half - 2)
            def _(i):
                d = half - 2 - i
                block_term(1, pos + d)
                block_term(0, pos - d)
        for a in range(2):
            block_term(a, pos)

    @pl.loop(0, rows // step_r)
    def _(i):
        o = pl.ds(pl.multiple_of(i * step_r, step_r), step_r)
        relu = jnp.maximum(acc[2, o, :], 0.0)
        hid[2, o, :] = (relu * relu).astype(BF16)

    wide_d = math.gcd(depth, 256)

    def partial(a, h, w):
        @pl.loop(0, depth // wide_d)
        def _(j):
            o = pl.ds(pl.multiple_of(j * wide_d, wide_d), wide_d)
            part[a, :, o] = lax.dot_general(
                hid[h], wts[w, o, :], (((1,), (1,)), ((), ())), preferred_element_type=F32).astype(BF16)

    def prow(yy, cc):
        return pl.multiple_of((yy * 2 + cc) * rows_dev, rows_dev)

    def od_copy(a, yy):
        return remote(part.at[a, pl.ds(prow(yy, 1 - c), rows_dev), :], dbuf.at[a, yy],
                      od_s.at[a, yy], od_r.at[a, yy], mate)

    def oy_copy(a, s):
        t = (y + y_size - 1 - s) % y_size
        return remote(part.at[a, pl.ds(prow(t, c), rows_dev), :], ybuf.at[a, s],
                      oy_s.at[a, s], oy_r.at[a, s], y_next)

    def send_partial(a, h, w):
        partial(a, h, w)
        for yy in range(y_size):
            od_copy(a, yy).start()

    send_partial(0, 0, 0)
    g_step(1, every if half > 2 else longs)
    send_partial(1, 2, 1)
    for a in range(2):
        for yy in range(y_size):
            od_copy(a, yy).wait_recv()
            add_rows(part.at[a], prow(yy, c), dbuf.at[a, yy], rows_dev)
        if y_size > 1:
            oy_copy(a, 0).start()
    if half - 1 > 2:
        @pl.loop(2, half - 1)
        def _(s):
            g_step(s, every)
    for s in range(1, y_size):
        for a in range(2):
            oy_copy(a, s - 1).wait_recv()
            t = (y + y_size - 1 - s) % y_size
            add_rows(part.at[a], prow(t, c), ybuf.at[a, s - 1], rows_dev)
            if s < y_size - 1:
                oy_copy(a, s).start()
    put_own = ((earlier_out, 0), (later_out, 1))
    for out, a in put_own:
        out[...] = part[a, pl.ds(prow(y, c), rows_dev), :]
    if half - 1 >= 2:
        g_step(half - 1, longs)

    ends = [(k, half - 1 - (k >= 2)) for k in range(4)]
    for k, q in tuple((k, q) for k, q in every if k >= 2) + longs:
        g_copy(k, ends[k][1], q).wait_recv()
    step_b = math.gcd(blk, 32)
    for a, out in ((0, up_out), (1, down_out)):
        @pl.loop(0, blk // step_b)
        def _(i):
            lo = pl.multiple_of(i * step_b, step_b)
            o = pl.ds(lo, step_b)
            got = grads[a, pl.ds(pl.multiple_of(fs * blk + lo, step_b), step_b), :].astype(F32)
            for k, s in ends:
                if arr_of[k] == a:
                    got += rbuf[k, s, o, :].astype(F32)
            out[o, :] = got.astype(BF16)

    for k, q in every:
        for s in range(half - (k >= 2)):
            w_copy(k, s, q).wait_send()
            g_copy(k, s, q).wait_send()
    for a in range(3):
        for s in range(y_size):
            if s < y_size - 1:
                ty_copy(a, s).wait_send()
            td_copy(a, s).wait_send()
    for a in range(2):
        for yy in range(y_size):
            od_copy(a, yy).wait_send()
        for s in range(y_size - 1):
            oy_copy(a, s).wait_send()


def plane_kernel(n, chunks,
                 later_ref, earlier_ref, cot_ref, up_ref, down_ref,
                 later_out, earlier_out, up_out, down_out,
                 tok, wts, hid, grads, gl, gr, fin, xbuf, part, dbuf, qa, qb,
                 t_s, t_r, wx_s, wz_s, w_r, g_s, g_r, f_s, f_r, d_s, d_r, q_s, q_r):
    rows_dev, depth = later_ref.shape
    blk, width = up_ref.shape
    z_size, zrows = n // 2, 2 * blk
    wide, cw = width // 2, width // 2 // chunks
    chip_rows = 2 * rows_dev
    fs, tp = lax.axis_index("fs"), lax.axis_index("tp")
    z, x, y, c = fs // 2, fs % 2, tp // 2, tp % 2
    last = z_size - 1

    right = {"fs": ((z + 1) % z_size) * 2 + x, "tp": tp}
    left = {"fs": ((z + last) % z_size) * 2 + x, "tp": tp}
    x_next = {"fs": z * 2 + 1 - x, "tp": tp}
    y_next = {"fs": fs, "tp": (1 - y) * 2 + c}
    mate = {"fs": fs, "tp": y * 2 + 1 - c}

    barrier = pltpu.get_barrier_semaphore()
    for other in (right, left, x_next, y_next, mate):
        pl.semaphore_signal(barrier, inc=1, device_id=other, device_id_type=MESH)
    pl.semaphore_wait(barrier, 5)

    def remote(src, dst, send, recv, to):
        return pltpu.make_async_remote_copy(
            src_ref=src, dst_ref=dst, send_sem=send, recv_sem=recv, device_id=to, device_id_type=MESH)

    def rows_at(start, count):
        return pl.ds(pl.multiple_of(start, math.gcd(count, 128)), count)

    own_w, own_t = (up_ref, down_ref), (earlier_ref, cot_ref, later_ref)

    def piece(m, h, f):
        return wts.at[m, h, rows_at(f * blk, blk), :]

    def own_cols(m, h, xx):
        return own_w[m].at[:, pl.ds(pl.multiple_of(xx * wide + h * cw, cw), cw)]

    def wx_copy(m, h):
        return remote(own_cols(m, h, 1 - x), piece(m, h, fs), wx_s.at[m, h], w_r.at[m, h, fs], x_next)

    def wz_copy(m, h, f, way, own=False):
        src = own_cols(m, h, x) if own else piece(m, h, f)
        return remote(src, piece(m, h, f), wz_s.at[way, m, h, f], w_r.at[m, h, f], left if way else right)

    def w_got(m, h, f):
        wz_copy(m, h, f, 0).wait_recv()

    def spread(m, h, f, own=False):
        @pl.when(z < last)
        def _():
            wz_copy(m, h, f, 0, own).start()

        @pl.when(z > 0)
        def _():
            wz_copy(m, h, f, 1, own).start()

    def from_x(h):
        for m in range(2):
            w_got(m, h, z * 2 + 1 - x)
            spread(m, h, z * 2 + 1 - x)

    def gather_step(h, d):
        for p in (x, 1 - x):
            for m in range(2):
                @pl.when(z >= d)
                def _():
                    f = (z - d) * 2 + p
                    w_got(m, h, f)

                    @pl.when(z < last)
                    def _():
                        wz_copy(m, h, f, 0).start()

                @pl.when(z + d < z_size)
                def _():
                    f = (z + d) * 2 + p
                    w_got(m, h, f)

                    @pl.when(z > 0)
                    def _():
                        wz_copy(m, h, f, 1).start()

    cut_t = rows_dev * 5 // 8 // 16 * 16
    moves = (
        (x, y, 0, rows_dev, x_next),
        (x, y, 0, rows_dev, y_next),
        (1 - x, y, 0, cut_t, y_next),
        (x, 1 - y, cut_t, rows_dev - cut_t, x_next),
        (x, y, 0, rows_dev, mate),
        (1 - x, y, 0, rows_dev, mate),
        (x, 1 - y, 0, rows_dev, mate),
        (1 - x, 1 - y, 0, cut_t, mate),
        (1 - x, 1 - y, cut_t, rows_dev - cut_t, mate),
    )

    def block_at(xx, yy, cc):
        return ((xx * 2 + yy) * 2 + cc) * rows_dev

    def t_copy(a, k, own=False):
        xx, yy, lo, count, to = moves[k]
        there = tok.at[a, rows_at(block_at(xx, yy, c) + lo, count), :]
        return remote(own_t[a] if own else there, there, t_s.at[a, k], t_r.at[a, k], to)

    def t_first(a):
        for k in (0, 1, 4):
            t_copy(a, k, True).start()

    def t_pass(a):
        t_copy(a, 1).wait_recv()
        t_copy(a, 3).start()
        t_copy(a, 6).start()
        t_copy(a, 0).wait_recv()
        t_copy(a, 2).start()
        t_copy(a, 5).start()

    def t_diagonal(a):
        t_copy(a, 2).wait_recv()
        t_copy(a, 7).start()
        t_copy(a, 3).wait_recv()
        t_copy(a, 8).start()

    def t_wait(a, kinds):
        for k in kinds:
            t_copy(a, k).wait_recv()

    def put(dst, dst_row, src, columns, count):
        step = math.gcd(count, 64)

        @pl.loop(0, count // step)
        def _(i):
            o = pl.multiple_of(i * step, step)
            dst[pl.ds(pl.multiple_of(dst_row + o, step), step), :] = src[pl.ds(o, step), columns]

    def chip_at(i):
        return (((x + i % 2) % 2) * 2 + (y + i // 2) % 2) * chip_rows

    def earlier_hidden(h, lo, hi):
        @pl.loop(lo, hi)
        def _(i):
            o = rows_at(chip_at(i), chip_rows)
            relu = jnp.maximum(jnp.dot(tok[0, o, :], wts[0, h], preferred_element_type=F32), 0.0)
            got = jnp.dot(tok[1, o, :], wts[1, h], preferred_element_type=F32)
            hid[0, h, o, :] = (2.0 * relu * got).astype(BF16)
            hid[1, h, o, :] = (relu * relu).astype(BF16)

    def later_hidden(h):
        @pl.loop(0, 4)
        def _(i):
            o = rows_at(i * chip_rows, chip_rows)
            relu = jnp.maximum(jnp.dot(tok[2, o, :], wts[0, h], preferred_element_type=F32), 0.0)
            hid[2, h, o, :] = (relu * relu).astype(BF16)

    def term(m, h, d):
        o = rows_at(d * zrows, zrows)
        grads[m, h, o, :] = lax.dot_general(
            tok[m, :, o], hid[m, h], (((0,), (0,)), ((), ())), preferred_element_type=F32).astype(BF16)

    def g_copy(m, h, d, way):
        src = grads.at[m, h, rows_at(d * zrows, zrows), :]
        return remote(src, (gr if way else gl).at[m, h, d], g_s.at[way, m, h, d], g_r.at[way, m, h, d],
                      left if way else right)

    def terms(h):
        @pl.loop(0, last)
        def _(k):
            @pl.when(last - k > z)
            def _():
                @pl.loop(0, 2)
                def _(m):
                    term(m, h, last - k)

                    @pl.when(z == 0)
                    def _():
                        g_copy(m, h, last - k, 0).start()

            @pl.when(k < z)
            def _():
                @pl.loop(0, 2)
                def _(m):
                    term(m, h, k)

                    @pl.when(z == last)
                    def _():
                        g_copy(m, h, k, 1).start()

        @pl.loop(0, 2)
        def _(m):
            term(m, h, z)

    def add_rows(dst, dst_row, src, count):
        step = math.gcd(count, 32)

        @pl.loop(0, count // step)
        def _(i):
            o = pl.multiple_of(i * step, step)
            at = pl.ds(pl.multiple_of(dst_row + o, math.gcd(step, 16)), step)
            dst[at, :] = (dst[at, :].astype(F32) + src[pl.ds(o, step), :].astype(F32)).astype(BF16)

    def reduce_step(h, k):
        for m in range(2):
            @pl.when((last - k > z) & (z > 0))
            def _():
                d = last - k
                g_copy(m, h, d, 0).wait_recv()
                add_rows(grads.at[m, h], d * zrows, gl.at[m, h, d], zrows)
                g_copy(m, h, d, 0).start()

            @pl.when((k < z) & (z < last))
            def _():
                g_copy(m, h, k, 1).wait_recv()
                add_rows(grads.at[m, h], k * zrows, gr.at[m, h, k], zrows)
                g_copy(m, h, k, 1).start()

    outs = (up_out, down_out)

    def f_copy(m, h):
        return remote(fin.at[m, h], xbuf.at[m, h], f_s.at[m, h], f_r.at[m, h], x_next)

    def total(m, h, xx, dst, columns, sources):
        step = math.gcd(blk, 32)

        @pl.loop(0, blk // step)
        def _(i):
            o = pl.multiple_of(i * step, step)
            at = pl.ds(pl.multiple_of(xx * blk + o, step), step)
            got = grads[m, h, pl.ds(pl.multiple_of(z * zrows + xx * blk + o, step), step), :].astype(F32)
            for src in sources:
                got += src[m, h, z, at, :].astype(F32)
            dst[pl.ds(o, step), columns] = got.astype(BF16)

    def finish(h):
        mine = pl.ds(pl.multiple_of(x * wide + h * cw, cw), cw)
        for m in range(2):
            @pl.when(z > 0)
            def _():
                g_copy(m, h, z, 0).wait_recv()

            @pl.when(z < last)
            def _():
                g_copy(m, h, z, 1).wait_recv()

            for case, sources in ((z == 0, (gr,)), (z == last, (gl,)), ((z > 0) & (z < last), (gl, gr))):
                @pl.when(case)
                def _():
                    total(m, h, 1 - x, fin.at[m, h], slice(None), sources)

            f_copy(m, h).start()
            for case, sources in ((z == 0, (gr,)), (z == last, (gl,)), ((z > 0) & (z < last), (gl, gr))):
                @pl.when(case)
                def _():
                    total(m, h, x, outs[m], mine, sources)

    def finish_x(h):
        theirs = pl.ds(pl.multiple_of((1 - x) * wide + h * cw, cw), cw)
        step = math.gcd(blk, 32)
        for m in range(2):
            f_copy(m, h).wait_recv()

            @pl.loop(0, blk // step)
            def _(i):
                o = pl.ds(pl.multiple_of(i * step, step), step)
                outs[m][o, theirs] = xbuf[m, h, o, :]

    tile = math.gcd(depth, 256)

    def partial(a, k, w):
        @pl.loop(0, depth // tile)
        def _(j):
            o = pl.ds(pl.multiple_of(j * tile, tile), tile)
            got = None
            for h in range(chunks):
                one = lax.dot_general(hid[k, h], wts[w, h, o, :], (((1,), (1,)), ((), ())),
                                      preferred_element_type=F32)
                got = one if got is None else got + one
            part[a, :, o] = got.astype(BF16)

    def d_copy(a, q):
        return remote(part.at[a, rows_at(q * chip_rows + (1 - c) * rows_dev, rows_dev), :], dbuf.at[a, q],
                      d_s.at[a, q], d_r.at[a, q], mate)

    def d_start(a):
        for q in range(4):
            d_copy(a, q).start()

    cut_q = rows_dev * 3 // 8 // 16 * 16
    low, high = (0, cut_q), (cut_q, rows_dev - cut_q)
    hops = (
        (1 - x, y, low, qa, 0, x_next),
        (1 - x, 1 - y, low, qa, 1, x_next),
        (x, 1 - y, high, qb, 0, y_next),
        (1 - x, 1 - y, high, qb, 1, y_next),
        (x, 1 - y, low, qa, 2, y_next),
        (1 - x, y, high, qb, 2, x_next),
    )

    def q_copy(a, k):
        xx, yy, (lo, count), buf, slot, to = hops[k]
        return remote(part.at[a, rows_at(block_at(xx, yy, c) + lo, count), :], buf.at[a, slot],
                      q_s.at[a, k], q_r.at[a, k], to)

    def q_first(a):
        for q in range(4):
            d_copy(a, q).wait_recv()
            add_rows(part.at[a], q * chip_rows + c * rows_dev, dbuf.at[a, q], rows_dev)
        for k in range(4):
            q_copy(a, k).start()

    def q_second(a):
        q_copy(a, 1).wait_recv()
        add_rows(part.at[a], block_at(x, 1 - y, c), qa.at[a, 1], cut_q)
        q_copy(a, 4).start()
        q_copy(a, 3).wait_recv()
        add_rows(part.at[a], block_at(1 - x, y, c) + cut_q, qb.at[a, 1], rows_dev - cut_q)
        q_copy(a, 5).start()

    def q_last(a, out):
        for k in (0, 4, 2, 5):
            q_copy(a, k).wait_recv()
        for (lo, count), buf in ((low, qa), (high, qb)):
            step = math.gcd(count, 16)

            @pl.loop(0, count // step)
            def _(i):
                o = pl.multiple_of(i * step, step)
                at = pl.ds(o, step)
                own = pl.ds(pl.multiple_of(block_at(x, y, c) + lo + o, step), step)
                out[pl.ds(pl.multiple_of(lo + o, step), step), :] = (
                    part[a, own, :].astype(F32) + buf[a, 0, at, :].astype(F32) + buf[a, 2, at, :].astype(F32)
                ).astype(BF16)

    for m in range(2):
        wx_copy(m, 0).start()
    for m in range(2):
        spread(m, 0, fs, True)
    t_first(0)
    t_first(1)
    for m in range(2):
        for h in range(chunks):
            cols = pl.ds(pl.multiple_of(x * wide + h * cw, cw), cw)
            put(wts.at[m, h], fs * blk, own_w[m], cols, blk)
    for a in range(3):
        put(tok.at[a], block_at(x, y, c), own_t[a], slice(None), rows_dev)
    from_x(0)
    gather_step(0, 1)
    t_pass(0)
    for d in range(2, last):
        gather_step(0, d)
    t_pass(1)
    for h in range(1, chunks):
        for m in range(2):
            wx_copy(m, h).start()
            spread(m, h, fs, True)
    t_first(2)
    gather_step(0, last)
    for a in range(2):
        t_wait(a, (4, 5, 6))
    earlier_hidden(0, 0, 3)
    for a in range(2):
        t_diagonal(a)
    for a in range(2):
        t_wait(a, (7, 8))
    earlier_hidden(0, 3, 4)
    terms(0)
    for h in range(1, chunks):
        from_x(h)
        gather_step(h, 1)
    reduce_step(0, 0)
    t_pass(2)
    for h in range(1, chunks):
        for d in range(2, last):
            gather_step(h, d)
    for k in range(1, last - 1):
        reduce_step(0, k)
    t_diagonal(2)
    t_wait(2, (4, 5, 6, 7, 8))
    later_hidden(0)
    for h in range(1, chunks):
        gather_step(h, last)
        earlier_hidden(h, 0, 4)
        terms(h)
    partial(0, 0, 0)
    d_start(0)
    for h in range(1, chunks):
        later_hidden(h)
    reduce_step(0, last - 1)
    finish(0)
    partial(1, 2, 1)
    d_start(1)
    q_first(0)
    q_first(1)
    for h in range(1, chunks):
        reduce_step(h, 0)
    q_second(0)
    for h in range(1, chunks):
        for k in range(1, last - 1):
            reduce_step(h, k)
    finish_x(0)
    q_second(1)
    q_last(0, earlier_out)
    for h in range(1, chunks):
        reduce_step(h, last - 1)
        finish(h)
    q_last(1, later_out)
    for h in range(1, chunks):
        finish_x(h)

    for m in range(2):
        for h in range(chunks):
            wx_copy(m, h).wait_send()
            f_copy(m, h).wait_send()

            @pl.loop(0, n)
            def _(f):
                @pl.when((f // 2 <= z) & (z < last))
                def _():
                    wz_copy(m, h, f, 0).wait_send()

                @pl.when((f // 2 >= z) & (z > 0))
                def _():
                    wz_copy(m, h, f, 1).wait_send()

            @pl.loop(0, z_size)
            def _(d):
                @pl.when(d > z)
                def _():
                    g_copy(m, h, d, 0).wait_send()

                @pl.when(d < z)
                def _():
                    g_copy(m, h, d, 1).wait_send()
    for a in range(3):
        for k in range(9):
            t_copy(a, k).wait_send()
    for a in range(2):
        for q in range(4):
            d_copy(a, q).wait_send()
        for k in range(6):
            q_copy(a, k).wait_send()


def plane_call(n, m, *args):
    rows_dev, depth = args[0].shape
    blk, width = args[3].shape
    z_size, chunks, rows = n // 2, 2, rows_dev * 8
    cw = width // 2 // chunks
    cut_q = rows_dev * 3 // 8 // 16 * 16
    dma = pltpu.SemaphoreType.DMA
    vmem = pl.BlockSpec(memory_space=pltpu.VMEM)
    return pl.pallas_call(
        functools.partial(plane_kernel, n, chunks),
        out_shape=(
            jax.ShapeDtypeStruct((rows_dev, depth), BF16),
            jax.ShapeDtypeStruct((rows_dev, depth), BF16),
            jax.ShapeDtypeStruct((blk, width), BF16),
            jax.ShapeDtypeStruct((blk, width), BF16),
        ),
        in_specs=[vmem] * 5,
        out_specs=(vmem,) * 4,
        scratch_shapes=[
            pltpu.VMEM((3, rows, depth), BF16),
            pltpu.VMEM((2, chunks, depth, cw), BF16),
            pltpu.VMEM((3, chunks, rows, cw), BF16),
            pltpu.VMEM((2, chunks, depth, cw), BF16),
            pltpu.VMEM((2, chunks, z_size, 2 * blk, cw), BF16),
            pltpu.VMEM((2, chunks, z_size, 2 * blk, cw), BF16),
            pltpu.VMEM((2, chunks, blk, cw), BF16),
            pltpu.VMEM((2, chunks, blk, cw), BF16),
            pltpu.VMEM((2, rows, depth), BF16),
            pltpu.VMEM((2, 4, rows_dev, depth), BF16),
            pltpu.VMEM((2, 3, cut_q, depth), BF16),
            pltpu.VMEM((2, 3, rows_dev - cut_q, depth), BF16),
            dma((3, 9)), dma((3, 9)), dma((2, chunks)), dma((2, 2, chunks, n)), dma((2, chunks, n)),
            dma((2, 2, chunks, z_size)), dma((2, 2, chunks, z_size)), dma((2, chunks)), dma((2, chunks)),
            dma((2, 4)), dma((2, 4)), dma((2, 6)), dma((2, 6)),
        ],
        compiler_params=pltpu.CompilerParams(
            collective_id=0, has_side_effects=True, vmem_limit_bytes=67043328
        ),
        name="feed_forward_planes",
    )(*args)


def ring_call(n, m, *args):
    rows_dev, depth = args[0].shape
    blk, width = args[3].shape
    rows, half, y_size = rows_dev * m, n // 2, m // 2
    dma = pltpu.SemaphoreType.DMA
    vmem = pl.BlockSpec(memory_space=pltpu.VMEM)
    sums = max(y_size - 1, 1)
    parts = 2 if width % 256 == 0 else 1
    return pl.pallas_call(
        functools.partial(kernel, n, m, parts),
        out_shape=(
            jax.ShapeDtypeStruct((rows_dev, depth), BF16),
            jax.ShapeDtypeStruct((rows_dev, depth), BF16),
            jax.ShapeDtypeStruct((blk, width), BF16),
            jax.ShapeDtypeStruct((blk, width), BF16),
        ),
        in_specs=[vmem] * 5,
        out_specs=(vmem,) * 4,
        scratch_shapes=[
            pltpu.VMEM((3, rows, depth), BF16),
            pltpu.VMEM((2, depth, width), BF16),
            pltpu.VMEM((3, rows, width), F32),
            pltpu.VMEM((3, rows, width), BF16),
            pltpu.VMEM((2, depth, width), BF16),
            pltpu.VMEM((4, half, blk, width), BF16),
            pltpu.VMEM((2, rows, depth), BF16),
            pltpu.VMEM((2, y_size, rows_dev, depth), BF16),
            pltpu.VMEM((2, sums, rows_dev, depth), BF16),
            dma((3, y_size)), dma((3, y_size)), dma((3, y_size)), dma((3, y_size)),
            *[dma((4, half, parts))] * 4,
            dma((2, y_size)), dma((2, y_size)), dma((2, sums)), dma((2, sums)),
        ],
        compiler_params=pltpu.CompilerParams(
            collective_id=0, has_side_effects=True, vmem_limit_bytes=67043328
        ),
        name="feed_forward_step",
    )(*args)


def body(n, m, later_rows, earlier_rows, cotangent, up_weight, down_weight, up_total, down_total):
    rows = later_rows.shape[0] * m
    factor = 1.0 / math.sqrt(rows * n)
    width = up_weight.shape[1]
    planar = columns_of(n) == 2 and n > 4 and m == 4 and width % 1024 == 0 and rows % 512 == 0
    later_out, earlier_grad, up_term, down_term = (plane_call if planar else ring_call)(
        n, m, later_rows, earlier_rows, cotangent, up_weight, down_weight)
    up_updated = up_total + up_term.astype(F32) * factor
    down_updated = down_total + down_term.astype(F32) * factor
    return later_out, earlier_grad, up_updated, down_updated


def solution(mesh):
    return jax.shard_map(
        functools.partial(body, mesh.shape["fs"], mesh.shape["tp"]),
        mesh=mesh,
        in_specs=(
            P(("fs", "tp"), None),
            P(("fs", "tp"), None),
            P(("fs", "tp"), None),
            P("fs", "tp"),
            P("fs", "tp"),
            P("fs", "tp"),
            P("fs", "tp"),
        ),
        out_specs=(P(("fs", "tp"), None), P(("fs", "tp"), None), P("fs", "tp"), P("fs", "tp")),
        check_vma=False,
    )
```

```python
import functools
import math

import jax
import jax.numpy as jnp
from jax import lax
from jax.experimental import pallas as pl
from jax.experimental.pallas import tpu as pltpu
from jax.sharding import PartitionSpec as P

MESH = pl.DeviceIdType.MESH
BF16 = jnp.bfloat16
F32 = jnp.float32


def columns_of(n):
    best = 1
    for x in range(1, n + 1):
        if n % x == 0 and 2 * x * x <= n and (n // x) % 2 == 0:
            best = x
    return best


def ring_to_fs(p, n, x_size):
    if x_size == 1:
        return p
    z_size, wide = n // x_size, x_size - 1
    body = z_size * wide
    z, r = p // wide, p % wide
    x = 1 + jnp.where(z % 2 == 0, r, wide - 1 - r)
    back = z_size - 1 - (p - body)
    return jnp.where(p < body, z * x_size + x, back * x_size)


def fs_to_ring(f, n, x_size):
    if x_size == 1:
        return f
    z_size, wide = n // x_size, x_size - 1
    z, x = f // x_size, f % x_size
    r = jnp.where(z % 2 == 0, x - 1, x_size - 1 - x)
    return jnp.where(x == 0, z_size * wide + z_size - 1 - z, z * wide + r)


def kernel(n, m, parts,
           later_ref, earlier_ref, cot_ref, up_ref, down_ref,
           later_out, earlier_out, up_out, down_out,
           tok, wts, acc, hid, grads, rbuf, part, dbuf, ybuf,
           ty_s, ty_r, td_s, td_r, w_s, w_r, g_s, g_r, od_s, od_r, oy_s, oy_r):
    rows_dev, depth = later_ref.shape
    blk, width = up_ref.shape
    rows = rows_dev * m
    half, y_size = n // 2, m // 2
    aligned = blk % 128 == 0
    wide_q = width // parts
    fs, tp = lax.axis_index("fs"), lax.axis_index("tp")
    x_size = columns_of(n)
    pos = fs_to_ring(fs, n, x_size)
    y, c = tp // 2, tp % 2

    def at_ring(p):
        return ring_to_fs((p + 2 * n) % n, n, x_size)

    right = {"fs": at_ring(pos + 1), "tp": tp}
    left = {"fs": at_ring(pos - 1), "tp": tp}
    mate = {"fs": fs, "tp": y * 2 + 1 - c}
    y_next = {"fs": fs, "tp": ((y + 1) % y_size) * 2 + c}
    y_prev = {"fs": fs, "tp": ((y + y_size - 1) % y_size) * 2 + c}

    barrier = pltpu.get_barrier_semaphore()
    for other in (right, left, mate, y_next, y_prev):
        pl.semaphore_signal(barrier, inc=1, device_id=other, device_id_type=MESH)
    pl.semaphore_wait(barrier, 5)

    def remote(src, dst, send, recv, to):
        return pltpu.make_async_remote_copy(
            src_ref=src, dst_ref=dst, send_sem=send, recv_sem=recv, device_id=to, device_id_type=MESH)

    def trows(a, t):
        return tok.at[a, pl.ds(pl.multiple_of(t * rows_dev, rows_dev), rows_dev), :]

    own_w, own_t = (up_ref, down_ref), (earlier_ref, cot_ref, later_ref)

    arr_of, sign_of = (0, 1, 1, 0), (1, -1, 1, -1)

    def cut(q):
        return pl.ds(q * wide_q, wide_q)

    def w_copy(k, s, q, first=False):
        f = at_ring(pos - sign_of[k] * s)
        there = wts.at[arr_of[k], pl.ds(pl.multiple_of(f * blk, blk), blk), cut(q)]
        src = own_w[arr_of[k]].at[:, cut(q)] if first else there
        return remote(src, there, w_s.at[k, s, q], w_r.at[k, s, q], right if sign_of[k] > 0 else left)

    def ty_copy(a, s, first=False):
        t = ((y + y_size - s) % y_size) * 2 + c
        return remote(own_t[a] if first else trows(a, t), trows(a, t), ty_s.at[a, s], ty_r.at[a, s], y_next)

    def td_copy(a, s, first=False):
        t = ((y + y_size - s) % y_size) * 2 + c
        return remote(own_t[a] if first else trows(a, t), trows(a, t), td_s.at[a, s], td_r.at[a, s], mate)

    every = tuple((k, q) for pair in ((0, 1), (2, 3)) for q in range(parts) for k in pair)
    longs = tuple((k, q) for k, q in every if k < 2)
    for k, q in every:
        w_copy(k, 0, q, True).start()
    for a in range(3):
        if y_size > 1:
            ty_copy(a, 0, True).start()
    for a in range(3):
        td_copy(a, 0, True).start()

    def put(dst, dst_row, src, count):
        step = math.gcd(count, 64)

        @pl.loop(0, count // step)
        def _(i):
            o = pl.multiple_of(i * step, step)
            dst[pl.ds(pl.multiple_of(dst_row + o, step), step), :] = src[pl.ds(o, step), :]

    for a in range(2):
        put(wts.at[a], fs * blk, own_w[a], blk)
    for a in range(3):
        put(tok.at[a], tp * rows_dev, own_t[a], rows_dev)

    tile = math.gcd(wide_q, 256)

    def multiply(a, w, rows_w, clear, q=None):
        first, count = (0, width) if q is None else (q * wide_q, wide_q)

        @pl.loop(0, count // tile)
        def _(j):
            o = pl.ds(pl.multiple_of(first + j * tile, tile), tile)
            got = jnp.dot(tok[a, :, rows_w], wts[w, rows_w, o], preferred_element_type=F32)
            if clear:
                acc[a, :, o] = got
            else:
                acc[a, :, o] += got

    def use(w, f, clear=False, q=None):
        if not aligned:
            return
        o = pl.ds(pl.multiple_of(f * blk, blk), blk)
        for a in ((0, 2) if w == 0 else (1,)):
            multiply(a, w, o, clear, q)

    def forward(s, present, go):
        for k, q in present:
            w_copy(k, s - 1, q).wait_recv()
            if (k, q) in go:
                w_copy(k, s, q).start()

    def use_step(s):
        for k in range(4):
            use(arr_of[k], at_ring(pos - sign_of[k] * s))

    forward(1, every, every if half > 2 else longs)
    for s in range(1, y_size):
        for a in range(3):
            ty_copy(a, s - 1).wait_recv()
            if s < y_size - 1:
                ty_copy(a, s).start()
            td_copy(a, s).start()
    for s in range(y_size):
        for a in range(3):
            td_copy(a, s).wait_recv()
    for w in range(2):
        use(w, fs, True)
    if half > 3:
        @pl.loop(2, half - 1)
        def _(s):
            forward(s, every, every)
            use_step(s - 1)
    if half > 2:
        forward(half - 1, every, longs)
        use_step(half - 2)
    use_step(half - 1)

    step_r = math.gcd(rows, 32)

    def activate(q):
        @pl.loop(0, rows // step_r)
        def _(i):
            o = pl.ds(pl.multiple_of(i * step_r, step_r), step_r)
            relu = jnp.maximum(acc[0, o, cut(q)], 0.0)
            hid[0, o, cut(q)] = (2.0 * relu * acc[1, o, cut(q)]).astype(BF16)
            hid[1, o, cut(q)] = (relu * relu).astype(BF16)

    def term(a, row, size, q=None):
        first, count = (0, width) if q is None else (q * wide_q, wide_q)

        @pl.loop(0, count // tile)
        def _(j):
            o = pl.ds(pl.multiple_of(first + j * tile, tile), tile)
            grads[a, pl.ds(row, size), o] = lax.dot_general(
                tok[a, :, pl.ds(row, size)], hid[a, :, o], (((0,), (0,)), ((), ())),
                preferred_element_type=F32).astype(BF16)

    def block_term(a, p, q=None):
        term(a, pl.multiple_of(at_ring(p) * blk, blk), blk, q)

    def g_copy(k, s, q):
        d = half - (k >= 2) - s
        f = at_ring(pos + sign_of[k] * d)
        src = grads.at[arr_of[k], pl.ds(pl.multiple_of(f * blk, blk), blk), cut(q)]
        return remote(src, rbuf.at[k, s, :, cut(q)], g_s.at[k, s, q], g_r.at[k, s, q],
                      right if sign_of[k] > 0 else left)

    def add_rows(dst, dst_row, src, count, columns=slice(None)):
        step = math.gcd(count, 32)

        @pl.loop(0, count // step)
        def _(i):
            o = pl.multiple_of(i * step, step)
            at = pl.ds(pl.multiple_of(dst_row + o, step), step)
            total = dst[at, columns].astype(F32) + src[pl.ds(o, step), columns].astype(F32)
            dst[at, columns] = total.astype(BF16)

    def g_step(s, which):
        for k, q in which:
            g_copy(k, s - 1, q).wait_recv()
            f = at_ring(pos + sign_of[k] * (half - (k >= 2) - s))
            add_rows(grads.at[arr_of[k]], f * blk, rbuf.at[k, s - 1], blk, cut(q))
            g_copy(k, s, q).start()

    wide = math.gcd(depth, 256)
    for q in range(parts):
        for k in (0, 1):
            w_copy(k, half - 1, q).wait_recv()
            use(arr_of[k], at_ring(pos - sign_of[k] * half), q=q)
        if not aligned:
            full = pl.ds(0, depth)
            for a, w in ((0, 0), (1, 1), (2, 0)):
                multiply(a, w, full, True, q)
        activate(q)
        if not aligned:
            for a in range(2):
                @pl.loop(0, depth // wide)
                def _(i):
                    term(a, pl.multiple_of(i * wide, wide), wide, q)
        for k in (0, 1):
            if aligned:
                block_term(arr_of[k], pos + sign_of[k] * half, q)
            g_copy(k, 0, q).start()
    for k in (2, 3):
        if aligned:
            block_term(arr_of[k], pos + sign_of[k] * (half - 1))
        for q in range(parts):
            g_copy(k, 0, q).start()
    if aligned:
        if half > 1:
            @pl.loop(0, half - 1)
            def _(i):
                d = half - 1 - i
                block_term(0, pos + d)
                block_term(1, pos - d)
        if half > 2:
            @pl.loop(0, half - 2)
            def _(i):
                d = half - 2 - i
                block_term(1, pos + d)
                block_term(0, pos - d)
        for a in range(2):
            block_term(a, pos)

    @pl.loop(0, rows // step_r)
    def _(i):
        o = pl.ds(pl.multiple_of(i * step_r, step_r), step_r)
        relu = jnp.maximum(acc[2, o, :], 0.0)
        hid[2, o, :] = (relu * relu).astype(BF16)

    wide_d = math.gcd(depth, 256)

    def partial(a, h, w):
        @pl.loop(0, depth // wide_d)
        def _(j):
            o = pl.ds(pl.multiple_of(j * wide_d, wide_d), wide_d)
            part[a, :, o] = lax.dot_general(
                hid[h], wts[w, o, :], (((1,), (1,)), ((), ())), preferred_element_type=F32).astype(BF16)

    def prow(yy, cc):
        return pl.multiple_of((yy * 2 + cc) * rows_dev, rows_dev)

    def od_copy(a, yy):
        return remote(part.at[a, pl.ds(prow(yy, 1 - c), rows_dev), :], dbuf.at[a, yy],
                      od_s.at[a, yy], od_r.at[a, yy], mate)

    def oy_copy(a, s):
        t = (y + y_size - 1 - s) % y_size
        return remote(part.at[a, pl.ds(prow(t, c), rows_dev), :], ybuf.at[a, s],
                      oy_s.at[a, s], oy_r.at[a, s], y_next)

    def send_partial(a, h, w):
        partial(a, h, w)
        for yy in range(y_size):
            od_copy(a, yy).start()

    send_partial(0, 0, 0)
    g_step(1, every if half > 2 else longs)
    send_partial(1, 2, 1)
    for a in range(2):
        for yy in range(y_size):
            od_copy(a, yy).wait_recv()
            add_rows(part.at[a], prow(yy, c), dbuf.at[a, yy], rows_dev)
        if y_size > 1:
            oy_copy(a, 0).start()
    if half - 1 > 2:
        @pl.loop(2, half - 1)
        def _(s):
            g_step(s, every)
    for s in range(1, y_size):
        for a in range(2):
            oy_copy(a, s - 1).wait_recv()
            t = (y + y_size - 1 - s) % y_size
            add_rows(part.at[a], prow(t, c), ybuf.at[a, s - 1], rows_dev)
            if s < y_size - 1:
                oy_copy(a, s).start()
    put_own = ((earlier_out, 0), (later_out, 1))
    for out, a in put_own:
        out[...] = part[a, pl.ds(prow(y, c), rows_dev), :]
    if half - 1 >= 2:
        g_step(half - 1, longs)

    ends = [(k, half - 1 - (k >= 2)) for k in range(4)]
    for k, q in tuple((k, q) for k, q in every if k >= 2) + longs:
        g_copy(k, ends[k][1], q).wait_recv()
    step_b = math.gcd(blk, 32)
    for a, out in ((0, up_out), (1, down_out)):
        @pl.loop(0, blk // step_b)
        def _(i):
            lo = pl.multiple_of(i * step_b, step_b)
            o = pl.ds(lo, step_b)
            got = grads[a, pl.ds(pl.multiple_of(fs * blk + lo, step_b), step_b), :].astype(F32)
            for k, s in ends:
                if arr_of[k] == a:
                    got += rbuf[k, s, o, :].astype(F32)
            out[o, :] = got.astype(BF16)

    for k, q in every:
        for s in range(half - (k >= 2)):
            w_copy(k, s, q).wait_send()
            g_copy(k, s, q).wait_send()
    for a in range(3):
        for s in range(y_size):
            if s < y_size - 1:
                ty_copy(a, s).wait_send()
            td_copy(a, s).wait_send()
    for a in range(2):
        for yy in range(y_size):
            od_copy(a, yy).wait_send()
        for s in range(y_size - 1):
            oy_copy(a, s).wait_send()


def plane_kernel(n, chunks,
                 later_ref, earlier_ref, cot_ref, up_ref, down_ref,
                 later_out, earlier_out, up_out, down_out,
                 tok, wts, hid, grads, gbuf, fin, xbuf, part, dbuf, qa, qb,
                 t_s, t_r, wx_s, wz_s, w_r, g_s, g_r, f_s, f_r, d_s, d_r, q_s, q_r):
    rows_dev, depth = later_ref.shape
    blk, width = up_ref.shape
    z_size, zrows = n // 2, 2 * blk
    wide, cw = width // 2, width // 2 // chunks
    chip_rows = 2 * rows_dev
    fs, tp = lax.axis_index("fs"), lax.axis_index("tp")
    z, x, y, c = fs // 2, fs % 2, tp // 2, tp % 2
    last = z_size - 1

    right = {"fs": ((z + 1) % z_size) * 2 + x, "tp": tp}
    left = {"fs": ((z + last) % z_size) * 2 + x, "tp": tp}
    x_next = {"fs": z * 2 + 1 - x, "tp": tp}
    y_next = {"fs": fs, "tp": (1 - y) * 2 + c}
    mate = {"fs": fs, "tp": y * 2 + 1 - c}

    barrier = pltpu.get_barrier_semaphore()
    for other in (right, left, x_next, y_next, mate):
        pl.semaphore_signal(barrier, inc=1, device_id=other, device_id_type=MESH)
    pl.semaphore_wait(barrier, 5)

    def remote(src, dst, send, recv, to):
        return pltpu.make_async_remote_copy(
            src_ref=src, dst_ref=dst, send_sem=send, recv_sem=recv, device_id=to, device_id_type=MESH)

    def rows_at(start, count):
        return pl.ds(pl.multiple_of(start, math.gcd(count, 128)), count)

    own_w, own_t = (up_ref, down_ref), (earlier_ref, cot_ref, later_ref)

    def piece(m, h, f):
        return wts.at[m, h, rows_at(f * blk, blk), :]

    def own_cols(m, h, xx):
        return own_w[m].at[:, pl.ds(pl.multiple_of(xx * wide + h * cw, cw), cw)]

    def wx_copy(m, h):
        return remote(own_cols(m, h, 1 - x), piece(m, h, fs), wx_s.at[m, h], w_r.at[m, h, fs], x_next)

    def wz_copy(m, h, f, way, own=False):
        src = own_cols(m, h, x) if own else piece(m, h, f)
        return remote(src, piece(m, h, f), wz_s.at[way, m, h, f], w_r.at[m, h, f], left if way else right)

    def w_got(m, h, f):
        wz_copy(m, h, f, 0).wait_recv()

    def spread(m, h, f, own=False):
        @pl.when(z < last)
        def _():
            wz_copy(m, h, f, 0, own).start()

        @pl.when(z > 0)
        def _():
            wz_copy(m, h, f, 1, own).start()

    def from_x(h, ms=(0, 1)):
        for m in ms:
            w_got(m, h, z * 2 + 1 - x)
            spread(m, h, z * 2 + 1 - x)

    def relay(h, d, columns=(0, 1), ms=(0, 1)):
        for m in ms:
            for p in columns:
                p = (x + p) % 2

                @pl.when((z >= d) & (z < last))
                def _():
                    w_got(m, h, (z - d) * 2 + p)
                    wz_copy(m, h, (z - d) * 2 + p, 0).start()

                @pl.when((z + d < z_size) & (z > 0))
                def _():
                    w_got(m, h, (z + d) * 2 + p)
                    wz_copy(m, h, (z + d) * 2 + p, 1).start()

    def settle(h, m):
        @pl.when((z == 0) | (z == last))
        def _():
            @pl.loop(1, z_size)
            def _(d):
                for p in range(2):
                    w_got(m, h, (z + d) % z_size * 2 + p)

    cut_t = rows_dev * 3 // 4 // 16 * 16
    moves = (
        (x, y, 0, rows_dev, x_next),
        (x, y, 0, rows_dev, y_next),
        (1 - x, y, 0, cut_t, y_next),
        (x, 1 - y, cut_t, rows_dev - cut_t, x_next),
        (x, y, 0, rows_dev, mate),
        (1 - x, y, 0, rows_dev, mate),
        (x, 1 - y, 0, rows_dev, mate),
        (1 - x, 1 - y, 0, cut_t, mate),
        (1 - x, 1 - y, cut_t, rows_dev - cut_t, mate),
    )

    def block_at(xx, yy, cc):
        return ((xx * 2 + yy) * 2 + cc) * rows_dev

    def t_copy(a, k, own=False):
        xx, yy, lo, count, to = moves[k]
        there = tok.at[a, rows_at(block_at(xx, yy, c) + lo, count), :]
        return remote(own_t[a] if own else there, there, t_s.at[a, k], t_r.at[a, k], to)

    def t_first(a):
        for k in (0, 1, 4):
            t_copy(a, k, True).start()

    def t_pass_y(a):
        t_copy(a, 1).wait_recv()
        t_copy(a, 3).start()
        t_copy(a, 6).start()

    def t_pass_x(a):
        t_copy(a, 0).wait_recv()
        t_copy(a, 2).start()
        t_copy(a, 5).start()

    def t_diagonal(a):
        t_copy(a, 2).wait_recv()
        t_copy(a, 7).start()
        t_copy(a, 3).wait_recv()
        t_copy(a, 8).start()

    def t_wait(a, kinds):
        for k in kinds:
            t_copy(a, k).wait_recv()

    def put(dst, dst_row, src, columns, count):
        step = math.gcd(count, 64)

        @pl.loop(0, count // step)
        def _(i):
            o = pl.multiple_of(i * step, step)
            dst[pl.ds(pl.multiple_of(dst_row + o, step), step), :] = src[pl.ds(o, step), columns]

    def chip_at(i):
        return (((x + i % 2) % 2) * 2 + (y + i // 2) % 2) * chip_rows

    def earlier_hidden(h, lo, hi):
        @pl.loop(lo, hi)
        def _(i):
            o = rows_at(chip_at(i), chip_rows)
            relu = jnp.maximum(jnp.dot(tok[0, o, :], wts[0, h], preferred_element_type=F32), 0.0)
            got = jnp.dot(tok[1, o, :], wts[1, h], preferred_element_type=F32)
            hid[0, h, o, :] = (2.0 * relu * got).astype(BF16)
            hid[1, h, o, :] = (relu * relu).astype(BF16)

    def later_hidden(h):
        @pl.loop(0, 4)
        def _(i):
            o = rows_at(i * chip_rows, chip_rows)
            relu = jnp.maximum(jnp.dot(tok[2, o, :], wts[0, h], preferred_element_type=F32), 0.0)
            hid[2, h, o, :] = (relu * relu).astype(BF16)

    def term(m, h, d):
        o = rows_at(d * zrows, zrows)
        grads[m, h, o, :] = lax.dot_general(
            tok[m, :, o], hid[m, h], (((0,), (0,)), ((), ())), preferred_element_type=F32).astype(BF16)

    def g_copy(m, h, d, way):
        src = grads.at[m, h, rows_at(d * zrows, zrows), :]
        to = {"fs": ((z + z_size + 1 - 2 * way) % z_size) * 2 + x, "tp": tp}
        return remote(src, gbuf.at[way, m, h, d], g_s.at[way, m, h, d], g_r.at[way, m, h, d], to)

    def terms(h, lo, hi):
        @pl.loop(lo, hi)
        def _(k):
            @pl.when(last - k > z)
            def _():
                @pl.loop(0, 2)
                def _(m):
                    term(m, h, last - k)

                    @pl.when(z == 0)
                    def _():
                        g_copy(m, h, last - k, 0).start()

            @pl.when(k < z)
            def _():
                @pl.loop(0, 2)
                def _(m):
                    term(m, h, k)

                    @pl.when(z == last)
                    def _():
                        g_copy(m, h, k, 1).start()

    def own_terms(h):
        @pl.loop(0, 2)
        def _(m):
            term(m, h, z)

    def add_rows(dst, dst_row, src, count):
        step = math.gcd(count, 32)

        @pl.loop(0, count // step)
        def _(i):
            o = pl.multiple_of(i * step, step)
            at = pl.ds(pl.multiple_of(dst_row + o, math.gcd(step, 16)), step)
            dst[at, :] = (dst[at, :].astype(F32) + src[pl.ds(o, step), :].astype(F32)).astype(BF16)

    side = 2 * z // z_size

    def reduce_step(h, k, m, near):
        way = side if near else 1 - side
        d = (1 - way) * (last - k) + way * k
        beyond = (1 - 2 * way) * (d - z)
        behind = (1 - way) * z + way * (last - z)

        @pl.when((beyond > 0) & (behind > 0))
        def _():
            g_copy(m, h, d, way).wait_recv()
            add_rows(grads.at[m, h], d * zrows, gbuf.at[way, m, h, d], zrows)
            g_copy(m, h, d, way).start()

    outs = (up_out, down_out)

    def f_copy(m, h):
        return remote(fin.at[m, h], xbuf.at[m, h], f_s.at[m, h], f_r.at[m, h], x_next)

    def total(m, h, xx, dst, columns, sources):
        step = math.gcd(blk, 32)

        @pl.loop(0, blk // step)
        def _(i):
            o = pl.multiple_of(i * step, step)
            at = pl.ds(pl.multiple_of(xx * blk + o, step), step)
            got = grads[m, h, pl.ds(pl.multiple_of(z * zrows + xx * blk + o, step), step), :].astype(F32)
            for src in sources:
                got += gbuf[src, m, h, z, at, :].astype(F32)
            dst[pl.ds(o, step), columns] = got.astype(BF16)

    def finish(h, ms=(0, 1)):
        mine = pl.ds(pl.multiple_of(x * wide + h * cw, cw), cw)
        for m in ms:
            @pl.when(z > 0)
            def _():
                g_copy(m, h, z, 0).wait_recv()

            @pl.when(z < last)
            def _():
                g_copy(m, h, z, 1).wait_recv()

            for case, sources in ((z == 0, (1,)), (z == last, (0,)), ((z > 0) & (z < last), (0, 1))):
                @pl.when(case)
                def _():
                    total(m, h, 1 - x, fin.at[m, h], slice(None), sources)

            f_copy(m, h).start()
            for case, sources in ((z == 0, (1,)), (z == last, (0,)), ((z > 0) & (z < last), (0, 1))):
                @pl.when(case)
                def _():
                    total(m, h, x, outs[m], mine, sources)

    def finish_x(h):
        theirs = pl.ds(pl.multiple_of((1 - x) * wide + h * cw, cw), cw)
        step = math.gcd(blk, 32)
        for m in range(2):
            f_copy(m, h).wait_recv()

            @pl.loop(0, blk // step)
            def _(i):
                o = pl.ds(pl.multiple_of(i * step, step), step)
                outs[m][o, theirs] = xbuf[m, h, o, :]

    tile = math.gcd(depth, 256)

    def partial(a, k, w):
        @pl.loop(0, depth // tile)
        def _(j):
            o = pl.ds(pl.multiple_of(j * tile, tile), tile)
            got = None
            for h in range(chunks):
                one = lax.dot_general(hid[k, h], wts[w, h, o, :], (((1,), (1,)), ((), ())),
                                      preferred_element_type=F32)
                got = one if got is None else got + one
            part[a, :, o] = got.astype(BF16)

    def d_copy(a, q):
        return remote(part.at[a, rows_at(q * chip_rows + (1 - c) * rows_dev, rows_dev), :], dbuf.at[a, q],
                      d_s.at[a, q], d_r.at[a, q], mate)

    def d_start(a):
        for q in range(4):
            d_copy(a, q).start()

    cut_q = rows_dev * 3 // 8 // 16 * 16
    low, high = (0, cut_q), (cut_q, rows_dev - cut_q)
    hops = (
        (1 - x, y, low, qa, 0, x_next),
        (1 - x, 1 - y, low, qa, 1, x_next),
        (x, 1 - y, high, qb, 0, y_next),
        (1 - x, 1 - y, high, qb, 1, y_next),
        (x, 1 - y, low, qa, 2, y_next),
        (1 - x, y, high, qb, 2, x_next),
    )

    def q_copy(a, k):
        xx, yy, (lo, count), buf, slot, to = hops[k]
        return remote(part.at[a, rows_at(block_at(xx, yy, c) + lo, count), :], buf.at[a, slot],
                      q_s.at[a, k], q_r.at[a, k], to)

    def q_first(a):
        for q in range(4):
            d_copy(a, q).wait_recv()
            add_rows(part.at[a], q * chip_rows + c * rows_dev, dbuf.at[a, q], rows_dev)
        for k in range(4):
            q_copy(a, k).start()

    def q_second(a):
        q_copy(a, 1).wait_recv()
        add_rows(part.at[a], block_at(x, 1 - y, c), qa.at[a, 1], cut_q)
        q_copy(a, 4).start()
        q_copy(a, 3).wait_recv()
        add_rows(part.at[a], block_at(1 - x, y, c) + cut_q, qb.at[a, 1], rows_dev - cut_q)
        q_copy(a, 5).start()

    def q_last(a, out):
        for k in (0, 4, 2, 5):
            q_copy(a, k).wait_recv()
        for (lo, count), buf in ((low, qa), (high, qb)):
            step = math.gcd(count, 16)

            @pl.loop(0, count // step)
            def _(i):
                o = pl.multiple_of(i * step, step)
                at = pl.ds(o, step)
                own = pl.ds(pl.multiple_of(block_at(x, y, c) + lo + o, step), step)
                out[pl.ds(pl.multiple_of(lo + o, step), step), :] = (
                    part[a, own, :].astype(F32) + buf[a, 0, at, :].astype(F32) + buf[a, 2, at, :].astype(F32)
                ).astype(BF16)

    for m in range(2):
        wx_copy(m, 0).start()
    for m in range(2):
        spread(m, 0, fs, True)
    t_first(0)
    t_first(1)
    for m in range(2):
        wx_copy(m, 1).start()
    for m in range(2):
        for h in range(chunks):
            cols = pl.ds(pl.multiple_of(x * wide + h * cw, cw), cw)
            put(wts.at[m, h], fs * blk, own_w[m], cols, blk)
    for a in range(3):
        put(tok.at[a], block_at(x, y, c), own_t[a], slice(None), rows_dev)
    from_x(0)
    relay(0, 1)
    t_pass_y(0)
    t_pass_x(0)
    relay(0, 2)
    t_pass_y(1)
    t_pass_x(1)
    for m in range(2):
        spread(m, 1, fs, True)
    t_first(2)
    settle(0, 0)
    settle(0, 1)
    for a in range(2):
        t_wait(a, (4, 5, 6))
    earlier_hidden(0, 0, 3)
    from_x(1)
    t_diagonal(0)
    relay(1, 1, (0,))
    t_diagonal(1)
    for a in range(2):
        t_wait(a, (7, 8))
    earlier_hidden(0, 3, 4)
    terms(0, 0, last)
    own_terms(0)
    t_pass_y(2)
    relay(1, 1, (1,), (0,))
    relay(1, 2, (0,), (0,))
    reduce_step(0, 0, 0, True)
    t_pass_x(2)
    relay(1, 2, (1,), (0,))
    relay(1, 1, (1,), (1,))
    relay(1, 2, (0,), (1,))
    reduce_step(0, 0, 1, True)
    relay(1, 2, (1,), (1,))
    reduce_step(0, 0, 0, False)
    t_diagonal(2)
    settle(1, 0)
    t_wait(2, (4, 5, 6, 7, 8))
    later_hidden(0)
    later_hidden(1)
    reduce_step(0, 1, 0, True)
    reduce_step(0, 0, 1, False)
    settle(1, 1)
    partial(1, 2, 1)
    d_start(1)
    earlier_hidden(1, 0, 4)
    reduce_step(0, 1, 1, True)
    terms(1, 0, 1)
    q_first(1)
    terms(1, 1, last)
    own_terms(1)
    partial(0, 0, 0)
    d_start(0)
    finish(0, (0,))
    finish(0, (1,))
    q_first(0)
    reduce_step(1, 0, 0, True)
    reduce_step(1, 0, 1, True)
    q_second(1)
    reduce_step(1, 0, 0, False)
    finish_x(0)
    reduce_step(1, 1, 0, True)
    reduce_step(1, 0, 1, False)
    reduce_step(1, 1, 1, True)
    q_second(0)
    q_last(1, later_out)
    q_last(0, earlier_out)
    finish(1, (0,))
    finish(1, (1,))
    finish_x(1)

    for m in range(2):
        for h in range(chunks):
            wx_copy(m, h).wait_send()
            f_copy(m, h).wait_send()

            @pl.loop(0, n)
            def _(f):
                @pl.when((f // 2 <= z) & (z < last))
                def _():
                    wz_copy(m, h, f, 0).wait_send()

                @pl.when((f // 2 >= z) & (z > 0))
                def _():
                    wz_copy(m, h, f, 1).wait_send()

            @pl.loop(0, z_size)
            def _(d):
                @pl.when(d > z)
                def _():
                    g_copy(m, h, d, 0).wait_send()

                @pl.when(d < z)
                def _():
                    g_copy(m, h, d, 1).wait_send()
    for a in range(3):
        for k in range(9):
            t_copy(a, k).wait_send()
    for a in range(2):
        for q in range(4):
            d_copy(a, q).wait_send()
        for k in range(6):
            q_copy(a, k).wait_send()


def plane_call(n, m, *args):
    rows_dev, depth = args[0].shape
    blk, width = args[3].shape
    z_size, chunks, rows = n // 2, 2, rows_dev * 8
    cw = width // 2 // chunks
    cut_q = rows_dev * 3 // 8 // 16 * 16
    dma = pltpu.SemaphoreType.DMA
    vmem = pl.BlockSpec(memory_space=pltpu.VMEM)
    return pl.pallas_call(
        functools.partial(plane_kernel, n, chunks),
        out_shape=(
            jax.ShapeDtypeStruct((rows_dev, depth), BF16),
            jax.ShapeDtypeStruct((rows_dev, depth), BF16),
            jax.ShapeDtypeStruct((blk, width), BF16),
            jax.ShapeDtypeStruct((blk, width), BF16),
        ),
        in_specs=[vmem] * 5,
        out_specs=(vmem,) * 4,
        scratch_shapes=[
            pltpu.VMEM((3, rows, depth), BF16),
            pltpu.VMEM((2, chunks, depth, cw), BF16),
            pltpu.VMEM((3, chunks, rows, cw), BF16),
            pltpu.VMEM((2, chunks, depth, cw), BF16),
            pltpu.VMEM((2, 2, chunks, z_size, 2 * blk, cw), BF16),
            pltpu.VMEM((2, chunks, blk, cw), BF16),
            pltpu.VMEM((2, chunks, blk, cw), BF16),
            pltpu.VMEM((2, rows, depth), BF16),
            pltpu.VMEM((2, 4, rows_dev, depth), BF16),
            pltpu.VMEM((2, 3, cut_q, depth), BF16),
            pltpu.VMEM((2, 3, rows_dev - cut_q, depth), BF16),
            dma((3, 9)), dma((3, 9)), dma((2, chunks)), dma((2, 2, chunks, n)), dma((2, chunks, n)),
            dma((2, 2, chunks, z_size)), dma((2, 2, chunks, z_size)), dma((2, chunks)), dma((2, chunks)),
            dma((2, 4)), dma((2, 4)), dma((2, 6)), dma((2, 6)),
        ],
        compiler_params=pltpu.CompilerParams(
            collective_id=0, has_side_effects=True, vmem_limit_bytes=67043328
        ),
        name="feed_forward_planes",
    )(*args)


def ring_call(n, m, *args):
    rows_dev, depth = args[0].shape
    blk, width = args[3].shape
    rows, half, y_size = rows_dev * m, n // 2, m // 2
    dma = pltpu.SemaphoreType.DMA
    vmem = pl.BlockSpec(memory_space=pltpu.VMEM)
    sums = max(y_size - 1, 1)
    parts = 2 if width % 256 == 0 else 1
    return pl.pallas_call(
        functools.partial(kernel, n, m, parts),
        out_shape=(
            jax.ShapeDtypeStruct((rows_dev, depth), BF16),
            jax.ShapeDtypeStruct((rows_dev, depth), BF16),
            jax.ShapeDtypeStruct((blk, width), BF16),
            jax.ShapeDtypeStruct((blk, width), BF16),
        ),
        in_specs=[vmem] * 5,
        out_specs=(vmem,) * 4,
        scratch_shapes=[
            pltpu.VMEM((3, rows, depth), BF16),
            pltpu.VMEM((2, depth, width), BF16),
            pltpu.VMEM((3, rows, width), F32),
            pltpu.VMEM((3, rows, width), BF16),
            pltpu.VMEM((2, depth, width), BF16),
            pltpu.VMEM((4, half, blk, width), BF16),
            pltpu.VMEM((2, rows, depth), BF16),
            pltpu.VMEM((2, y_size, rows_dev, depth), BF16),
            pltpu.VMEM((2, sums, rows_dev, depth), BF16),
            dma((3, y_size)), dma((3, y_size)), dma((3, y_size)), dma((3, y_size)),
            *[dma((4, half, parts))] * 4,
            dma((2, y_size)), dma((2, y_size)), dma((2, sums)), dma((2, sums)),
        ],
        compiler_params=pltpu.CompilerParams(
            collective_id=0, has_side_effects=True, vmem_limit_bytes=67043328
        ),
        name="feed_forward_step",
    )(*args)


def body(n, m, later_rows, earlier_rows, cotangent, up_weight, down_weight, up_total, down_total):
    rows = later_rows.shape[0] * m
    factor = 1.0 / math.sqrt(rows * n)
    width = up_weight.shape[1]
    planar = columns_of(n) == 2 and n == 8 and m == 4 and width % 1024 == 0 and rows % 512 == 0
    later_out, earlier_grad, up_term, down_term = (plane_call if planar else ring_call)(
        n, m, later_rows, earlier_rows, cotangent, up_weight, down_weight)
    up_updated = up_total + up_term.astype(F32) * factor
    down_updated = down_total + down_term.astype(F32) * factor
    return later_out, earlier_grad, up_updated, down_updated


def solution(mesh):
    return jax.shard_map(
        functools.partial(body, mesh.shape["fs"], mesh.shape["tp"]),
        mesh=mesh,
        in_specs=(
            P(("fs", "tp"), None),
            P(("fs", "tp"), None),
            P(("fs", "tp"), None),
            P("fs", "tp"),
            P("fs", "tp"),
            P("fs", "tp"),
            P("fs", "tp"),
        ),
        out_specs=(P(("fs", "tp"), None), P(("fs", "tp"), None), P("fs", "tp"), P("fs", "tp")),
        check_vma=False,
    )
```

```python
import functools
import math

import jax
import jax.numpy as jnp
from jax import lax
from jax.experimental import pallas as pl
from jax.experimental.pallas import tpu as pltpu
from jax.sharding import PartitionSpec as P

MESH = pl.DeviceIdType.MESH
BF16 = jnp.bfloat16
F32 = jnp.float32


def columns_of(n):
    best = 1
    for x in range(1, n + 1):
        if n % x == 0 and 2 * x * x <= n and (n // x) % 2 == 0:
            best = x
    return best


def ring_to_fs(p, n, x_size):
    if x_size == 1:
        return p
    z_size, wide = n // x_size, x_size - 1
    body = z_size * wide
    z, r = p // wide, p % wide
    x = 1 + jnp.where(z % 2 == 0, r, wide - 1 - r)
    back = z_size - 1 - (p - body)
    return jnp.where(p < body, z * x_size + x, back * x_size)


def fs_to_ring(f, n, x_size):
    if x_size == 1:
        return f
    z_size, wide = n // x_size, x_size - 1
    z, x = f // x_size, f % x_size
    r = jnp.where(z % 2 == 0, x - 1, x_size - 1 - x)
    return jnp.where(x == 0, z_size * wide + z_size - 1 - z, z * wide + r)


def kernel(n, m, parts,
           later_ref, earlier_ref, cot_ref, up_ref, down_ref,
           later_out, earlier_out, up_out, down_out,
           tok, wts, acc, hid, grads, rbuf, part, dbuf, ybuf,
           ty_s, ty_r, td_s, td_r, w_s, w_r, g_s, g_r, od_s, od_r, oy_s, oy_r):
    rows_dev, depth = later_ref.shape
    blk, width = up_ref.shape
    rows = rows_dev * m
    half, y_size = n // 2, m // 2
    aligned = blk % 128 == 0
    wide_q = width // parts
    fs, tp = lax.axis_index("fs"), lax.axis_index("tp")
    x_size = columns_of(n)
    pos = fs_to_ring(fs, n, x_size)
    y, c = tp // 2, tp % 2

    def at_ring(p):
        return ring_to_fs((p + 2 * n) % n, n, x_size)

    right = {"fs": at_ring(pos + 1), "tp": tp}
    left = {"fs": at_ring(pos - 1), "tp": tp}
    mate = {"fs": fs, "tp": y * 2 + 1 - c}
    y_next = {"fs": fs, "tp": ((y + 1) % y_size) * 2 + c}
    y_prev = {"fs": fs, "tp": ((y + y_size - 1) % y_size) * 2 + c}

    barrier = pltpu.get_barrier_semaphore()
    for other in (right, left, mate, y_next, y_prev):
        pl.semaphore_signal(barrier, inc=1, device_id=other, device_id_type=MESH)
    pl.semaphore_wait(barrier, 5)

    def remote(src, dst, send, recv, to):
        return pltpu.make_async_remote_copy(
            src_ref=src, dst_ref=dst, send_sem=send, recv_sem=recv, device_id=to, device_id_type=MESH)

    def trows(a, t):
        return tok.at[a, pl.ds(pl.multiple_of(t * rows_dev, rows_dev), rows_dev), :]

    own_w, own_t = (up_ref, down_ref), (earlier_ref, cot_ref, later_ref)

    arr_of, sign_of = (0, 1, 1, 0), (1, -1, 1, -1)

    def cut(q):
        return pl.ds(q * wide_q, wide_q)

    def w_copy(k, s, q, first=False):
        f = at_ring(pos - sign_of[k] * s)
        there = wts.at[arr_of[k], pl.ds(pl.multiple_of(f * blk, blk), blk), cut(q)]
        src = own_w[arr_of[k]].at[:, cut(q)] if first else there
        return remote(src, there, w_s.at[k, s, q], w_r.at[k, s, q], right if sign_of[k] > 0 else left)

    def ty_copy(a, s, first=False):
        t = ((y + y_size - s) % y_size) * 2 + c
        return remote(own_t[a] if first else trows(a, t), trows(a, t), ty_s.at[a, s], ty_r.at[a, s], y_next)

    def td_copy(a, s, first=False):
        t = ((y + y_size - s) % y_size) * 2 + c
        return remote(own_t[a] if first else trows(a, t), trows(a, t), td_s.at[a, s], td_r.at[a, s], mate)

    every = tuple((k, q) for pair in ((0, 1), (2, 3)) for q in range(parts) for k in pair)
    longs = tuple((k, q) for k, q in every if k < 2)
    for k, q in every:
        w_copy(k, 0, q, True).start()
    for a in range(3):
        if y_size > 1:
            ty_copy(a, 0, True).start()
    for a in range(3):
        td_copy(a, 0, True).start()

    def put(dst, dst_row, src, count):
        step = math.gcd(count, 64)

        @pl.loop(0, count // step)
        def _(i):
            o = pl.multiple_of(i * step, step)
            dst[pl.ds(pl.multiple_of(dst_row + o, step), step), :] = src[pl.ds(o, step), :]

    for a in range(2):
        put(wts.at[a], fs * blk, own_w[a], blk)
    for a in range(3):
        put(tok.at[a], tp * rows_dev, own_t[a], rows_dev)

    tile = math.gcd(wide_q, 256)

    def multiply(a, w, rows_w, clear, q=None):
        first, count = (0, width) if q is None else (q * wide_q, wide_q)

        @pl.loop(0, count // tile)
        def _(j):
            o = pl.ds(pl.multiple_of(first + j * tile, tile), tile)
            got = jnp.dot(tok[a, :, rows_w], wts[w, rows_w, o], preferred_element_type=F32)
            if clear:
                acc[a, :, o] = got
            else:
                acc[a, :, o] += got

    def use(w, f, clear=False, q=None):
        if not aligned:
            return
        o = pl.ds(pl.multiple_of(f * blk, blk), blk)
        for a in ((0, 2) if w == 0 else (1,)):
            multiply(a, w, o, clear, q)

    def forward(s, present, go):
        for k, q in present:
            w_copy(k, s - 1, q).wait_recv()
            if (k, q) in go:
                w_copy(k, s, q).start()

    def use_step(s):
        for k in range(4):
            use(arr_of[k], at_ring(pos - sign_of[k] * s))

    forward(1, every, every if half > 2 else longs)
    for s in range(1, y_size):
        for a in range(3):
            ty_copy(a, s - 1).wait_recv()
            if s < y_size - 1:
                ty_copy(a, s).start()
            td_copy(a, s).start()
    for s in range(y_size):
        for a in range(3):
            td_copy(a, s).wait_recv()
    for w in range(2):
        use(w, fs, True)
    if half > 3:
        @pl.loop(2, half - 1)
        def _(s):
            forward(s, every, every)
            use_step(s - 1)
    if half > 2:
        forward(half - 1, every, longs)
        use_step(half - 2)
    use_step(half - 1)

    step_r = math.gcd(rows, 32)

    def activate(q):
        @pl.loop(0, rows // step_r)
        def _(i):
            o = pl.ds(pl.multiple_of(i * step_r, step_r), step_r)
            relu = jnp.maximum(acc[0, o, cut(q)], 0.0)
            hid[0, o, cut(q)] = (2.0 * relu * acc[1, o, cut(q)]).astype(BF16)
            hid[1, o, cut(q)] = (relu * relu).astype(BF16)

    def term(a, row, size, q=None):
        first, count = (0, width) if q is None else (q * wide_q, wide_q)

        @pl.loop(0, count // tile)
        def _(j):
            o = pl.ds(pl.multiple_of(first + j * tile, tile), tile)
            grads[a, pl.ds(row, size), o] = lax.dot_general(
                tok[a, :, pl.ds(row, size)], hid[a, :, o], (((0,), (0,)), ((), ())),
                preferred_element_type=F32).astype(BF16)

    def block_term(a, p, q=None):
        term(a, pl.multiple_of(at_ring(p) * blk, blk), blk, q)

    def g_copy(k, s, q):
        d = half - (k >= 2) - s
        f = at_ring(pos + sign_of[k] * d)
        src = grads.at[arr_of[k], pl.ds(pl.multiple_of(f * blk, blk), blk), cut(q)]
        return remote(src, rbuf.at[k, s, :, cut(q)], g_s.at[k, s, q], g_r.at[k, s, q],
                      right if sign_of[k] > 0 else left)

    def add_rows(dst, dst_row, src, count, columns=slice(None)):
        step = math.gcd(count, 32)

        @pl.loop(0, count // step)
        def _(i):
            o = pl.multiple_of(i * step, step)
            at = pl.ds(pl.multiple_of(dst_row + o, step), step)
            total = dst[at, columns].astype(F32) + src[pl.ds(o, step), columns].astype(F32)
            dst[at, columns] = total.astype(BF16)

    def g_step(s, which):
        for k, q in which:
            g_copy(k, s - 1, q).wait_recv()
            f = at_ring(pos + sign_of[k] * (half - (k >= 2) - s))
            add_rows(grads.at[arr_of[k]], f * blk, rbuf.at[k, s - 1], blk, cut(q))
            g_copy(k, s, q).start()

    wide = math.gcd(depth, 256)
    for q in range(parts):
        for k in (0, 1):
            w_copy(k, half - 1, q).wait_recv()
            use(arr_of[k], at_ring(pos - sign_of[k] * half), q=q)
        if not aligned:
            full = pl.ds(0, depth)
            for a, w in ((0, 0), (1, 1), (2, 0)):
                multiply(a, w, full, True, q)
        activate(q)
        if not aligned:
            for a in range(2):
                @pl.loop(0, depth // wide)
                def _(i):
                    term(a, pl.multiple_of(i * wide, wide), wide, q)
        for k in (0, 1):
            if aligned:
                block_term(arr_of[k], pos + sign_of[k] * half, q)
            g_copy(k, 0, q).start()
    for k in (2, 3):
        if aligned:
            block_term(arr_of[k], pos + sign_of[k] * (half - 1))
        for q in range(parts):
            g_copy(k, 0, q).start()
    if aligned:
        if half > 1:
            @pl.loop(0, half - 1)
            def _(i):
                d = half - 1 - i
                block_term(0, pos + d)
                block_term(1, pos - d)
        if half > 2:
            @pl.loop(0, half - 2)
            def _(i):
                d = half - 2 - i
                block_term(1, pos + d)
                block_term(0, pos - d)
        for a in range(2):
            block_term(a, pos)

    @pl.loop(0, rows // step_r)
    def _(i):
        o = pl.ds(pl.multiple_of(i * step_r, step_r), step_r)
        relu = jnp.maximum(acc[2, o, :], 0.0)
        hid[2, o, :] = (relu * relu).astype(BF16)

    wide_d = math.gcd(depth, 256)

    def partial(a, h, w):
        @pl.loop(0, depth // wide_d)
        def _(j):
            o = pl.ds(pl.multiple_of(j * wide_d, wide_d), wide_d)
            part[a, :, o] = lax.dot_general(
                hid[h], wts[w, o, :], (((1,), (1,)), ((), ())), preferred_element_type=F32).astype(BF16)

    def prow(yy, cc):
        return pl.multiple_of((yy * 2 + cc) * rows_dev, rows_dev)

    def od_copy(a, yy):
        return remote(part.at[a, pl.ds(prow(yy, 1 - c), rows_dev), :], dbuf.at[a, yy],
                      od_s.at[a, yy], od_r.at[a, yy], mate)

    def oy_copy(a, s):
        t = (y + y_size - 1 - s) % y_size
        return remote(part.at[a, pl.ds(prow(t, c), rows_dev), :], ybuf.at[a, s],
                      oy_s.at[a, s], oy_r.at[a, s], y_next)

    def send_partial(a, h, w):
        partial(a, h, w)
        for yy in range(y_size):
            od_copy(a, yy).start()

    send_partial(0, 0, 0)
    g_step(1, every if half > 2 else longs)
    send_partial(1, 2, 1)
    for a in range(2):
        for yy in range(y_size):
            od_copy(a, yy).wait_recv()
            add_rows(part.at[a], prow(yy, c), dbuf.at[a, yy], rows_dev)
        if y_size > 1:
            oy_copy(a, 0).start()
    if half - 1 > 2:
        @pl.loop(2, half - 1)
        def _(s):
            g_step(s, every)
    for s in range(1, y_size):
        for a in range(2):
            oy_copy(a, s - 1).wait_recv()
            t = (y + y_size - 1 - s) % y_size
            add_rows(part.at[a], prow(t, c), ybuf.at[a, s - 1], rows_dev)
            if s < y_size - 1:
                oy_copy(a, s).start()
    put_own = ((earlier_out, 0), (later_out, 1))
    for out, a in put_own:
        out[...] = part[a, pl.ds(prow(y, c), rows_dev), :]
    if half - 1 >= 2:
        g_step(half - 1, longs)

    ends = [(k, half - 1 - (k >= 2)) for k in range(4)]
    for k, q in tuple((k, q) for k, q in every if k >= 2) + longs:
        g_copy(k, ends[k][1], q).wait_recv()
    step_b = math.gcd(blk, 32)
    for a, out in ((0, up_out), (1, down_out)):
        @pl.loop(0, blk // step_b)
        def _(i):
            lo = pl.multiple_of(i * step_b, step_b)
            o = pl.ds(lo, step_b)
            got = grads[a, pl.ds(pl.multiple_of(fs * blk + lo, step_b), step_b), :].astype(F32)
            for k, s in ends:
                if arr_of[k] == a:
                    got += rbuf[k, s, o, :].astype(F32)
            out[o, :] = got.astype(BF16)

    for k, q in every:
        for s in range(half - (k >= 2)):
            w_copy(k, s, q).wait_send()
            g_copy(k, s, q).wait_send()
    for a in range(3):
        for s in range(y_size):
            if s < y_size - 1:
                ty_copy(a, s).wait_send()
            td_copy(a, s).wait_send()
    for a in range(2):
        for yy in range(y_size):
            od_copy(a, yy).wait_send()
        for s in range(y_size - 1):
            oy_copy(a, s).wait_send()


def plane_kernel(n, chunks, factor,
                 later_ref, earlier_ref, cot_ref, up_ref, down_ref, up_total, down_total,
                 later_out, earlier_out, up_out, down_out,
                 tok, wts, hid, grads, gbuf, fin, xbuf, part, dbuf, qa, qb, stage, sums,
                 l_s, o_s, t_s, t_r, wx_s, wz_s, w_r, g_s, g_r, f_s, f_r, d_s, d_r, q_s, q_r, q_l):
    rows_dev, depth = later_ref.shape
    blk, width = up_ref.shape
    z_size, zrows = n // 2, 2 * blk
    wide, cw = width // 2, width // 2 // chunks
    chip_rows = 2 * rows_dev
    fs, tp = lax.axis_index("fs"), lax.axis_index("tp")
    z, x, y, c = fs // 2, fs % 2, tp // 2, tp % 2
    last = z_size - 1

    right = {"fs": ((z + 1) % z_size) * 2 + x, "tp": tp}
    left = {"fs": ((z + last) % z_size) * 2 + x, "tp": tp}
    x_next = {"fs": z * 2 + 1 - x, "tp": tp}
    y_next = {"fs": fs, "tp": (1 - y) * 2 + c}
    mate = {"fs": fs, "tp": y * 2 + 1 - c}

    def block_at(xx, yy, cc):
        return ((xx * 2 + yy) * 2 + cc) * rows_dev

    def rows_at(start, count):
        return pl.ds(pl.multiple_of(start, math.gcd(count, 128)), count)

    def columns_at(xx, h):
        return pl.ds(pl.multiple_of(xx * wide + h * cw, cw), cw)

    own_w, own_t = (up_ref, down_ref), (earlier_ref, cot_ref, later_ref)

    def load_w(m, h):
        return pltpu.make_async_copy(
            own_w[m].at[:, columns_at(x, h)], wts.at[m, h, rows_at(fs * blk, blk), :], l_s.at[m * chunks + h])

    def load_t(a):
        return pltpu.make_async_copy(
            own_t[a], tok.at[a, rows_at(block_at(x, y, c), rows_dev), :], l_s.at[2 * chunks + a])

    for m in range(2):
        load_w(m, 0).start()
    load_t(0).start()
    load_t(1).start()
    for m in range(2):
        load_w(m, 1).start()
    load_t(2).start()
    totals = tuple(
        pltpu.make_async_copy(total, sums.at[m], l_s.at[2 * chunks + 3 + m])
        for m, total in enumerate((up_total, down_total)))
    for m in range(2):
        totals[m].start()

    barrier = pltpu.get_barrier_semaphore()
    for other in (right, left, x_next, y_next, mate):
        pl.semaphore_signal(barrier, inc=1, device_id=other, device_id_type=MESH)
    pl.semaphore_wait(barrier, 5)

    def remote(src, dst, send, recv, to):
        return pltpu.make_async_remote_copy(
            src_ref=src, dst_ref=dst, send_sem=send, recv_sem=recv, device_id=to, device_id_type=MESH)

    def piece(m, h, f):
        return wts.at[m, h, rows_at(f * blk, blk), :]

    def wx_copy(m, h):
        return remote(own_w[m].at[:, columns_at(1 - x, h)], piece(m, h, fs), wx_s, w_r.at[m, h, fs], x_next)

    def wz_copy(m, h, f, way):
        return remote(piece(m, h, f), piece(m, h, f), wz_s.at[way, m, h], w_r.at[m, h, f], left if way else right)

    def w_got(m, h, f):
        wz_copy(m, h, f, 0).wait_recv()

    def spread(m, h, f):
        @pl.when(z < last)
        def _():
            wz_copy(m, h, f, 0).start()

        @pl.when(z > 0)
        def _():
            wz_copy(m, h, f, 1).start()

    def from_x(h, ms=(0, 1)):
        for m in ms:
            w_got(m, h, z * 2 + 1 - x)
            spread(m, h, z * 2 + 1 - x)

    def relay(h, d, columns=(0, 1), ms=(0, 1)):
        for m in ms:
            for p in columns:
                p = (x + p) % 2

                @pl.when((z >= d) & (z < last))
                def _():
                    w_got(m, h, (z - d) * 2 + p)
                    wz_copy(m, h, (z - d) * 2 + p, 0).start()

                @pl.when((z + d < z_size) & (z > 0))
                def _():
                    w_got(m, h, (z + d) * 2 + p)
                    wz_copy(m, h, (z + d) * 2 + p, 1).start()

    def settle(h, m, lo, hi):
        @pl.when((z == 0) | (z == last))
        def _():
            @pl.loop(lo, hi)
            def _(d):
                for p in range(2):
                    w_got(m, h, jnp.where(z == 0, d, last - d) * 2 + p)

    def moves(cut_t):
        return (
            (x, y, 0, rows_dev, x_next, 0),
            (x, y, 0, rows_dev, y_next, 1),
            (1 - x, y, 0, cut_t, y_next, 2),
            (x, 1 - y, cut_t, rows_dev - cut_t, x_next, 3),
            (x, y, 0, rows_dev, mate, 4),
            (1 - x, y, 0, rows_dev, mate, 4),
            (x, 1 - y, 0, rows_dev, mate, 4),
            (1 - x, 1 - y, 0, cut_t, mate, 5),
            (1 - x, 1 - y, cut_t, rows_dev - cut_t, mate, 5),
        )

    cuts = tuple(rows_dev * part // 4 // 16 * 16 for part in (3, 3, 2))

    def t_copy(a, k):
        xx, yy, lo, count, to, got = moves(cuts[a])[k]
        there = tok.at[a, rows_at(block_at(xx, yy, c) + lo, count), :]
        return remote(there, there, t_s.at[a], t_r.at[a, got], to)

    def t_first(a):
        load_t(a).wait()
        for k in (0, 1, 4):
            t_copy(a, k).start()

    def t_pass_y(a):
        t_copy(a, 1).wait_recv()
        t_copy(a, 3).start()
        t_copy(a, 6).start()

    def t_pass_x(a):
        t_copy(a, 0).wait_recv()
        t_copy(a, 2).start()
        t_copy(a, 5).start()

    def t_diagonal(a):
        t_copy(a, 2).wait_recv()
        t_copy(a, 7).start()
        t_copy(a, 3).wait_recv()
        t_copy(a, 8).start()

    def t_mate(a):
        there = tok.at[a, pl.ds(0, 3 * rows_dev), :]
        remote(there, there, t_s.at[a], t_r.at[a, 4], mate).wait_recv()

    def t_mate_diagonal(a):
        there = tok.at[a, pl.ds(0, rows_dev), :]
        remote(there, there, t_s.at[a], t_r.at[a, 5], mate).wait_recv()

    def chip_at(i):
        return (((x + i % 2) % 2) * 2 + (y + i // 2) % 2) * chip_rows

    def earlier_hidden(h, lo, hi):
        @pl.loop(lo, hi)
        def _(i):
            o = rows_at(chip_at(i), chip_rows)
            relu = jnp.maximum(jnp.dot(tok[0, o, :], wts[0, h], preferred_element_type=F32), 0.0)
            got = jnp.dot(tok[1, o, :], wts[1, h], preferred_element_type=F32)
            hid[0, h, o, :] = (2.0 * relu * got).astype(BF16)
            hid[1, h, o, :] = (relu * relu).astype(BF16)

    def later_hidden(h):
        @pl.loop(0, 4)
        def _(i):
            o = rows_at(i * chip_rows, chip_rows)
            relu = jnp.maximum(jnp.dot(tok[2, o, :], wts[0, h], preferred_element_type=F32), 0.0)
            hid[2, h, o, :] = (relu * relu).astype(BF16)

    def term(m, h, d):
        o = rows_at(d * zrows, zrows)
        grads[m, h, o, :] = lax.dot_general(
            tok[m, :, o], hid[m, h], (((0,), (0,)), ((), ())), preferred_element_type=F32).astype(BF16)

    def half_at(d, half):
        return d * zrows + (x + 1 - half) % 2 * blk

    def g_copy(m, h, d, way, half):
        src = grads.at[m, h, rows_at(half_at(d, half), blk), :]
        to = {"fs": ((z + z_size + 1 - 2 * way) % z_size) * 2 + x, "tp": tp}
        slot = d + 1 - way
        return remote(src, gbuf.at[m, h, slot, half], g_s.at[way, m, h], g_r.at[m, h, slot, half], to)

    def terms(h, lo, hi):
        @pl.loop(lo, hi)
        def _(k):
            @pl.when(last - k > z)
            def _():
                @pl.loop(0, 2)
                def _(m):
                    term(m, h, last - k)

                    @pl.when(z == 0)
                    def _():
                        for half in range(2):
                            g_copy(m, h, last - k, 0, half).start()

            @pl.when(k < z)
            def _():
                @pl.loop(0, 2)
                def _(m):
                    term(m, h, k)

                    @pl.when(z == last)
                    def _():
                        for half in range(2):
                            g_copy(m, h, k, 1, half).start()

    def own_terms(h):
        @pl.loop(0, 2)
        def _(m):
            term(m, h, z)

    def add_rows(dst, dst_row, src, count, columns=slice(None)):
        step = math.gcd(count, 32)

        @pl.loop(0, count // step)
        def _(i):
            o = pl.multiple_of(i * step, step)
            at = pl.ds(pl.multiple_of(dst_row + o, math.gcd(step, 16)), step)
            dst[at, columns] = (dst[at, columns].astype(F32) + src[pl.ds(o, step), columns].astype(F32)).astype(BF16)

    side = 2 * z // z_size

    def reduce_step(h, k, m, near):
        way = side if near else 1 - side
        d = (1 - way) * (last - k) + way * k
        beyond = (1 - 2 * way) * (d - z)
        behind = (1 - way) * z + way * (last - z)

        @pl.when((beyond > 0) & (behind > 0))
        def _():
            for half in range(2):
                g_copy(m, h, d, way, half).wait_recv()
                add_rows(grads.at[m, h], half_at(d, half), gbuf.at[m, h, d + 1 - way, half], blk)
                g_copy(m, h, d, way, half).start()

    outs = (up_out, down_out)

    def f_copy(m, h):
        return remote(fin.at[m, h], xbuf.at[m, h], f_s, f_r.at[m, h], x_next)

    def total(m, h, half, sources):
        step = math.gcd(blk, 32)

        @pl.loop(0, blk // step)
        def _(i):
            o = pl.multiple_of(i * step, step)
            at = pl.ds(o, step)
            got = grads[m, h, pl.ds(pl.multiple_of(half_at(z, half) + o, step), step), :].astype(F32)
            for src in sources:
                got += gbuf[m, h, z + 1 - src, half, at, :].astype(F32)
            if half:
                sums[m, at, columns_at(x, h)] += got * factor
            else:
                fin[m, h, at, :] = got.astype(BF16)

    def store_sum(m, h, xx):
        there = columns_at(xx, h)
        return pltpu.make_async_copy(sums.at[m, :, there], outs[m].at[:, there], o_s.at[m])

    def finish(h, m):
        for half in range(2):
            @pl.when(z > 0)
            def _():
                g_copy(m, h, z, 0, half).wait_recv()

            @pl.when(z < last)
            def _():
                g_copy(m, h, z, 1, half).wait_recv()

            for case, sources in ((z == 0, (1,)), (z == last, (0,)), ((z > 0) & (z < last), (0, 1))):
                @pl.when(case)
                def _():
                    total(m, h, half, sources)

            (store_sum(m, h, x) if half else f_copy(m, h)).start()

    def finish_x(h, m):
        f_copy(m, h).wait_recv()
        step = math.gcd(blk, 32)

        @pl.loop(0, blk // step)
        def _(i):
            at = pl.ds(pl.multiple_of(i * step, step), step)
            sums[m, at, columns_at(1 - x, h)] += xbuf[m, h, at, :].astype(F32) * factor

        store_sum(m, h, 1 - x).start()

    span = 2 * blk
    tile = math.gcd(span, 256)

    def span_at(i):
        return rows_at(((1 - side) * i + side * (last - i)) * span, span)

    def partial(a, k, w, i):
        first = ((1 - side) * i + side * (last - i)) * span

        @pl.loop(0, span // tile)
        def _(j):
            o = rows_at(first + j * tile, tile)
            got = None
            for h in range(chunks):
                one = lax.dot_general(hid[k, h], wts[w, h, o, :], (((1,), (1,)), ((), ())),
                                      preferred_element_type=F32)
                got = one if got is None else got + one
            part[a, :, o] = got.astype(BF16)

        for q in range(4):
            d_copy(a, q, i).start()

    def d_copy(a, q, i):
        return remote(part.at[a, rows_at(q * chip_rows + (1 - c) * rows_dev, rows_dev), span_at(i)],
                      dbuf.at[a, q, :, span_at(i)], d_s.at[a], d_r.at[a, i], mate)

    cut_q = rows_dev * 3 // 8 // 16 * 16
    low, high = (0, cut_q), (cut_q, rows_dev - cut_q)
    hops = (
        (1 - x, y, low, qa, 0, x_next),
        (1 - x, 1 - y, low, qa, 1, x_next),
        (x, 1 - y, high, qb, 0, y_next),
        (1 - x, 1 - y, high, qb, 1, y_next),
        (x, 1 - y, low, qa, 2, y_next),
        (1 - x, y, high, qb, 2, x_next),
    )

    def q_copy(a, k, i):
        xx, yy, (lo, count), buf, slot, to = hops[k]
        return remote(part.at[a, rows_at(block_at(xx, yy, c) + lo, count), span_at(i)],
                      buf.at[a, slot, :, span_at(i)], q_s.at[a], q_r.at[a, k // 2, i] if k in (1, 3) else q_l.at[a], to)

    def q_first(a, i):
        there = dbuf.at[a, :, :, span_at(i)]
        remote(there, there, d_s.at[a], d_r.at[a, i], mate).wait_recv()
        for q in range(4):
            add_rows(part.at[a], q * chip_rows + c * rows_dev, dbuf.at[a, q], rows_dev, span_at(i))
        for k in (1, 3):
            q_copy(a, k, i).start()

    def q_rest(a, i):
        for k in (0, 2):
            q_copy(a, k, i).start()

    def q_second(a, i):
        q_copy(a, 1, i).wait_recv()
        add_rows(part.at[a], block_at(x, 1 - y, c), qa.at[a, 1], cut_q, span_at(i))
        q_copy(a, 4, i).start()
        q_copy(a, 3, i).wait_recv()
        add_rows(part.at[a], block_at(1 - x, y, c) + cut_q, qb.at[a, 1], rows_dev - cut_q, span_at(i))
        q_copy(a, 5, i).start()

    def over(lo, hi, *calls):
        @pl.loop(lo, hi)
        def _(i):
            for call in calls:
                call(i)

    def store_out(a):
        return pltpu.make_async_copy(stage.at[a], (earlier_out, later_out)[a], o_s.at[2 + a])

    def q_last(a):
        there = part.at[a, pl.ds(0, 2 * rows_dev), :]
        remote(there, there, q_s.at[a], q_l.at[a], x_next).wait_recv()
        for (lo, count), buf in ((low, qa), (high, qb)):
            step = math.gcd(count, 16)

            @pl.loop(0, count // step)
            def _(i):
                o = pl.multiple_of(i * step, step)
                at = pl.ds(o, step)
                own = pl.ds(pl.multiple_of(block_at(x, y, c) + lo + o, step), step)
                stage[a, pl.ds(pl.multiple_of(lo + o, step), step), :] = (
                    part[a, own, :].astype(F32) + buf[a, 0, at, :].astype(F32) + buf[a, 2, at, :].astype(F32)
                ).astype(BF16)

        store_out(a).start()

    for m in range(2):
        wx_copy(m, 0).start()
    for m in range(2):
        load_w(m, 0).wait()
        spread(m, 0, fs)
    t_first(0)
    t_first(1)
    for m in range(2):
        wx_copy(m, 1).start()
    from_x(0)
    relay(0, 1)
    t_pass_y(0)
    t_pass_x(0)
    relay(0, 2)
    t_pass_y(1)
    t_pass_x(1)
    for m in range(2):
        load_w(m, 1).wait()
        spread(m, 1, fs)
    t_first(2)
    for m in range(2):
        settle(0, m, 1, z_size)
    for a in range(2):
        t_mate(a)
    earlier_hidden(0, 0, 3)
    from_x(1)
    t_diagonal(0)
    relay(1, 1, (0,))
    t_diagonal(1)
    for a in range(2):
        t_mate_diagonal(a)
    earlier_hidden(0, 3, 4)
    terms(0, 0, last)
    own_terms(0)
    relay(1, 1, (1,), (0,))
    relay(1, 2, (0,), (0,))
    t_pass_y(2)
    reduce_step(0, 0, 0, True)
    relay(1, 2, (1,), (0,))
    relay(1, 1, (1,), (1,))
    relay(1, 2, (0,), (1,))
    t_pass_x(2)
    reduce_step(0, 0, 1, True)
    relay(1, 2, (1,), (1,))
    reduce_step(0, 0, 0, False)
    t_diagonal(2)
    settle(1, 0, 1, z_size)
    t_mate(2)
    t_mate_diagonal(2)
    later_hidden(0)
    later_hidden(1)
    reduce_step(0, 1, 0, True)
    reduce_step(0, 0, 1, False)
    settle(1, 1, 1, last)
    over(0, last, lambda i: partial(1, 2, 1, i))
    settle(1, 1, last, z_size)
    partial(1, 2, 1, last)
    over(0, last, lambda i: q_first(1, i))
    earlier_hidden(1, 0, 4)
    reduce_step(0, 1, 1, True)
    terms(1, 0, 1)
    q_first(1, last)
    over(0, z_size, lambda i: q_rest(1, i))
    terms(1, 1, last)
    own_terms(1)
    partial(0, 0, 0, 0)
    over(1, z_size, lambda i: partial(0, 0, 0, i), lambda i: q_first(0, i - 1))
    for m in range(2):
        totals[m].wait()
        finish(0, m)
    q_first(0, last)
    over(0, z_size, lambda i: q_second(1, i))
    over(0, z_size, lambda i: q_rest(0, i))
    reduce_step(1, 0, 0, True)
    reduce_step(1, 0, 1, True)
    reduce_step(1, 0, 0, False)
    over(0, z_size, lambda i: q_second(0, i))
    finish_x(0, 0)
    finish_x(0, 1)
    reduce_step(1, 1, 0, True)
    reduce_step(1, 0, 1, False)
    reduce_step(1, 1, 1, True)
    finish(1, 0)
    q_last(1)
    finish(1, 1)
    q_last(0)
    finish_x(1, 0)
    finish_x(1, 1)

    def sent(ref, semaphore):
        remote(ref, ref, semaphore, f_r.at[0, 0], mate).wait_send()

    four = wts.at[0, 0, pl.ds(0, 2 * chunks * blk), :]
    sent(four, wx_s)
    sent(four, f_s)
    for m in range(2):
        pltpu.make_async_copy(outs[m], outs[m], o_s.at[m]).wait()
        for h in range(chunks):
            for way in range(2):
                for hops_left in range(1, z_size):
                    @pl.when((last - z if way == 0 else z) == hops_left)
                    def _():
                        sent(wts.at[m, h, pl.ds(0, (z_size - hops_left) * zrows), :], wz_s.at[way, m, h])
                        sent(grads.at[m, h, pl.ds(0, hops_left * zrows), :], g_s.at[way, m, h])
    for a in range(3):
        sent(tok.at[a, pl.ds(0, 7 * rows_dev), :], t_s.at[a])
    for a in range(2):
        store_out(a).wait()
        sent(part.at[a, pl.ds(0, 4 * rows_dev), :], d_s.at[a])
        sent(part.at[a, pl.ds(0, 3 * rows_dev), :], q_s.at[a])


def plane_call(n, factor, *args):
    rows_dev, depth = args[0].shape
    blk, width = args[3].shape
    z_size, chunks, rows = n // 2, 2, rows_dev * 8
    cw = width // 2 // chunks
    cut_q = rows_dev * 3 // 8 // 16 * 16
    dma = pltpu.SemaphoreType.DMA
    hbm = pl.BlockSpec(memory_space=pltpu.HBM)
    return pl.pallas_call(
        functools.partial(plane_kernel, n, chunks, factor),
        out_shape=(
            jax.ShapeDtypeStruct((rows_dev, depth), BF16),
            jax.ShapeDtypeStruct((rows_dev, depth), BF16),
            jax.ShapeDtypeStruct((blk, width), F32),
            jax.ShapeDtypeStruct((blk, width), F32),
        ),
        in_specs=[hbm] * 7,
        out_specs=(hbm,) * 4,
        scratch_shapes=[
            pltpu.VMEM((3, rows, depth), BF16),
            pltpu.VMEM((2, chunks, depth, cw), BF16),
            pltpu.VMEM((3, chunks, rows, cw), BF16),
            pltpu.VMEM((2, chunks, depth, cw), BF16),
            pltpu.VMEM((2, chunks, z_size + 1, 2, blk, cw), BF16),
            pltpu.VMEM((2, chunks, blk, cw), BF16),
            pltpu.VMEM((2, chunks, blk, cw), BF16),
            pltpu.VMEM((2, rows, depth), BF16),
            pltpu.VMEM((2, 4, rows_dev, depth), BF16),
            pltpu.VMEM((2, 3, cut_q, depth), BF16),
            pltpu.VMEM((2, 3, rows_dev - cut_q, depth), BF16),
            pltpu.VMEM((2, rows_dev, depth), BF16),
            pltpu.VMEM((2, blk, width), F32),
            dma((2 * chunks + 5,)), dma((4,)), dma((3,)), dma((3, 6)), dma, dma((2, 2, chunks)), dma((2, chunks, n)),
            dma((2, 2, chunks)), dma((2, chunks, z_size + 1, 2)), dma, dma((2, chunks)),
            dma((2,)), dma((2, z_size)), dma((2,)), dma((2, 2, z_size)), dma((2,)),
        ],
        compiler_params=pltpu.CompilerParams(
            collective_id=0, has_side_effects=True, vmem_limit_bytes=67043328
        ),
        name="feed_forward_planes",
    )(*args)


def hand_on_kernel(*refs):
    count = (len(refs) - 2) // 3
    ins, outs, held, in_s, out_s = refs[:count], refs[count:2 * count], refs[2 * count:-2], refs[-2], refs[-1]
    loads, stores = [], []
    for a, (src, kept, dst) in enumerate(zip(ins, held, outs)):
        half = src.shape[0] // 2
        for i in range(2):
            o = pl.ds(i * half, half)
            loads.append(pltpu.make_async_copy(src.at[o, :], kept.at[o, :], in_s.at[a, i]))
            stores.append(pltpu.make_async_copy(kept.at[o, :], dst.at[o, :], out_s.at[a, i]))
    for load in loads:
        load.start()
    for load, store in zip(loads, stores):
        load.wait()
        store.start()
    for store in stores:
        store.wait()


def hand_on(*arrays):
    count = len(arrays)
    hbm = pl.BlockSpec(memory_space=pltpu.HBM)
    return pl.pallas_call(
        hand_on_kernel,
        out_shape=tuple(jax.ShapeDtypeStruct(a.shape, a.dtype) for a in arrays),
        in_specs=[hbm] * count,
        out_specs=(hbm,) * count,
        scratch_shapes=[*(pltpu.VMEM(a.shape, a.dtype) for a in arrays),
                        pltpu.SemaphoreType.DMA((count, 2)), pltpu.SemaphoreType.DMA((count, 2))],
        compiler_params=pltpu.CompilerParams(vmem_limit_bytes=67043328),
        name="feed_forward_results",
    )(*arrays)


def ring_call(n, m, *args):
    rows_dev, depth = args[0].shape
    blk, width = args[3].shape
    rows, half, y_size = rows_dev * m, n // 2, m // 2
    dma = pltpu.SemaphoreType.DMA
    vmem = pl.BlockSpec(memory_space=pltpu.VMEM)
    sums = max(y_size - 1, 1)
    parts = 2 if width % 256 == 0 else 1
    return pl.pallas_call(
        functools.partial(kernel, n, m, parts),
        out_shape=(
            jax.ShapeDtypeStruct((rows_dev, depth), BF16),
            jax.ShapeDtypeStruct((rows_dev, depth), BF16),
            jax.ShapeDtypeStruct((blk, width), BF16),
            jax.ShapeDtypeStruct((blk, width), BF16),
        ),
        in_specs=[vmem] * 5,
        out_specs=(vmem,) * 4,
        scratch_shapes=[
            pltpu.VMEM((3, rows, depth), BF16),
            pltpu.VMEM((2, depth, width), BF16),
            pltpu.VMEM((3, rows, width), F32),
            pltpu.VMEM((3, rows, width), BF16),
            pltpu.VMEM((2, depth, width), BF16),
            pltpu.VMEM((4, half, blk, width), BF16),
            pltpu.VMEM((2, rows, depth), BF16),
            pltpu.VMEM((2, y_size, rows_dev, depth), BF16),
            pltpu.VMEM((2, sums, rows_dev, depth), BF16),
            dma((3, y_size)), dma((3, y_size)), dma((3, y_size)), dma((3, y_size)),
            *[dma((4, half, parts))] * 4,
            dma((2, y_size)), dma((2, y_size)), dma((2, sums)), dma((2, sums)),
        ],
        compiler_params=pltpu.CompilerParams(
            collective_id=0, has_side_effects=True, vmem_limit_bytes=67043328
        ),
        name="feed_forward_step",
    )(*args)


def body(n, m, later_rows, earlier_rows, cotangent, up_weight, down_weight, up_total, down_total):
    rows = later_rows.shape[0] * m
    factor = 1.0 / math.sqrt(rows * n)
    width = up_weight.shape[1]
    planar = columns_of(n) == 2 and n == 8 and m == 4 and width % 1024 == 0 and rows % 512 == 0
    planes = (later_rows, earlier_rows, cotangent, up_weight, down_weight)
    if planar:
        return tuple(hand_on(*plane_call(n, factor, *planes, up_total, down_total)))
    later_out, earlier_grad, up_term, down_term = ring_call(n, m, *planes)
    up_updated = up_total + up_term.astype(F32) * factor
    down_updated = down_total + down_term.astype(F32) * factor
    return later_out, earlier_grad, up_updated, down_updated


def solution(mesh):
    return jax.shard_map(
        functools.partial(body, mesh.shape["fs"], mesh.shape["tp"]),
        mesh=mesh,
        in_specs=(
            P(("fs", "tp"), None),
            P(("fs", "tp"), None),
            P(("fs", "tp"), None),
            P("fs", "tp"),
            P("fs", "tp"),
            P("fs", "tp"),
            P("fs", "tp"),
        ),
        out_specs=(P(("fs", "tp"), None), P(("fs", "tp"), None), P("fs", "tp"), P("fs", "tp")),
        check_vma=False,
    )
```

```python
import functools
import math

import jax
import jax.numpy as jnp
from jax import lax
from jax.experimental import pallas as pl
from jax.experimental.pallas import tpu as pltpu
from jax.sharding import PartitionSpec as P

MESH = pl.DeviceIdType.MESH
BF16 = jnp.bfloat16
F32 = jnp.float32


def columns_of(n):
    best = 1
    for x in range(1, n + 1):
        if n % x == 0 and 2 * x * x <= n and (n // x) % 2 == 0:
            best = x
    return best


def ring_to_fs(p, n, x_size):
    if x_size == 1:
        return p
    z_size, wide = n // x_size, x_size - 1
    body = z_size * wide
    z, r = p // wide, p % wide
    x = 1 + jnp.where(z % 2 == 0, r, wide - 1 - r)
    back = z_size - 1 - (p - body)
    return jnp.where(p < body, z * x_size + x, back * x_size)


def fs_to_ring(f, n, x_size):
    if x_size == 1:
        return f
    z_size, wide = n // x_size, x_size - 1
    z, x = f // x_size, f % x_size
    r = jnp.where(z % 2 == 0, x - 1, x_size - 1 - x)
    return jnp.where(x == 0, z_size * wide + z_size - 1 - z, z * wide + r)


def kernel(n, m, parts,
           later_ref, earlier_ref, cot_ref, up_ref, down_ref,
           later_out, earlier_out, up_out, down_out,
           tok, wts, acc, hid, grads, rbuf, part, dbuf, ybuf,
           ty_s, ty_r, td_s, td_r, w_s, w_r, g_s, g_r, od_s, od_r, oy_s, oy_r):
    rows_dev, depth = later_ref.shape
    blk, width = up_ref.shape
    rows = rows_dev * m
    half, y_size = n // 2, m // 2
    aligned = blk % 128 == 0
    wide_q = width // parts
    fs, tp = lax.axis_index("fs"), lax.axis_index("tp")
    x_size = columns_of(n)
    pos = fs_to_ring(fs, n, x_size)
    y, c = tp // 2, tp % 2

    def at_ring(p):
        return ring_to_fs((p + 2 * n) % n, n, x_size)

    right = {"fs": at_ring(pos + 1), "tp": tp}
    left = {"fs": at_ring(pos - 1), "tp": tp}
    mate = {"fs": fs, "tp": y * 2 + 1 - c}
    y_next = {"fs": fs, "tp": ((y + 1) % y_size) * 2 + c}
    y_prev = {"fs": fs, "tp": ((y + y_size - 1) % y_size) * 2 + c}

    barrier = pltpu.get_barrier_semaphore()
    for other in (right, left, mate, y_next, y_prev):
        pl.semaphore_signal(barrier, inc=1, device_id=other, device_id_type=MESH)
    pl.semaphore_wait(barrier, 5)

    def remote(src, dst, send, recv, to):
        return pltpu.make_async_remote_copy(
            src_ref=src, dst_ref=dst, send_sem=send, recv_sem=recv, device_id=to, device_id_type=MESH)

    def trows(a, t):
        return tok.at[a, pl.ds(pl.multiple_of(t * rows_dev, rows_dev), rows_dev), :]

    own_w, own_t = (up_ref, down_ref), (earlier_ref, cot_ref, later_ref)

    arr_of, sign_of = (0, 1, 1, 0), (1, -1, 1, -1)

    def cut(q):
        return pl.ds(q * wide_q, wide_q)

    def w_copy(k, s, q, first=False):
        f = at_ring(pos - sign_of[k] * s)
        there = wts.at[arr_of[k], pl.ds(pl.multiple_of(f * blk, blk), blk), cut(q)]
        src = own_w[arr_of[k]].at[:, cut(q)] if first else there
        return remote(src, there, w_s.at[k, s, q], w_r.at[k, s, q], right if sign_of[k] > 0 else left)

    def ty_copy(a, s, first=False):
        t = ((y + y_size - s) % y_size) * 2 + c
        return remote(own_t[a] if first else trows(a, t), trows(a, t), ty_s.at[a, s], ty_r.at[a, s], y_next)

    def td_copy(a, s, first=False):
        t = ((y + y_size - s) % y_size) * 2 + c
        return remote(own_t[a] if first else trows(a, t), trows(a, t), td_s.at[a, s], td_r.at[a, s], mate)

    every = tuple((k, q) for pair in ((0, 1), (2, 3)) for q in range(parts) for k in pair)
    longs = tuple((k, q) for k, q in every if k < 2)
    for k, q in every:
        w_copy(k, 0, q, True).start()
    for a in range(3):
        if y_size > 1:
            ty_copy(a, 0, True).start()
    for a in range(3):
        td_copy(a, 0, True).start()

    def put(dst, dst_row, src, count):
        step = math.gcd(count, 64)

        @pl.loop(0, count // step)
        def _(i):
            o = pl.multiple_of(i * step, step)
            dst[pl.ds(pl.multiple_of(dst_row + o, step), step), :] = src[pl.ds(o, step), :]

    for a in range(2):
        put(wts.at[a], fs * blk, own_w[a], blk)
    for a in range(3):
        put(tok.at[a], tp * rows_dev, own_t[a], rows_dev)

    tile = math.gcd(wide_q, 256)

    def multiply(a, w, rows_w, clear, q=None):
        first, count = (0, width) if q is None else (q * wide_q, wide_q)

        @pl.loop(0, count // tile)
        def _(j):
            o = pl.ds(pl.multiple_of(first + j * tile, tile), tile)
            got = jnp.dot(tok[a, :, rows_w], wts[w, rows_w, o], preferred_element_type=F32)
            if clear:
                acc[a, :, o] = got
            else:
                acc[a, :, o] += got

    def use(w, f, clear=False, q=None):
        if not aligned:
            return
        o = pl.ds(pl.multiple_of(f * blk, blk), blk)
        for a in ((0, 2) if w == 0 else (1,)):
            multiply(a, w, o, clear, q)

    def forward(s, present, go):
        for k, q in present:
            w_copy(k, s - 1, q).wait_recv()
            if (k, q) in go:
                w_copy(k, s, q).start()

    def use_step(s):
        for k in range(4):
            use(arr_of[k], at_ring(pos - sign_of[k] * s))

    forward(1, every, every if half > 2 else longs)
    for s in range(1, y_size):
        for a in range(3):
            ty_copy(a, s - 1).wait_recv()
            if s < y_size - 1:
                ty_copy(a, s).start()
            td_copy(a, s).start()
    for s in range(y_size):
        for a in range(3):
            td_copy(a, s).wait_recv()
    for w in range(2):
        use(w, fs, True)
    if half > 3:
        @pl.loop(2, half - 1)
        def _(s):
            forward(s, every, every)
            use_step(s - 1)
    if half > 2:
        forward(half - 1, every, longs)
        use_step(half - 2)
    use_step(half - 1)

    step_r = math.gcd(rows, 32)

    def activate(q):
        @pl.loop(0, rows // step_r)
        def _(i):
            o = pl.ds(pl.multiple_of(i * step_r, step_r), step_r)
            relu = jnp.maximum(acc[0, o, cut(q)], 0.0)
            hid[0, o, cut(q)] = (2.0 * relu * acc[1, o, cut(q)]).astype(BF16)
            hid[1, o, cut(q)] = (relu * relu).astype(BF16)

    def term(a, row, size, q=None):
        first, count = (0, width) if q is None else (q * wide_q, wide_q)

        @pl.loop(0, count // tile)
        def _(j):
            o = pl.ds(pl.multiple_of(first + j * tile, tile), tile)
            grads[a, pl.ds(row, size), o] = lax.dot_general(
                tok[a, :, pl.ds(row, size)], hid[a, :, o], (((0,), (0,)), ((), ())),
                preferred_element_type=F32).astype(BF16)

    def block_term(a, p, q=None):
        term(a, pl.multiple_of(at_ring(p) * blk, blk), blk, q)

    def g_copy(k, s, q):
        d = half - (k >= 2) - s
        f = at_ring(pos + sign_of[k] * d)
        src = grads.at[arr_of[k], pl.ds(pl.multiple_of(f * blk, blk), blk), cut(q)]
        return remote(src, rbuf.at[k, s, :, cut(q)], g_s.at[k, s, q], g_r.at[k, s, q],
                      right if sign_of[k] > 0 else left)

    def add_rows(dst, dst_row, src, count, columns=slice(None)):
        step = math.gcd(count, 32)

        @pl.loop(0, count // step)
        def _(i):
            o = pl.multiple_of(i * step, step)
            at = pl.ds(pl.multiple_of(dst_row + o, step), step)
            total = dst[at, columns].astype(F32) + src[pl.ds(o, step), columns].astype(F32)
            dst[at, columns] = total.astype(BF16)

    def g_step(s, which):
        for k, q in which:
            g_copy(k, s - 1, q).wait_recv()
            f = at_ring(pos + sign_of[k] * (half - (k >= 2) - s))
            add_rows(grads.at[arr_of[k]], f * blk, rbuf.at[k, s - 1], blk, cut(q))
            g_copy(k, s, q).start()

    wide = math.gcd(depth, 256)
    for q in range(parts):
        for k in (0, 1):
            w_copy(k, half - 1, q).wait_recv()
            use(arr_of[k], at_ring(pos - sign_of[k] * half), q=q)
        if not aligned:
            full = pl.ds(0, depth)
            for a, w in ((0, 0), (1, 1), (2, 0)):
                multiply(a, w, full, True, q)
        activate(q)
        if not aligned:
            for a in range(2):
                @pl.loop(0, depth // wide)
                def _(i):
                    term(a, pl.multiple_of(i * wide, wide), wide, q)
        for k in (0, 1):
            if aligned:
                block_term(arr_of[k], pos + sign_of[k] * half, q)
            g_copy(k, 0, q).start()
    for k in (2, 3):
        if aligned:
            block_term(arr_of[k], pos + sign_of[k] * (half - 1))
        for q in range(parts):
            g_copy(k, 0, q).start()
    if aligned:
        if half > 1:
            @pl.loop(0, half - 1)
            def _(i):
                d = half - 1 - i
                block_term(0, pos + d)
                block_term(1, pos - d)
        if half > 2:
            @pl.loop(0, half - 2)
            def _(i):
                d = half - 2 - i
                block_term(1, pos + d)
                block_term(0, pos - d)
        for a in range(2):
            block_term(a, pos)

    @pl.loop(0, rows // step_r)
    def _(i):
        o = pl.ds(pl.multiple_of(i * step_r, step_r), step_r)
        relu = jnp.maximum(acc[2, o, :], 0.0)
        hid[2, o, :] = (relu * relu).astype(BF16)

    wide_d = math.gcd(depth, 256)

    def partial(a, h, w):
        @pl.loop(0, depth // wide_d)
        def _(j):
            o = pl.ds(pl.multiple_of(j * wide_d, wide_d), wide_d)
            part[a, :, o] = lax.dot_general(
                hid[h], wts[w, o, :], (((1,), (1,)), ((), ())), preferred_element_type=F32).astype(BF16)

    def prow(yy, cc):
        return pl.multiple_of((yy * 2 + cc) * rows_dev, rows_dev)

    def od_copy(a, yy):
        return remote(part.at[a, pl.ds(prow(yy, 1 - c), rows_dev), :], dbuf.at[a, yy],
                      od_s.at[a, yy], od_r.at[a, yy], mate)

    def oy_copy(a, s):
        t = (y + y_size - 1 - s) % y_size
        return remote(part.at[a, pl.ds(prow(t, c), rows_dev), :], ybuf.at[a, s],
                      oy_s.at[a, s], oy_r.at[a, s], y_next)

    def send_partial(a, h, w):
        partial(a, h, w)
        for yy in range(y_size):
            od_copy(a, yy).start()

    send_partial(0, 0, 0)
    g_step(1, every if half > 2 else longs)
    send_partial(1, 2, 1)
    for a in range(2):
        for yy in range(y_size):
            od_copy(a, yy).wait_recv()
            add_rows(part.at[a], prow(yy, c), dbuf.at[a, yy], rows_dev)
        if y_size > 1:
            oy_copy(a, 0).start()
    if half - 1 > 2:
        @pl.loop(2, half - 1)
        def _(s):
            g_step(s, every)
    for s in range(1, y_size):
        for a in range(2):
            oy_copy(a, s - 1).wait_recv()
            t = (y + y_size - 1 - s) % y_size
            add_rows(part.at[a], prow(t, c), ybuf.at[a, s - 1], rows_dev)
            if s < y_size - 1:
                oy_copy(a, s).start()
    put_own = ((earlier_out, 0), (later_out, 1))
    for out, a in put_own:
        out[...] = part[a, pl.ds(prow(y, c), rows_dev), :]
    if half - 1 >= 2:
        g_step(half - 1, longs)

    ends = [(k, half - 1 - (k >= 2)) for k in range(4)]
    for k, q in tuple((k, q) for k, q in every if k >= 2) + longs:
        g_copy(k, ends[k][1], q).wait_recv()
    step_b = math.gcd(blk, 32)
    for a, out in ((0, up_out), (1, down_out)):
        @pl.loop(0, blk // step_b)
        def _(i):
            lo = pl.multiple_of(i * step_b, step_b)
            o = pl.ds(lo, step_b)
            got = grads[a, pl.ds(pl.multiple_of(fs * blk + lo, step_b), step_b), :].astype(F32)
            for k, s in ends:
                if arr_of[k] == a:
                    got += rbuf[k, s, o, :].astype(F32)
            out[o, :] = got.astype(BF16)

    for k, q in every:
        for s in range(half - (k >= 2)):
            w_copy(k, s, q).wait_send()
            g_copy(k, s, q).wait_send()
    for a in range(3):
        for s in range(y_size):
            if s < y_size - 1:
                ty_copy(a, s).wait_send()
            td_copy(a, s).wait_send()
    for a in range(2):
        for yy in range(y_size):
            od_copy(a, yy).wait_send()
        for s in range(y_size - 1):
            oy_copy(a, s).wait_send()


def plane_kernel(n, chunks, factor,
                 later_ref, earlier_ref, cot_ref, up_ref, down_ref, up_total, down_total,
                 later_out, earlier_out, up_out, down_out,
                 tok, wts, act, hid, grads, gbuf, fin, xbuf, part, dbuf, qa, qb, stage, sums,
                 l_s, o_s, t_s, t_r, wx_s, wz_s, w_r, g_s, g_r, f_s, f_r, d_s, d_r, q_s, q_r, q_l):
    rows_dev, depth = later_ref.shape
    blk, width = up_ref.shape
    z_size, zrows = n // 2, 2 * blk
    wide, cw = width // 2, width // 2 // chunks
    chip_rows = 2 * rows_dev
    fs, tp = lax.axis_index("fs"), lax.axis_index("tp")
    z, x, y, c = fs // 2, fs % 2, tp // 2, tp % 2
    last = z_size - 1
    side = 2 * z // z_size
    span = 2 * blk

    right = {"fs": ((z + 1) % z_size) * 2 + x, "tp": tp}
    left = {"fs": ((z + last) % z_size) * 2 + x, "tp": tp}
    x_next = {"fs": z * 2 + 1 - x, "tp": tp}
    y_next = {"fs": fs, "tp": (1 - y) * 2 + c}
    mate = {"fs": fs, "tp": y * 2 + 1 - c}

    def block_at(xx, yy, cc):
        return ((xx * 2 + yy) * 2 + cc) * rows_dev

    def rows_at(start, count):
        return pl.ds(pl.multiple_of(start, math.gcd(count, 128)), count)

    def columns_at(xx, h):
        return pl.ds(pl.multiple_of(xx * wide + h * cw, cw), cw)

    own_w, own_t = (up_ref, down_ref), (earlier_ref, cot_ref, later_ref)

    def load_w(m, h):
        return pltpu.make_async_copy(
            own_w[m].at[:, columns_at(x, h)], wts.at[m, h, rows_at(fs * blk, blk), :], l_s.at[m * chunks + h])

    def load_t(a):
        return pltpu.make_async_copy(
            own_t[a], tok.at[a, rows_at(block_at(x, y, c), rows_dev), :], l_s.at[2 * chunks + a])

    for m in range(2):
        load_w(m, 0).start()
    load_t(0).start()
    load_t(1).start()
    for m in range(2):
        load_w(m, 1).start()
    load_t(2).start()
    totals = tuple(
        pltpu.make_async_copy(total, sums.at[m], l_s.at[2 * chunks + 3 + m])
        for m, total in enumerate((up_total, down_total)))
    for m in range(2):
        totals[m].start()

    barrier = pltpu.get_barrier_semaphore()
    for other in (right, left, x_next, y_next, mate):
        pl.semaphore_signal(barrier, inc=1, device_id=other, device_id_type=MESH)
    pl.semaphore_wait(barrier, 5)

    def remote(src, dst, send, recv, to):
        return pltpu.make_async_remote_copy(
            src_ref=src, dst_ref=dst, send_sem=send, recv_sem=recv, device_id=to, device_id_type=MESH)

    def piece(m, h, f):
        return wts.at[m, h, rows_at(f * blk, blk), :]

    def wx_copy(m, h):
        return remote(own_w[m].at[:, columns_at(1 - x, h)], piece(m, h, fs), wx_s, w_r.at[m, h, fs], x_next)

    def wz_copy(m, h, f, way):
        return remote(piece(m, h, f), piece(m, h, f), wz_s.at[way, m, h], w_r.at[m, h, f], left if way else right)

    def w_got(m, h, f):
        wz_copy(m, h, f, 0).wait_recv()

    def spread(m, h, f):
        @pl.when(z < last)
        def _():
            wz_copy(m, h, f, 0).start()

        @pl.when(z > 0)
        def _():
            wz_copy(m, h, f, 1).start()

    def spread_at(m, h, f, ends):
        @pl.when((z == 0) | (z == last) if ends else (z > 0) & (z < last))
        def _():
            spread(m, h, f)

    def from_x(h, ms=(0, 1)):
        for m in ms:
            w_got(m, h, z * 2 + 1 - x)
            spread(m, h, z * 2 + 1 - x)

    def from_x_at(h, ms, ends):
        @pl.when((z == 0) | (z == last) if ends else (z > 0) & (z < last))
        def _():
            from_x(h, ms)

    def relay(h, d, columns=(0, 1), ms=(0, 1)):
        for m in ms:
            for p in columns:
                p = (x + p) % 2

                @pl.when((z >= d) & (z < last))
                def _():
                    w_got(m, h, (z - d) * 2 + p)
                    wz_copy(m, h, (z - d) * 2 + p, 0).start()

                @pl.when((z + d < z_size) & (z > 0))
                def _():
                    w_got(m, h, (z + d) * 2 + p)
                    wz_copy(m, h, (z + d) * 2 + p, 1).start()

    def settle(h, m, lo, hi):
        @pl.when((z == 0) | (z == last))
        def _():
            @pl.loop(lo, hi)
            def _(d):
                for p in range(2):
                    w_got(m, h, jnp.where(z == 0, d, last - d) * 2 + p)

    def moves(cut_t):
        return (
            (x, y, 0, rows_dev, x_next, 0),
            (x, y, 0, rows_dev, y_next, 1),
            (1 - x, y, 0, cut_t, y_next, 2),
            (x, 1 - y, cut_t, rows_dev - cut_t, x_next, 3),
            (x, y, 0, rows_dev, mate, 4),
            (1 - x, y, 0, rows_dev, mate, 4),
            (x, 1 - y, 0, rows_dev, mate, 4),
            (1 - x, 1 - y, 0, cut_t, mate, 5),
            (1 - x, 1 - y, cut_t, rows_dev - cut_t, mate, 5),
        )

    cuts = tuple(rows_dev * part // 8 // 16 * 16 for part in (7, 5, 4))

    def facing(i):
        return (1 - side) * (last - i) + side * i

    def t_ref(a, start, count, u):
        columns = slice(None) if u is None else rows_at(facing(u) * span, span)
        return tok.at[a, rows_at(start, count), columns]

    def t_got(a, k, u):
        if a == 2:
            return t_r.at[moves(0)[k][-1]]
        return t_r.at[6 + (a * 5 + min(k, 4)) * z_size + (0 if a == 0 and k > 3 else u)]

    def t_copy(a, k, u=None):
        xx, yy, lo, count, to, _ = moves(cuts[a])[k]
        there = t_ref(a, block_at(xx, yy, c) + lo, count, u)
        return remote(there, there, t_s.at[a], t_got(a, k, u), to)

    def t_own(a, u=None):
        for k in (0, 1, 4):
            t_copy(a, k, u).start()

    def t_pass(a, u=None):
        t_copy(a, 1, u).wait_recv()
        t_copy(a, 3, u).start()
        t_copy(a, 6, u).start()
        t_copy(a, 0, u).wait_recv()
        t_copy(a, 2, u).start()
        t_copy(a, 5, u).start()

    def t_diagonal(a, u=None):
        t_copy(a, 2, u).wait_recv()
        t_copy(a, 7, u).start()
        t_copy(a, 3, u).wait_recv()
        t_copy(a, 8, u).start()

    def t_mate(a, u=None):
        there = t_ref(a, 0, 4 * rows_dev, u)
        remote(there, there, t_s.at[a], t_got(a, 4, u), mate).wait_recv()

    def t_mate_blocks():
        there = t_ref(2, 0, 3 * rows_dev, None)
        remote(there, there, t_s.at[2], t_r.at[4], mate).wait_recv()

    def t_mate_diagonal():
        there = t_ref(2, 0, rows_dev, None)
        remote(there, there, t_s.at[2], t_r.at[5], mate).wait_recv()

    def earlier_hidden(h):
        @pl.loop(0, 4)
        def _(i):
            o = rows_at(i * chip_rows, chip_rows)
            relu = jnp.maximum(jnp.dot(tok[0, o, :], wts[0, h], preferred_element_type=F32), 0.0)
            act[o, :] = relu
            hid[1, h, o, :] = (relu * relu).astype(BF16)

    def earlier_pre_grad(h):
        @pl.loop(0, 4)
        def _(i):
            o = rows_at(i * chip_rows, chip_rows)
            got = jnp.dot(tok[1, o, :], wts[1, h], preferred_element_type=F32)
            hid[0, h, o, :] = (2.0 * act[o, :] * got).astype(BF16)

    def chip_at(i):
        return (((x + i % 2) % 2) * 2 + (y + i // 2) % 2) * chip_rows

    def later_hidden(h, lo, hi):
        @pl.loop(lo, hi)
        def _(i):
            o = rows_at(chip_at(i), chip_rows)
            relu = jnp.maximum(jnp.dot(tok[2, o, :], wts[0, h], preferred_element_type=F32), 0.0)
            hid[2, h, o, :] = (relu * relu).astype(BF16)

    def term(m, h, d):
        o = rows_at(d * zrows, zrows)
        grads[m, h, o, :] = lax.dot_general(
            tok[m, :, o], hid[m, h], (((0,), (0,)), ((), ())), preferred_element_type=F32).astype(BF16)

    def half_at(d, half):
        return d * zrows + (x + 1 - half) % 2 * blk

    def g_copy(m, h, d, way, half):
        src = grads.at[m, h, rows_at(half_at(d, half), blk), :]
        to = {"fs": ((z + z_size + 1 - 2 * way) % z_size) * 2 + x, "tp": tp}
        slot = d + 1 - way
        return remote(src, gbuf.at[m, h, slot, half], g_s.at[way, m, h], g_r.at[m, h, slot, half], to)

    def term_step(m, h, i):
        d = facing(i)
        term(m, h, d)

        @pl.when(((z == 0) | (z == last)) & (i < last))
        def _():
            for half in range(2):
                g_copy(m, h, d, side, half).start()

    def add_rows(dst, dst_row, src, count, columns=slice(None)):
        step = math.gcd(count, 32)

        @pl.loop(0, count // step)
        def _(i):
            o = pl.multiple_of(i * step, step)
            at = pl.ds(pl.multiple_of(dst_row + o, math.gcd(step, 16)), step)
            dst[at, columns] = (dst[at, columns].astype(F32) + src[pl.ds(o, step), columns].astype(F32)).astype(BF16)

    def reduce_step(h, k, m, near):
        way = side if near else 1 - side
        d = (1 - way) * (last - k) + way * k
        beyond = (1 - 2 * way) * (d - z)
        behind = (1 - way) * z + way * (last - z)

        @pl.when((beyond > 0) & (behind > 0))
        def _():
            for half in range(2):
                g_copy(m, h, d, way, half).wait_recv()
                add_rows(grads.at[m, h], half_at(d, half), gbuf.at[m, h, d + 1 - way, half], blk)
                g_copy(m, h, d, way, half).start()

    outs = (up_out, down_out)

    def f_copy(m, h):
        return remote(fin.at[m, h], xbuf.at[m, h], f_s, f_r.at[m, h], x_next)

    def total(m, h, half, sources):
        step = math.gcd(blk, 32)

        @pl.loop(0, blk // step)
        def _(i):
            o = pl.multiple_of(i * step, step)
            at = pl.ds(o, step)
            got = grads[m, h, pl.ds(pl.multiple_of(half_at(z, half) + o, step), step), :].astype(F32)
            for src in sources:
                got += gbuf[m, h, z + 1 - src, half, at, :].astype(F32)
            if half:
                sums[m, at, columns_at(x, h)] += got * factor
            else:
                fin[m, h, at, :] = got.astype(BF16)

    def store_sum(m, h, xx):
        there = columns_at(xx, h)
        return pltpu.make_async_copy(sums.at[m, :, there], outs[m].at[:, there], o_s.at[m])

    def finish(h, m):
        for half in range(2):
            @pl.when(z > 0)
            def _():
                g_copy(m, h, z, 0, half).wait_recv()

            @pl.when(z < last)
            def _():
                g_copy(m, h, z, 1, half).wait_recv()

            for case, sources in ((z == 0, (1,)), (z == last, (0,)), ((z > 0) & (z < last), (0, 1))):
                @pl.when(case)
                def _():
                    total(m, h, half, sources)

            (store_sum(m, h, x) if half else f_copy(m, h)).start()

    def finish_at(h, m, ends):
        @pl.when((z == 0) | (z == last) if ends else (z > 0) & (z < last))
        def _():
            finish(h, m)

    def finish_x(h, m):
        f_copy(m, h).wait_recv()
        step = math.gcd(blk, 32)

        @pl.loop(0, blk // step)
        def _(i):
            at = pl.ds(pl.multiple_of(i * step, step), step)
            sums[m, at, columns_at(1 - x, h)] += xbuf[m, h, at, :].astype(F32) * factor

        store_sum(m, h, 1 - x).start()

    tile = math.gcd(span, 256)

    def span_at(i):
        return rows_at(((1 - side) * i + side * (last - i)) * span, span)

    def partial(a, k, w, i):
        first = ((1 - side) * i + side * (last - i)) * span

        @pl.loop(0, span // tile)
        def _(j):
            o = rows_at(first + j * tile, tile)
            got = None
            for h in range(chunks):
                one = lax.dot_general(hid[k, h], wts[w, h, o, :], (((1,), (1,)), ((), ())),
                                      preferred_element_type=F32)
                got = one if got is None else got + one
            part[a, :, o] = got.astype(BF16)

        for q in range(4):
            d_copy(a, q, i).start()

    def d_copy(a, q, i):
        return remote(part.at[a, rows_at(q * chip_rows + (1 - c) * rows_dev, rows_dev), span_at(i)],
                      dbuf.at[a, q, :, span_at(i)], d_s.at[a], d_r.at[a, i], mate)

    cuts_q = tuple(rows_dev * share // 8 // 16 * 16 for share in (2, 2))
    hops = (
        (1 - x, y, 0, qa, 0, x_next),
        (1 - x, 1 - y, 0, qa, 1, x_next),
        (x, 1 - y, 1, qb, 0, y_next),
        (1 - x, 1 - y, 1, qb, 1, y_next),
        (x, 1 - y, 0, qa, 2, y_next),
        (1 - x, y, 1, qb, 2, x_next),
    )

    def bounds(a, high):
        return (cuts_q[a], rows_dev - cuts_q[a]) if high else (0, cuts_q[a])

    def q_copy(a, k, i):
        xx, yy, high, buf, slot, to = hops[k]
        lo, count = bounds(a, high)
        return remote(part.at[a, rows_at(block_at(xx, yy, c) + lo, count), span_at(i)],
                      buf.at[a, slot, pl.ds(0, count), span_at(i)], q_s.at[a], q_r.at[a, k // 2, i] if k in (1, 3) else q_l.at[a], to)

    def q_first(a, i):
        there = dbuf.at[a, :, :, span_at(i)]
        remote(there, there, d_s.at[a], d_r.at[a, i], mate).wait_recv()
        for q in range(4):
            add_rows(part.at[a], q * chip_rows + c * rows_dev, dbuf.at[a, q], rows_dev, span_at(i))
        for k in (1, 3):
            q_copy(a, k, i).start()

    def q_rest(a, i):
        for k in (0, 2):
            q_copy(a, k, i).start()

    def q_second(a, i):
        q_copy(a, 1, i).wait_recv()
        add_rows(part.at[a], block_at(x, 1 - y, c), qa.at[a, 1], cuts_q[a], span_at(i))
        q_copy(a, 4, i).start()
        q_copy(a, 3, i).wait_recv()
        add_rows(part.at[a], block_at(1 - x, y, c) + cuts_q[a], qb.at[a, 1], rows_dev - cuts_q[a], span_at(i))
        q_copy(a, 5, i).start()

    def over(lo, hi, *calls):
        @pl.loop(lo, hi)
        def _(i):
            for call in calls:
                call(i)

    def store_out(a):
        return pltpu.make_async_copy(stage.at[a], (earlier_out, later_out)[a], o_s.at[2 + a])

    def q_last(a):
        there = part.at[a, pl.ds(0, 2 * rows_dev), :]
        remote(there, there, q_s.at[a], q_l.at[a], x_next).wait_recv()
        for high, buf in enumerate((qa, qb)):
            lo, count = bounds(a, high)
            step = math.gcd(count, 16)

            @pl.loop(0, count // step)
            def _(i):
                o = pl.multiple_of(i * step, step)
                at = pl.ds(o, step)
                own = pl.ds(pl.multiple_of(block_at(x, y, c) + lo + o, step), step)
                stage[a, pl.ds(pl.multiple_of(lo + o, step), step), :] = (
                    part[a, own, :].astype(F32) + buf[a, 0, at, :].astype(F32) + buf[a, 2, at, :].astype(F32)
                ).astype(BF16)

        store_out(a).start()

    wx_copy(0, 0).start()
    for m in range(2):
        load_w(m, 0).wait()
        spread(m, 0, fs)
    load_t(0).wait()
    for u in range(z_size):
        t_own(0, u)
    wx_copy(1, 0).start()
    from_x(0, (0,))
    relay(0, 1, (0,), (0,))
    t_pass(0, 0)
    t_pass(0, 1)
    relay(0, 1, (0,), (1,))
    relay(0, 1, (1,), (0,))
    t_pass(0, 2)
    relay(0, 2, (0,), (0,))
    t_pass(0, 3)
    for m in range(2):
        wx_copy(m, 1).start()
    load_t(1).wait()
    t_own(1, 0)
    t_own(1, 1)
    t_diagonal(0, 0)
    t_diagonal(0, 1)
    relay(0, 2, (1,), (0,))
    from_x(0, (1,))
    relay(0, 2, (0,), (1,))
    for m in range(2):
        load_w(m, 1).wait()
        spread_at(m, 1, fs, True)
    t_diagonal(0, 2)
    t_diagonal(0, 3)
    relay(0, 1, (1,), (1,))
    settle(0, 0, 1, z_size)
    t_mate(0)
    earlier_hidden(0)
    t_pass(1, 0)
    t_own(1, 2)
    relay(0, 2, (1,), (1,))
    from_x_at(1, (0, 1), True)
    spread_at(0, 1, fs, False)
    from_x_at(1, (0,), False)
    t_pass(1, 1)
    t_own(1, 3)
    t_diagonal(1, 0)
    t_mate(1, 0)
    term_step(1, 0, 0)
    relay(1, 1, (0,), (0,))
    t_pass(1, 2)
    t_diagonal(1, 1)
    t_mate(1, 1)
    term_step(1, 0, 1)
    relay(1, 1, (1,), (0,))
    spread_at(1, 1, fs, False)
    from_x_at(1, (1,), False)
    t_pass(1, 3)
    load_t(2).wait()
    t_own(2)
    t_diagonal(1, 2)
    t_mate(1, 2)
    term_step(1, 0, 2)
    reduce_step(0, 0, 1, True)
    t_diagonal(1, 3)
    t_mate(1, 3)
    settle(0, 1, 1, z_size)
    earlier_pre_grad(0)
    relay(1, 2, (0, 1), (0,))
    over(0, z_size, lambda i: term_step(0, 0, i))
    relay(1, 1, (0, 1), (1,))
    reduce_step(0, 1, 1, True)
    term_step(1, 0, last)
    t_pass(2)
    t_mate_blocks()
    later_hidden(0, 0, 3)
    settle(1, 0, 1, z_size)
    later_hidden(1, 0, 3)
    relay(1, 2, (0, 1), (1,))
    reduce_step(0, 0, 1, False)
    t_diagonal(2)
    t_mate_diagonal()
    for h in range(2):
        later_hidden(h, 3, 4)
    reduce_step(0, 0, 0, True)
    settle(1, 1, 1, last)
    partial(1, 2, 1, 0)
    over(1, last, lambda i: partial(1, 2, 1, i), lambda i: q_first(1, i - 1), lambda i: q_rest(1, i - 1))
    earlier_hidden(1)
    q_first(1, last - 1)
    q_rest(1, last - 1)
    over(0, z_size, lambda i: term_step(1, 1, i))
    q_second(1, 0)
    for m in range(2):
        totals[m].wait()
    finish_at(0, 1, False)
    reduce_step(0, 1, 0, True)
    settle(1, 1, last, z_size)
    partial(1, 2, 1, last)
    q_second(1, 1)
    reduce_step(0, 0, 0, False)
    earlier_pre_grad(1)
    q_first(1, last)
    q_rest(1, last)
    over(0, z_size, lambda i: term_step(0, 1, i))
    q_second(1, 2)
    finish_at(0, 1, True)
    reduce_step(1, 0, 1, True)
    partial(0, 0, 0, 0)
    over(1, z_size, lambda i: partial(0, 0, 0, i), lambda i: q_first(0, i - 1))
    reduce_step(1, 1, 1, True)
    q_second(1, last)
    q_first(0, last)
    over(0, z_size, lambda i: q_rest(0, i))
    finish(0, 0)
    reduce_step(1, 0, 1, False)
    finish(1, 1)
    reduce_step(1, 0, 0, True)
    over(0, z_size, lambda i: q_second(0, i))
    reduce_step(1, 1, 0, True)
    reduce_step(1, 0, 0, False)
    finish_x(0, 1)
    q_last(1)
    finish(1, 0)
    finish_x(0, 0)
    finish_x(1, 1)
    q_last(0)
    finish_x(1, 0)

    def sent(ref, semaphore):
        remote(ref, ref, semaphore, f_r.at[0, 0], mate).wait_send()

    four = wts.at[0, 0, pl.ds(0, 2 * chunks * blk), :]
    sent(four, wx_s)
    sent(four, f_s)
    for m in range(2):
        pltpu.make_async_copy(outs[m], outs[m], o_s.at[m]).wait()
        for h in range(chunks):
            for way in range(2):
                for hops_left in range(1, z_size):
                    @pl.when((last - z if way == 0 else z) == hops_left)
                    def _():
                        sent(wts.at[m, h, pl.ds(0, (z_size - hops_left) * zrows), :], wz_s.at[way, m, h])
                        sent(grads.at[m, h, pl.ds(0, hops_left * zrows), :], g_s.at[way, m, h])
    for a in range(3):
        sent(tok.at[a, pl.ds(0, 7 * rows_dev), :], t_s.at[a])
    for a in range(2):
        store_out(a).wait()
        sent(part.at[a, pl.ds(0, 4 * rows_dev), :], d_s.at[a])
        sent(part.at[a, pl.ds(0, 3 * rows_dev), :], q_s.at[a])


def plane_call(n, factor, *args):
    rows_dev, depth = args[0].shape
    blk, width = args[3].shape
    z_size, chunks, rows = n // 2, 2, rows_dev * 8
    cw = width // 2 // chunks
    low, high = rows_dev * 2 // 8 // 16 * 16, rows_dev - rows_dev * 2 // 8 // 16 * 16
    dma = pltpu.SemaphoreType.DMA
    hbm = pl.BlockSpec(memory_space=pltpu.HBM)
    return pl.pallas_call(
        functools.partial(plane_kernel, n, chunks, factor),
        out_shape=(
            jax.ShapeDtypeStruct((rows_dev, depth), BF16),
            jax.ShapeDtypeStruct((rows_dev, depth), BF16),
            jax.ShapeDtypeStruct((blk, width), F32),
            jax.ShapeDtypeStruct((blk, width), F32),
        ),
        in_specs=[hbm] * 7,
        out_specs=(hbm,) * 4,
        scratch_shapes=[
            pltpu.VMEM((3, rows, depth), BF16),
            pltpu.VMEM((2, chunks, depth, cw), BF16),
            pltpu.VMEM((rows, cw), F32),
            pltpu.VMEM((3, chunks, rows, cw), BF16),
            pltpu.VMEM((2, chunks, depth, cw), BF16),
            pltpu.VMEM((2, chunks, z_size + 1, 2, blk, cw), BF16),
            pltpu.VMEM((2, chunks, blk, cw), BF16),
            pltpu.VMEM((2, chunks, blk, cw), BF16),
            pltpu.VMEM((2, rows, depth), BF16),
            pltpu.VMEM((2, 4, rows_dev, depth), BF16),
            pltpu.VMEM((2, 3, low, depth), BF16),
            pltpu.VMEM((2, 3, high, depth), BF16),
            pltpu.VMEM((2, rows_dev, depth), BF16),
            pltpu.VMEM((2, blk, width), F32),
            dma((2 * chunks + 5,)), dma((4,)), dma((3,)), dma((6 + 10 * z_size,)), dma, dma((2, 2, chunks)), dma((2, chunks, n)),
            dma((2, 2, chunks)), dma((2, chunks, z_size + 1, 2)), dma, dma((2, chunks)),
            dma((2,)), dma((2, z_size)), dma((2,)), dma((2, 2, z_size)), dma((2,)),
        ],
        compiler_params=pltpu.CompilerParams(
            collective_id=0, has_side_effects=True, vmem_limit_bytes=67043328
        ),
        name="feed_forward_planes",
    )(*args)


def hand_on_kernel(*refs):
    count = (len(refs) - 2) // 3
    ins, outs, held, in_s, out_s = refs[:count], refs[count:2 * count], refs[2 * count:-2], refs[-2], refs[-1]
    loads, stores = [], []
    for a, (src, kept, dst) in enumerate(zip(ins, held, outs)):
        half = src.shape[0] // 2
        for i in range(2):
            o = pl.ds(i * half, half)
            loads.append(pltpu.make_async_copy(src.at[o, :], kept.at[o, :], in_s.at[a, i]))
            stores.append(pltpu.make_async_copy(kept.at[o, :], dst.at[o, :], out_s.at[a, i]))
    for load in loads:
        load.start()
    for load, store in zip(loads, stores):
        load.wait()
        store.start()
    for store in stores:
        store.wait()


def hand_on(*arrays):
    count = len(arrays)
    hbm = pl.BlockSpec(memory_space=pltpu.HBM)
    return pl.pallas_call(
        hand_on_kernel,
        out_shape=tuple(jax.ShapeDtypeStruct(a.shape, a.dtype) for a in arrays),
        in_specs=[hbm] * count,
        out_specs=(hbm,) * count,
        scratch_shapes=[*(pltpu.VMEM(a.shape, a.dtype) for a in arrays),
                        pltpu.SemaphoreType.DMA((count, 2)), pltpu.SemaphoreType.DMA((count, 2))],
        compiler_params=pltpu.CompilerParams(vmem_limit_bytes=67043328),
        name="feed_forward_results",
    )(*arrays)


def ring_call(n, m, *args):
    rows_dev, depth = args[0].shape
    blk, width = args[3].shape
    rows, half, y_size = rows_dev * m, n // 2, m // 2
    dma = pltpu.SemaphoreType.DMA
    vmem = pl.BlockSpec(memory_space=pltpu.VMEM)
    sums = max(y_size - 1, 1)
    parts = 2 if width % 256 == 0 else 1
    return pl.pallas_call(
        functools.partial(kernel, n, m, parts),
        out_shape=(
            jax.ShapeDtypeStruct((rows_dev, depth), BF16),
            jax.ShapeDtypeStruct((rows_dev, depth), BF16),
            jax.ShapeDtypeStruct((blk, width), BF16),
            jax.ShapeDtypeStruct((blk, width), BF16),
        ),
        in_specs=[vmem] * 5,
        out_specs=(vmem,) * 4,
        scratch_shapes=[
            pltpu.VMEM((3, rows, depth), BF16),
            pltpu.VMEM((2, depth, width), BF16),
            pltpu.VMEM((3, rows, width), F32),
            pltpu.VMEM((3, rows, width), BF16),
            pltpu.VMEM((2, depth, width), BF16),
            pltpu.VMEM((4, half, blk, width), BF16),
            pltpu.VMEM((2, rows, depth), BF16),
            pltpu.VMEM((2, y_size, rows_dev, depth), BF16),
            pltpu.VMEM((2, sums, rows_dev, depth), BF16),
            dma((3, y_size)), dma((3, y_size)), dma((3, y_size)), dma((3, y_size)),
            *[dma((4, half, parts))] * 4,
            dma((2, y_size)), dma((2, y_size)), dma((2, sums)), dma((2, sums)),
        ],
        compiler_params=pltpu.CompilerParams(
            collective_id=0, has_side_effects=True, vmem_limit_bytes=67043328
        ),
        name="feed_forward_step",
    )(*args)


def body(n, m, later_rows, earlier_rows, cotangent, up_weight, down_weight, up_total, down_total):
    rows = later_rows.shape[0] * m
    factor = 1.0 / math.sqrt(rows * n)
    width = up_weight.shape[1]
    planar = columns_of(n) == 2 and n == 8 and m == 4 and width % 1024 == 0 and rows % 512 == 0
    planes = (later_rows, earlier_rows, cotangent, up_weight, down_weight)
    if planar:
        return tuple(hand_on(*plane_call(n, factor, *planes, up_total, down_total)))
    later_out, earlier_grad, up_term, down_term = ring_call(n, m, *planes)
    up_updated = up_total + up_term.astype(F32) * factor
    down_updated = down_total + down_term.astype(F32) * factor
    return later_out, earlier_grad, up_updated, down_updated


def solution(mesh):
    return jax.shard_map(
        functools.partial(body, mesh.shape["fs"], mesh.shape["tp"]),
        mesh=mesh,
        in_specs=(
            P(("fs", "tp"), None),
            P(("fs", "tp"), None),
            P(("fs", "tp"), None),
            P("fs", "tp"),
            P("fs", "tp"),
            P("fs", "tp"),
            P("fs", "tp"),
        ),
        out_specs=(P(("fs", "tp"), None), P(("fs", "tp"), None), P("fs", "tp"), P("fs", "tp")),
        check_vma=False,
    )
```

```python
import functools
import math

import jax
import jax.numpy as jnp
from jax import lax
from jax.experimental import pallas as pl
from jax.experimental.pallas import tpu as pltpu
from jax.sharding import PartitionSpec as P

MESH = pl.DeviceIdType.MESH
BF16 = jnp.bfloat16
F32 = jnp.float32


def columns_of(n):
    best = 1
    for x in range(1, n + 1):
        if n % x == 0 and 2 * x * x <= n and (n // x) % 2 == 0:
            best = x
    return best


def ring_to_fs(p, n, x_size):
    if x_size == 1:
        return p
    z_size, wide = n // x_size, x_size - 1
    body = z_size * wide
    z, r = p // wide, p % wide
    x = 1 + jnp.where(z % 2 == 0, r, wide - 1 - r)
    back = z_size - 1 - (p - body)
    return jnp.where(p < body, z * x_size + x, back * x_size)


def fs_to_ring(f, n, x_size):
    if x_size == 1:
        return f
    z_size, wide = n // x_size, x_size - 1
    z, x = f // x_size, f % x_size
    r = jnp.where(z % 2 == 0, x - 1, x_size - 1 - x)
    return jnp.where(x == 0, z_size * wide + z_size - 1 - z, z * wide + r)


def kernel(n, m, parts,
           later_ref, earlier_ref, cot_ref, up_ref, down_ref,
           later_out, earlier_out, up_out, down_out,
           tok, wts, acc, hid, grads, rbuf, part, dbuf, ybuf,
           ty_s, ty_r, td_s, td_r, w_s, w_r, g_s, g_r, od_s, od_r, oy_s, oy_r):
    rows_dev, depth = later_ref.shape
    blk, width = up_ref.shape
    rows = rows_dev * m
    half, y_size = n // 2, m // 2
    aligned = blk % 128 == 0
    wide_q = width // parts
    fs, tp = lax.axis_index("fs"), lax.axis_index("tp")
    x_size = columns_of(n)
    pos = fs_to_ring(fs, n, x_size)
    y, c = tp // 2, tp % 2

    def at_ring(p):
        return ring_to_fs((p + 2 * n) % n, n, x_size)

    right = {"fs": at_ring(pos + 1), "tp": tp}
    left = {"fs": at_ring(pos - 1), "tp": tp}
    mate = {"fs": fs, "tp": y * 2 + 1 - c}
    y_next = {"fs": fs, "tp": ((y + 1) % y_size) * 2 + c}
    y_prev = {"fs": fs, "tp": ((y + y_size - 1) % y_size) * 2 + c}

    barrier = pltpu.get_barrier_semaphore()
    for other in (right, left, mate, y_next, y_prev):
        pl.semaphore_signal(barrier, inc=1, device_id=other, device_id_type=MESH)
    pl.semaphore_wait(barrier, 5)

    def remote(src, dst, send, recv, to):
        return pltpu.make_async_remote_copy(
            src_ref=src, dst_ref=dst, send_sem=send, recv_sem=recv, device_id=to, device_id_type=MESH)

    def trows(a, t):
        return tok.at[a, pl.ds(pl.multiple_of(t * rows_dev, rows_dev), rows_dev), :]

    own_w, own_t = (up_ref, down_ref), (earlier_ref, cot_ref, later_ref)

    arr_of, sign_of = (0, 1, 1, 0), (1, -1, 1, -1)

    def cut(q):
        return pl.ds(q * wide_q, wide_q)

    def w_copy(k, s, q, first=False):
        f = at_ring(pos - sign_of[k] * s)
        there = wts.at[arr_of[k], pl.ds(pl.multiple_of(f * blk, blk), blk), cut(q)]
        src = own_w[arr_of[k]].at[:, cut(q)] if first else there
        return remote(src, there, w_s.at[k, s, q], w_r.at[k, s, q], right if sign_of[k] > 0 else left)

    def ty_copy(a, s, first=False):
        t = ((y + y_size - s) % y_size) * 2 + c
        return remote(own_t[a] if first else trows(a, t), trows(a, t), ty_s.at[a, s], ty_r.at[a, s], y_next)

    def td_copy(a, s, first=False):
        t = ((y + y_size - s) % y_size) * 2 + c
        return remote(own_t[a] if first else trows(a, t), trows(a, t), td_s.at[a, s], td_r.at[a, s], mate)

    every = tuple((k, q) for pair in ((0, 1), (2, 3)) for q in range(parts) for k in pair)
    longs = tuple((k, q) for k, q in every if k < 2)
    for k, q in every:
        w_copy(k, 0, q, True).start()
    for a in range(3):
        if y_size > 1:
            ty_copy(a, 0, True).start()
    for a in range(3):
        td_copy(a, 0, True).start()

    def put(dst, dst_row, src, count):
        step = math.gcd(count, 64)

        @pl.loop(0, count // step)
        def _(i):
            o = pl.multiple_of(i * step, step)
            dst[pl.ds(pl.multiple_of(dst_row + o, step), step), :] = src[pl.ds(o, step), :]

    for a in range(2):
        put(wts.at[a], fs * blk, own_w[a], blk)
    for a in range(3):
        put(tok.at[a], tp * rows_dev, own_t[a], rows_dev)

    tile = math.gcd(wide_q, 256)

    def multiply(a, w, rows_w, clear, q=None):
        first, count = (0, width) if q is None else (q * wide_q, wide_q)

        @pl.loop(0, count // tile)
        def _(j):
            o = pl.ds(pl.multiple_of(first + j * tile, tile), tile)
            got = jnp.dot(tok[a, :, rows_w], wts[w, rows_w, o], preferred_element_type=F32)
            if clear:
                acc[a, :, o] = got
            else:
                acc[a, :, o] += got

    def use(w, f, clear=False, q=None):
        if not aligned:
            return
        o = pl.ds(pl.multiple_of(f * blk, blk), blk)
        for a in ((0, 2) if w == 0 else (1,)):
            multiply(a, w, o, clear, q)

    def forward(s, present, go):
        for k, q in present:
            w_copy(k, s - 1, q).wait_recv()
            if (k, q) in go:
                w_copy(k, s, q).start()

    def use_step(s):
        for k in range(4):
            use(arr_of[k], at_ring(pos - sign_of[k] * s))

    forward(1, every, every if half > 2 else longs)
    for s in range(1, y_size):
        for a in range(3):
            ty_copy(a, s - 1).wait_recv()
            if s < y_size - 1:
                ty_copy(a, s).start()
            td_copy(a, s).start()
    for s in range(y_size):
        for a in range(3):
            td_copy(a, s).wait_recv()
    for w in range(2):
        use(w, fs, True)
    if half > 3:
        @pl.loop(2, half - 1)
        def _(s):
            forward(s, every, every)
            use_step(s - 1)
    if half > 2:
        forward(half - 1, every, longs)
        use_step(half - 2)
    use_step(half - 1)

    step_r = math.gcd(rows, 32)

    def activate(q):
        @pl.loop(0, rows // step_r)
        def _(i):
            o = pl.ds(pl.multiple_of(i * step_r, step_r), step_r)
            relu = jnp.maximum(acc[0, o, cut(q)], 0.0)
            hid[0, o, cut(q)] = (2.0 * relu * acc[1, o, cut(q)]).astype(BF16)
            hid[1, o, cut(q)] = (relu * relu).astype(BF16)

    def term(a, row, size, q=None):
        first, count = (0, width) if q is None else (q * wide_q, wide_q)

        @pl.loop(0, count // tile)
        def _(j):
            o = pl.ds(pl.multiple_of(first + j * tile, tile), tile)
            grads[a, pl.ds(row, size), o] = lax.dot_general(
                tok[a, :, pl.ds(row, size)], hid[a, :, o], (((0,), (0,)), ((), ())),
                preferred_element_type=F32).astype(BF16)

    def block_term(a, p, q=None):
        term(a, pl.multiple_of(at_ring(p) * blk, blk), blk, q)

    def g_copy(k, s, q):
        d = half - (k >= 2) - s
        f = at_ring(pos + sign_of[k] * d)
        src = grads.at[arr_of[k], pl.ds(pl.multiple_of(f * blk, blk), blk), cut(q)]
        return remote(src, rbuf.at[k, s, :, cut(q)], g_s.at[k, s, q], g_r.at[k, s, q],
                      right if sign_of[k] > 0 else left)

    def add_rows(dst, dst_row, src, count, columns=slice(None)):
        step = math.gcd(count, 32)

        @pl.loop(0, count // step)
        def _(i):
            o = pl.multiple_of(i * step, step)
            at = pl.ds(pl.multiple_of(dst_row + o, step), step)
            total = dst[at, columns].astype(F32) + src[pl.ds(o, step), columns].astype(F32)
            dst[at, columns] = total.astype(BF16)

    def g_step(s, which):
        for k, q in which:
            g_copy(k, s - 1, q).wait_recv()
            f = at_ring(pos + sign_of[k] * (half - (k >= 2) - s))
            add_rows(grads.at[arr_of[k]], f * blk, rbuf.at[k, s - 1], blk, cut(q))
            g_copy(k, s, q).start()

    wide = math.gcd(depth, 256)
    for q in range(parts):
        for k in (0, 1):
            w_copy(k, half - 1, q).wait_recv()
            use(arr_of[k], at_ring(pos - sign_of[k] * half), q=q)
        if not aligned:
            full = pl.ds(0, depth)
            for a, w in ((0, 0), (1, 1), (2, 0)):
                multiply(a, w, full, True, q)
        activate(q)
        if not aligned:
            for a in range(2):
                @pl.loop(0, depth // wide)
                def _(i):
                    term(a, pl.multiple_of(i * wide, wide), wide, q)
        for k in (0, 1):
            if aligned:
                block_term(arr_of[k], pos + sign_of[k] * half, q)
            g_copy(k, 0, q).start()
    for k in (2, 3):
        if aligned:
            block_term(arr_of[k], pos + sign_of[k] * (half - 1))
        for q in range(parts):
            g_copy(k, 0, q).start()
    if aligned:
        if half > 1:
            @pl.loop(0, half - 1)
            def _(i):
                d = half - 1 - i
                block_term(0, pos + d)
                block_term(1, pos - d)
        if half > 2:
            @pl.loop(0, half - 2)
            def _(i):
                d = half - 2 - i
                block_term(1, pos + d)
                block_term(0, pos - d)
        for a in range(2):
            block_term(a, pos)

    @pl.loop(0, rows // step_r)
    def _(i):
        o = pl.ds(pl.multiple_of(i * step_r, step_r), step_r)
        relu = jnp.maximum(acc[2, o, :], 0.0)
        hid[2, o, :] = (relu * relu).astype(BF16)

    wide_d = math.gcd(depth, 256)

    def partial(a, h, w):
        @pl.loop(0, depth // wide_d)
        def _(j):
            o = pl.ds(pl.multiple_of(j * wide_d, wide_d), wide_d)
            part[a, :, o] = lax.dot_general(
                hid[h], wts[w, o, :], (((1,), (1,)), ((), ())), preferred_element_type=F32).astype(BF16)

    def prow(yy, cc):
        return pl.multiple_of((yy * 2 + cc) * rows_dev, rows_dev)

    def od_copy(a, yy):
        return remote(part.at[a, pl.ds(prow(yy, 1 - c), rows_dev), :], dbuf.at[a, yy],
                      od_s.at[a, yy], od_r.at[a, yy], mate)

    def oy_copy(a, s):
        t = (y + y_size - 1 - s) % y_size
        return remote(part.at[a, pl.ds(prow(t, c), rows_dev), :], ybuf.at[a, s],
                      oy_s.at[a, s], oy_r.at[a, s], y_next)

    def send_partial(a, h, w):
        partial(a, h, w)
        for yy in range(y_size):
            od_copy(a, yy).start()

    send_partial(0, 0, 0)
    g_step(1, every if half > 2 else longs)
    send_partial(1, 2, 1)
    for a in range(2):
        for yy in range(y_size):
            od_copy(a, yy).wait_recv()
            add_rows(part.at[a], prow(yy, c), dbuf.at[a, yy], rows_dev)
        if y_size > 1:
            oy_copy(a, 0).start()
    if half - 1 > 2:
        @pl.loop(2, half - 1)
        def _(s):
            g_step(s, every)
    for s in range(1, y_size):
        for a in range(2):
            oy_copy(a, s - 1).wait_recv()
            t = (y + y_size - 1 - s) % y_size
            add_rows(part.at[a], prow(t, c), ybuf.at[a, s - 1], rows_dev)
            if s < y_size - 1:
                oy_copy(a, s).start()
    put_own = ((earlier_out, 0), (later_out, 1))
    for out, a in put_own:
        out[...] = part[a, pl.ds(prow(y, c), rows_dev), :]
    if half - 1 >= 2:
        g_step(half - 1, longs)

    ends = [(k, half - 1 - (k >= 2)) for k in range(4)]
    for k, q in tuple((k, q) for k, q in every if k >= 2) + longs:
        g_copy(k, ends[k][1], q).wait_recv()
    step_b = math.gcd(blk, 32)
    for a, out in ((0, up_out), (1, down_out)):
        @pl.loop(0, blk // step_b)
        def _(i):
            lo = pl.multiple_of(i * step_b, step_b)
            o = pl.ds(lo, step_b)
            got = grads[a, pl.ds(pl.multiple_of(fs * blk + lo, step_b), step_b), :].astype(F32)
            for k, s in ends:
                if arr_of[k] == a:
                    got += rbuf[k, s, o, :].astype(F32)
            out[o, :] = got.astype(BF16)

    for k, q in every:
        for s in range(half - (k >= 2)):
            w_copy(k, s, q).wait_send()
            g_copy(k, s, q).wait_send()
    for a in range(3):
        for s in range(y_size):
            if s < y_size - 1:
                ty_copy(a, s).wait_send()
            td_copy(a, s).wait_send()
    for a in range(2):
        for yy in range(y_size):
            od_copy(a, yy).wait_send()
        for s in range(y_size - 1):
            oy_copy(a, s).wait_send()


def plane_kernel(n, chunks, factor,
                 later_ref, earlier_ref, cot_ref, up_ref, down_ref, up_total, down_total,
                 later_out, earlier_out, up_out, down_out,
                 tok, wts, act, hid, grads, gbuf, fin, xbuf, part, dbuf, qa, qb, stage, sums,
                 l_s, o_s, t_s, t_r, wx_s, wz_s, w_r, g_s, g_r, f_s, f_r, d_s, d_r, q_s, q_r, q_l):
    rows_dev, depth = later_ref.shape
    blk, width = up_ref.shape
    z_size, zrows = n // 2, 2 * blk
    wide, cw = width // 2, width // 2 // chunks
    chip_rows = 2 * rows_dev
    fs, tp = lax.axis_index("fs"), lax.axis_index("tp")
    z, x, y, c = fs // 2, fs % 2, tp // 2, tp % 2
    last = z_size - 1
    side = 2 * z // z_size
    span = 2 * blk

    right = {"fs": ((z + 1) % z_size) * 2 + x, "tp": tp}
    left = {"fs": ((z + last) % z_size) * 2 + x, "tp": tp}
    x_next = {"fs": z * 2 + 1 - x, "tp": tp}
    y_next = {"fs": fs, "tp": (1 - y) * 2 + c}
    mate = {"fs": fs, "tp": y * 2 + 1 - c}

    def block_at(xx, yy, cc):
        return ((xx * 2 + yy) * 2 + cc) * rows_dev

    def rows_at(start, count):
        return pl.ds(pl.multiple_of(start, math.gcd(count, 128)), count)

    def columns_at(xx, h):
        return pl.ds(pl.multiple_of(xx * wide + h * cw, cw), cw)

    own_w, own_t = (up_ref, down_ref), (earlier_ref, cot_ref, later_ref)

    def load_w(m, h):
        return pltpu.make_async_copy(
            own_w[m].at[:, columns_at(x, h)], wts.at[m, h, rows_at(fs * blk, blk), :], l_s.at[m * chunks + h])

    def load_t(a):
        return pltpu.make_async_copy(
            own_t[a], tok.at[a, rows_at(block_at(x, y, c), rows_dev), :], l_s.at[2 * chunks + a])

    for m in range(2):
        load_w(m, 0).start()
    load_t(0).start()
    load_t(1).start()
    for m in range(2):
        load_w(m, 1).start()
    load_t(2).start()
    totals = tuple(
        pltpu.make_async_copy(total, sums.at[m], l_s.at[2 * chunks + 3 + m])
        for m, total in enumerate((up_total, down_total)))
    for m in range(2):
        totals[m].start()

    barrier = pltpu.get_barrier_semaphore()
    for other in (right, left, x_next, y_next, mate):
        pl.semaphore_signal(barrier, inc=1, device_id=other, device_id_type=MESH)
    pl.semaphore_wait(barrier, 5)

    def remote(src, dst, send, recv, to):
        return pltpu.make_async_remote_copy(
            src_ref=src, dst_ref=dst, send_sem=send, recv_sem=recv, device_id=to, device_id_type=MESH)

    def piece(m, h, f):
        return wts.at[m, h, rows_at(f * blk, blk), :]

    def wx_copy(m, h):
        return remote(own_w[m].at[:, columns_at(1 - x, h)], piece(m, h, fs), wx_s, w_r.at[m, h, fs], x_next)

    def wz_copy(m, h, f, way):
        return remote(piece(m, h, f), piece(m, h, f), wz_s.at[way, m, h], w_r.at[m, h, f], left if way else right)

    def w_got(m, h, f):
        wz_copy(m, h, f, 0).wait_recv()

    def spread(m, h, f):
        @pl.when(z < last)
        def _():
            wz_copy(m, h, f, 0).start()

        @pl.when(z > 0)
        def _():
            wz_copy(m, h, f, 1).start()

    def spread_at(m, h, f, ends):
        @pl.when((z == 0) | (z == last) if ends else (z > 0) & (z < last))
        def _():
            spread(m, h, f)

    def from_x(h, ms=(0, 1)):
        for m in ms:
            w_got(m, h, z * 2 + 1 - x)
            spread(m, h, z * 2 + 1 - x)

    def from_x_at(h, ms, ends):
        @pl.when((z == 0) | (z == last) if ends else (z > 0) & (z < last))
        def _():
            from_x(h, ms)

    def relay(h, d, columns=(0, 1), ms=(0, 1)):
        for m in ms:
            for p in columns:
                p = (x + p) % 2

                @pl.when((z >= d) & (z < last))
                def _():
                    w_got(m, h, (z - d) * 2 + p)
                    wz_copy(m, h, (z - d) * 2 + p, 0).start()

                @pl.when((z + d < z_size) & (z > 0))
                def _():
                    w_got(m, h, (z + d) * 2 + p)
                    wz_copy(m, h, (z + d) * 2 + p, 1).start()

    def settle(h, m, lo, hi):
        @pl.when((z == 0) | (z == last))
        def _():
            @pl.loop(lo, hi)
            def _(d):
                for p in range(2):
                    w_got(m, h, jnp.where(z == 0, d, last - d) * 2 + p)

    def moves(cut_t):
        return (
            (x, y, 0, rows_dev, x_next),
            (x, y, 0, rows_dev, y_next),
            (1 - x, y, 0, cut_t, y_next),
            (x, 1 - y, cut_t, rows_dev - cut_t, x_next),
            (x, y, 0, rows_dev, mate),
            (1 - x, y, 0, rows_dev, mate),
            (x, 1 - y, 0, rows_dev, mate),
            (1 - x, 1 - y, 0, cut_t, mate),
            (1 - x, 1 - y, cut_t, rows_dev - cut_t, mate),
        )

    cuts = tuple(rows_dev * part // 8 // 16 * 16 for part in (7, 5, 4))

    def facing(i):
        return (1 - side) * (last - i) + side * i

    def t_ref(a, start, count, u):
        return tok.at[a, rows_at(start, count), slice(None) if u is None else rows_at(facing(u) * span, span)]

    def t_got(a, k, u):
        slot = u if k < 4 or a == 1 else k // 7 if a == 2 else 0
        return t_r.at[a, min(k, 4), slot]

    def t_copy(a, k, u):
        xx, yy, lo, count, to = moves(cuts[a])[k]
        there = t_ref(a, block_at(xx, yy, c) + lo, count, u)
        return remote(there, there, t_s.at[a], t_got(a, k, u), to)

    def t_own(a, u):
        for k in (0, 1, 4):
            t_copy(a, k, u).start()

    def t_pass(a, u):
        t_copy(a, 1, u).wait_recv()
        t_copy(a, 3, u).start()
        t_copy(a, 6, u).start()
        t_copy(a, 0, u).wait_recv()
        t_copy(a, 2, u).start()
        t_copy(a, 5, u).start()

    def t_diagonal(a, u):
        t_copy(a, 2, u).wait_recv()
        t_copy(a, 7, u).start()
        t_copy(a, 3, u).wait_recv()
        t_copy(a, 8, u).start()

    def t_mate(a, u=None):
        there = t_ref(a, 0, 4 * rows_dev, u)
        remote(there, there, t_s.at[a], t_got(a, 4, u), mate).wait_recv()

    def t_mate_blocks():
        there = t_ref(2, 0, 3 * rows_dev, None)
        remote(there, there, t_s.at[2], t_got(2, 4, None), mate).wait_recv()

    def t_mate_diagonal():
        there = t_ref(2, 0, rows_dev, None)
        remote(there, there, t_s.at[2], t_got(2, 7, None), mate).wait_recv()

    def earlier_hidden(h):
        @pl.loop(0, 4)
        def _(i):
            o = rows_at(i * chip_rows, chip_rows)
            relu = jnp.maximum(jnp.dot(tok[0, o, :], wts[0, h], preferred_element_type=F32), 0.0)
            act[o, :] = relu
            hid[1, h, o, :] = (relu * relu).astype(BF16)

    def earlier_pre_grad(h):
        @pl.loop(0, 4)
        def _(i):
            o = rows_at(i * chip_rows, chip_rows)
            got = jnp.dot(tok[1, o, :], wts[1, h], preferred_element_type=F32)
            hid[0, h, o, :] = (2.0 * act[o, :] * got).astype(BF16)

    def chip_at(i):
        return (((x + i % 2) % 2) * 2 + (y + i // 2) % 2) * chip_rows

    def later_hidden(h, lo, hi):
        @pl.loop(lo, hi)
        def _(i):
            o = rows_at(chip_at(i), chip_rows)
            relu = jnp.maximum(jnp.dot(tok[2, o, :], wts[0, h], preferred_element_type=F32), 0.0)
            hid[2, h, o, :] = (relu * relu).astype(BF16)

    def term(m, h, d):
        o = rows_at(d * zrows, zrows)
        grads[m, h, o, :] = lax.dot_general(
            tok[m, :, o], hid[m, h], (((0,), (0,)), ((), ())), preferred_element_type=F32).astype(BF16)

    def half_at(d, half):
        return d * zrows + (x + 1 - half) % 2 * blk

    def g_copy(m, h, d, way, half):
        src = grads.at[m, h, rows_at(half_at(d, half), blk), :]
        to = {"fs": ((z + z_size + 1 - 2 * way) % z_size) * 2 + x, "tp": tp}
        slot = d + 1 - way
        return remote(src, gbuf.at[m, h, slot, half], g_s.at[way, m, h], g_r.at[m, h, slot, half], to)

    def term_step(m, h, i):
        d = facing(i)
        term(m, h, d)

        @pl.when(((z == 0) | (z == last)) & (i < last))
        def _():
            for half in range(2):
                g_copy(m, h, d, side, half).start()

    def add_rows(dst, dst_row, src, count, columns=slice(None)):
        step = math.gcd(count, 32)

        @pl.loop(0, count // step)
        def _(i):
            o = pl.multiple_of(i * step, step)
            at = pl.ds(pl.multiple_of(dst_row + o, math.gcd(step, 16)), step)
            dst[at, columns] = (dst[at, columns].astype(F32) + src[pl.ds(o, step), columns].astype(F32)).astype(BF16)

    def reduce_step(h, k, m, near):
        way = side if near else 1 - side
        d = (1 - way) * (last - k) + way * k
        beyond = (1 - 2 * way) * (d - z)
        behind = (1 - way) * z + way * (last - z)

        @pl.when((beyond > 0) & (behind > 0))
        def _():
            for half in range(2):
                g_copy(m, h, d, way, half).wait_recv()
                add_rows(grads.at[m, h], half_at(d, half), gbuf.at[m, h, d + 1 - way, half], blk)
                g_copy(m, h, d, way, half).start()

    outs = (up_out, down_out)

    def f_copy(m, h):
        return remote(fin.at[m, h], xbuf.at[m, h], f_s, f_r.at[m, h], x_next)

    def total(m, h, half, sources):
        step = math.gcd(blk, 32)

        @pl.loop(0, blk // step)
        def _(i):
            o = pl.multiple_of(i * step, step)
            at = pl.ds(o, step)
            got = grads[m, h, pl.ds(pl.multiple_of(half_at(z, half) + o, step), step), :].astype(F32)
            for src in sources:
                got += gbuf[m, h, z + 1 - src, half, at, :].astype(F32)
            if half:
                sums[m, at, columns_at(x, h)] += got * factor
            else:
                fin[m, h, at, :] = got.astype(BF16)

    def store_sum(m, h, xx):
        there = columns_at(xx, h)
        return pltpu.make_async_copy(sums.at[m, :, there], outs[m].at[:, there], o_s.at[m])

    def finish(h, m):
        for half in range(2):
            @pl.when(z > 0)
            def _():
                g_copy(m, h, z, 0, half).wait_recv()

            @pl.when(z < last)
            def _():
                g_copy(m, h, z, 1, half).wait_recv()

            for case, sources in ((z == 0, (1,)), (z == last, (0,)), ((z > 0) & (z < last), (0, 1))):
                @pl.when(case)
                def _():
                    total(m, h, half, sources)

            (store_sum(m, h, x) if half else f_copy(m, h)).start()

    def finish_at(h, m, ends):
        @pl.when((z == 0) | (z == last) if ends else (z > 0) & (z < last))
        def _():
            finish(h, m)

    def finish_x(h, m):
        f_copy(m, h).wait_recv()
        step = math.gcd(blk, 32)

        @pl.loop(0, blk // step)
        def _(i):
            at = pl.ds(pl.multiple_of(i * step, step), step)
            sums[m, at, columns_at(1 - x, h)] += xbuf[m, h, at, :].astype(F32) * factor

        store_sum(m, h, 1 - x).start()

    tile = math.gcd(span, 256)

    def span_at(i):
        return rows_at(((1 - side) * i + side * (last - i)) * span, span)

    def partial(a, k, w, i):
        first = ((1 - side) * i + side * (last - i)) * span

        @pl.loop(0, span // tile)
        def _(j):
            o = rows_at(first + j * tile, tile)
            got = None
            for h in range(chunks):
                one = lax.dot_general(hid[k, h], wts[w, h, o, :], (((1,), (1,)), ((), ())),
                                      preferred_element_type=F32)
                got = one if got is None else got + one
            part[a, :, o] = got.astype(BF16)

        for q in range(4):
            d_copy(a, q, i).start()

    def d_copy(a, q, i):
        return remote(part.at[a, rows_at(q * chip_rows + (1 - c) * rows_dev, rows_dev), span_at(i)],
                      dbuf.at[a, q, :, span_at(i)], d_s.at[a], d_r.at[a, i], mate)

    cuts_q = tuple(rows_dev * share // 8 // 16 * 16 for share in (2, 3))
    hops = (
        (1 - x, y, 0, qa, 0, x_next),
        (1 - x, 1 - y, 0, qa, 1, x_next),
        (x, 1 - y, 1, qb, 0, y_next),
        (1 - x, 1 - y, 1, qb, 1, y_next),
        (x, 1 - y, 0, qa, 2, y_next),
        (1 - x, y, 1, qb, 2, x_next),
    )

    def bounds(a, high):
        return (cuts_q[a], rows_dev - cuts_q[a]) if high else (0, cuts_q[a])

    def q_copy(a, k, i):
        xx, yy, high, buf, slot, to = hops[k]
        lo, count = bounds(a, high)
        return remote(part.at[a, rows_at(block_at(xx, yy, c) + lo, count), span_at(i)],
                      buf.at[a, slot, pl.ds(0, count), span_at(i)], q_s.at[a], q_r.at[a, k // 2, i] if k in (1, 3) else q_l.at[a], to)

    def q_first(a, i):
        there = dbuf.at[a, :, :, span_at(i)]
        remote(there, there, d_s.at[a], d_r.at[a, i], mate).wait_recv()
        for q in range(4):
            add_rows(part.at[a], q * chip_rows + c * rows_dev, dbuf.at[a, q], rows_dev, span_at(i))
        for k in (1, 3):
            q_copy(a, k, i).start()

    def q_rest(a, i):
        for k in (0, 2):
            q_copy(a, k, i).start()

    def q_second_y(a, i):
        q_copy(a, 1, i).wait_recv()
        add_rows(part.at[a], block_at(x, 1 - y, c), qa.at[a, 1], cuts_q[a], span_at(i))
        q_copy(a, 4, i).start()

    def q_second_x(a, i):
        q_copy(a, 3, i).wait_recv()
        add_rows(part.at[a], block_at(1 - x, y, c) + cuts_q[a], qb.at[a, 1], rows_dev - cuts_q[a], span_at(i))
        q_copy(a, 5, i).start()

    def over(lo, hi, *calls):
        @pl.loop(lo, hi)
        def _(i):
            for call in calls:
                call(i)

    def store_out(a):
        return pltpu.make_async_copy(stage.at[a], (earlier_out, later_out)[a], o_s.at[2 + a])

    def q_last(a):
        there = part.at[a, pl.ds(0, 2 * rows_dev), :]
        remote(there, there, q_s.at[a], q_l.at[a], x_next).wait_recv()
        for high, buf in enumerate((qa, qb)):
            lo, count = bounds(a, high)
            step = math.gcd(count, 16)

            @pl.loop(0, count // step)
            def _(i):
                o = pl.multiple_of(i * step, step)
                at = pl.ds(o, step)
                own = pl.ds(pl.multiple_of(block_at(x, y, c) + lo + o, step), step)
                stage[a, pl.ds(pl.multiple_of(lo + o, step), step), :] = (
                    part[a, own, :].astype(F32) + buf[a, 0, at, :].astype(F32) + buf[a, 2, at, :].astype(F32)
                ).astype(BF16)

        store_out(a).start()

    wx_copy(0, 0).start()
    for m in range(2):
        load_w(m, 0).wait()
        spread(m, 0, fs)
    load_t(0).wait()
    for u in range(z_size):
        t_own(0, u)
    wx_copy(1, 0).start()
    from_x(0, (0,))
    relay(0, 1, (0,), (0,))
    t_pass(0, 0)
    t_pass(0, 1)
    relay(0, 1, (0,), (1,))
    relay(0, 1, (1,), (0,))
    t_pass(0, 2)
    relay(0, 2, (0,), (0,))
    t_pass(0, 3)
    for m in range(2):
        wx_copy(m, 1).start()
    load_t(1).wait()
    t_own(1, 0)
    t_own(1, 1)
    t_diagonal(0, 0)
    t_diagonal(0, 1)
    relay(0, 2, (1,), (0,))
    from_x(0, (1,))
    relay(0, 2, (0,), (1,))
    for m in range(2):
        load_w(m, 1).wait()
        spread_at(m, 1, fs, True)
    t_diagonal(0, 2)
    t_diagonal(0, 3)
    relay(0, 1, (1,), (1,))
    settle(0, 0, 1, z_size)
    t_mate(0)
    earlier_hidden(0)
    t_pass(1, 0)
    t_own(1, 2)
    relay(0, 2, (1,), (1,))
    from_x_at(1, (0, 1), True)
    spread_at(0, 1, fs, False)
    from_x_at(1, (0,), False)
    t_pass(1, 1)
    t_own(1, 3)
    t_diagonal(1, 0)
    t_mate(1, 0)
    term_step(1, 0, 0)
    relay(1, 1, (0,), (0,))
    t_pass(1, 2)
    t_diagonal(1, 1)
    t_mate(1, 1)
    term_step(1, 0, 1)
    relay(1, 1, (1,), (0,))
    spread_at(1, 1, fs, False)
    from_x_at(1, (1,), False)
    t_pass(1, 3)
    load_t(2).wait()
    for u in range(z_size):
        t_own(2, u)
    t_diagonal(1, 2)
    t_mate(1, 2)
    term_step(1, 0, 2)
    reduce_step(0, 0, 1, True)
    t_diagonal(1, 3)
    t_mate(1, 3)
    settle(0, 1, 1, z_size)
    earlier_pre_grad(0)
    t_pass(2, 0)
    relay(1, 2, (0, 1), (0,))
    over(0, z_size, lambda i: term_step(0, 0, i))
    t_pass(2, 1)
    relay(1, 1, (0, 1), (1,))
    reduce_step(0, 1, 1, True)
    term_step(1, 0, last)
    t_pass(2, 2)
    t_diagonal(2, 0)
    t_pass(2, 3)
    t_diagonal(2, 1)
    t_mate_blocks()
    later_hidden(0, 0, 3)
    settle(1, 0, 1, z_size)
    later_hidden(1, 0, 3)
    relay(1, 2, (0, 1), (1,))
    reduce_step(0, 0, 1, False)
    t_diagonal(2, 2)
    t_diagonal(2, 3)
    t_mate_diagonal()
    for h in range(2):
        later_hidden(h, 3, 4)
    reduce_step(0, 0, 0, True)
    settle(1, 1, 1, last)
    partial(1, 2, 1, 0)
    partial(1, 2, 1, 1)
    q_first(1, 0)
    q_rest(1, 0)
    earlier_hidden(1)
    q_first(1, 1)
    q_rest(1, 1)
    term_step(1, 1, 0)
    over(2, last, lambda i: partial(1, 2, 1, i))
    term_step(1, 1, 1)
    q_first(1, 2)
    over(2, z_size, lambda i: term_step(1, 1, i))
    q_second_x(1, 0)
    for m in range(2):
        totals[m].wait()
    finish_at(0, 1, False)
    reduce_step(0, 1, 0, True)
    settle(1, 1, last, z_size)
    partial(1, 2, 1, last)
    q_second_x(1, 1)
    reduce_step(0, 0, 0, False)
    earlier_pre_grad(1)
    q_first(1, last)
    q_rest(1, 2)
    over(0, z_size, lambda i: term_step(0, 1, i))
    q_second_x(1, 2)
    finish_at(0, 1, True)
    reduce_step(1, 0, 1, True)
    partial(0, 0, 0, 0)
    over(1, z_size, lambda i: partial(0, 0, 0, i), lambda i: q_first(0, i - 1))
    reduce_step(1, 1, 1, True)
    q_second_x(1, last)
    q_first(0, last)
    q_rest(1, last)
    over(0, z_size, lambda i: q_second_y(1, i))
    over(0, z_size, lambda i: q_rest(0, i))
    finish(0, 0)
    reduce_step(1, 0, 1, False)
    over(0, last, lambda i: q_second_x(0, i))
    finish(1, 1)
    reduce_step(1, 0, 0, True)
    q_second_x(0, last)
    over(0, z_size, lambda i: q_second_y(0, i))
    reduce_step(1, 1, 0, True)
    reduce_step(1, 0, 0, False)
    finish_x(0, 1)
    q_last(1)
    finish(1, 0)
    finish_x(0, 0)
    finish_x(1, 1)
    q_last(0)
    finish_x(1, 0)

    def sent(ref, semaphore):
        remote(ref, ref, semaphore, f_r.at[0, 0], mate).wait_send()

    four = wts.at[0, 0, pl.ds(0, 2 * chunks * blk), :]
    sent(four, wx_s)
    sent(four, f_s)
    for m in range(2):
        pltpu.make_async_copy(outs[m], outs[m], o_s.at[m]).wait()
        for h in range(chunks):
            for way in range(2):
                for hops_left in range(1, z_size):
                    @pl.when((last - z if way == 0 else z) == hops_left)
                    def _():
                        sent(wts.at[m, h, pl.ds(0, (z_size - hops_left) * zrows), :], wz_s.at[way, m, h])
                        sent(grads.at[m, h, pl.ds(0, hops_left * zrows), :], g_s.at[way, m, h])
    for a in range(3):
        sent(tok.at[a, pl.ds(0, 7 * rows_dev), :], t_s.at[a])
    for a in range(2):
        store_out(a).wait()
        sent(part.at[a, pl.ds(0, 4 * rows_dev), :], d_s.at[a])
        sent(part.at[a, pl.ds(0, 3 * rows_dev), :], q_s.at[a])


def plane_call(n, factor, *args):
    rows_dev, depth = args[0].shape
    blk, width = args[3].shape
    z_size, chunks, rows = n // 2, 2, rows_dev * 8
    cw = width // 2 // chunks
    low, high = rows_dev * 3 // 8 // 16 * 16, rows_dev - rows_dev * 2 // 8 // 16 * 16
    dma = pltpu.SemaphoreType.DMA
    hbm = pl.BlockSpec(memory_space=pltpu.HBM)
    return pl.pallas_call(
        functools.partial(plane_kernel, n, chunks, factor),
        out_shape=(
            jax.ShapeDtypeStruct((rows_dev, depth), BF16),
            jax.ShapeDtypeStruct((rows_dev, depth), BF16),
            jax.ShapeDtypeStruct((blk, width), F32),
            jax.ShapeDtypeStruct((blk, width), F32),
        ),
        in_specs=[hbm] * 7,
        out_specs=(hbm,) * 4,
        scratch_shapes=[
            pltpu.VMEM((3, rows, depth), BF16),
            pltpu.VMEM((2, chunks, depth, cw), BF16),
            pltpu.VMEM((rows, cw), F32),
            pltpu.VMEM((3, chunks, rows, cw), BF16),
            pltpu.VMEM((2, chunks, depth, cw), BF16),
            pltpu.VMEM((2, chunks, z_size + 1, 2, blk, cw), BF16),
            pltpu.VMEM((2, chunks, blk, cw), BF16),
            pltpu.VMEM((2, chunks, blk, cw), BF16),
            pltpu.VMEM((2, rows, depth), BF16),
            pltpu.VMEM((2, 4, rows_dev, depth), BF16),
            pltpu.VMEM((2, 3, low, depth), BF16),
            pltpu.VMEM((2, 3, high, depth), BF16),
            pltpu.VMEM((2, rows_dev, depth), BF16),
            pltpu.VMEM((2, blk, width), F32),
            dma((2 * chunks + 5,)), dma((4,)), dma((3,)), dma((3, 5, z_size)), dma, dma((2, 2, chunks)), dma((2, chunks, n)),
            dma((2, 2, chunks)), dma((2, chunks, z_size + 1, 2)), dma, dma((2, chunks)),
            dma((2,)), dma((2, z_size)), dma((2,)), dma((2, 2, z_size)), dma((2,)),
        ],
        compiler_params=pltpu.CompilerParams(
            collective_id=0, has_side_effects=True, vmem_limit_bytes=67043328
        ),
        name="feed_forward_planes",
    )(*args)


def hand_on_kernel(*refs):
    count = (len(refs) - 2) // 3
    ins, outs, held, in_s, out_s = refs[:count], refs[count:2 * count], refs[2 * count:-2], refs[-2], refs[-1]
    loads, stores = [], []
    for a, (src, kept, dst) in enumerate(zip(ins, held, outs)):
        half = src.shape[0] // 2
        for i in range(2):
            o = pl.ds(i * half, half)
            loads.append(pltpu.make_async_copy(src.at[o, :], kept.at[o, :], in_s.at[a, i]))
            stores.append(pltpu.make_async_copy(kept.at[o, :], dst.at[o, :], out_s.at[a]))
    for load in loads:
        load.start()
    for load, store in zip(loads, stores):
        load.wait()
        store.start()
    for a, (kept, dst) in enumerate(zip(held, outs)):
        pltpu.make_async_copy(kept, dst, out_s.at[a]).wait()


def hand_on(*arrays):
    count = len(arrays)
    hbm = pl.BlockSpec(memory_space=pltpu.HBM)
    return pl.pallas_call(
        hand_on_kernel,
        out_shape=tuple(jax.ShapeDtypeStruct(a.shape, a.dtype) for a in arrays),
        in_specs=[hbm] * count,
        out_specs=(hbm,) * count,
        scratch_shapes=[*(pltpu.VMEM(a.shape, a.dtype) for a in arrays),
                        pltpu.SemaphoreType.DMA((count, 2)), pltpu.SemaphoreType.DMA((count,))],
        compiler_params=pltpu.CompilerParams(vmem_limit_bytes=67043328),
        name="feed_forward_results",
    )(*arrays)


def ring_call(n, m, *args):
    rows_dev, depth = args[0].shape
    blk, width = args[3].shape
    rows, half, y_size = rows_dev * m, n // 2, m // 2
    dma = pltpu.SemaphoreType.DMA
    vmem = pl.BlockSpec(memory_space=pltpu.VMEM)
    sums = max(y_size - 1, 1)
    parts = 2 if width % 256 == 0 else 1
    return pl.pallas_call(
        functools.partial(kernel, n, m, parts),
        out_shape=(
            jax.ShapeDtypeStruct((rows_dev, depth), BF16),
            jax.ShapeDtypeStruct((rows_dev, depth), BF16),
            jax.ShapeDtypeStruct((blk, width), BF16),
            jax.ShapeDtypeStruct((blk, width), BF16),
        ),
        in_specs=[vmem] * 5,
        out_specs=(vmem,) * 4,
        scratch_shapes=[
            pltpu.VMEM((3, rows, depth), BF16),
            pltpu.VMEM((2, depth, width), BF16),
            pltpu.VMEM((3, rows, width), F32),
            pltpu.VMEM((3, rows, width), BF16),
            pltpu.VMEM((2, depth, width), BF16),
            pltpu.VMEM((4, half, blk, width), BF16),
            pltpu.VMEM((2, rows, depth), BF16),
            pltpu.VMEM((2, y_size, rows_dev, depth), BF16),
            pltpu.VMEM((2, sums, rows_dev, depth), BF16),
            dma((3, y_size)), dma((3, y_size)), dma((3, y_size)), dma((3, y_size)),
            *[dma((4, half, parts))] * 4,
            dma((2, y_size)), dma((2, y_size)), dma((2, sums)), dma((2, sums)),
        ],
        compiler_params=pltpu.CompilerParams(
            collective_id=0, has_side_effects=True, vmem_limit_bytes=67043328
        ),
        name="feed_forward_step",
    )(*args)


def body(n, m, later_rows, earlier_rows, cotangent, up_weight, down_weight, up_total, down_total):
    rows = later_rows.shape[0] * m
    factor = 1.0 / math.sqrt(rows * n)
    width = up_weight.shape[1]
    planar = columns_of(n) == 2 and n == 8 and m == 4 and width % 1024 == 0 and rows % 512 == 0
    planes = (later_rows, earlier_rows, cotangent, up_weight, down_weight)
    if planar:
        return tuple(hand_on(*plane_call(n, factor, *planes, up_total, down_total)))
    later_out, earlier_grad, up_term, down_term = ring_call(n, m, *planes)
    up_updated = up_total + up_term.astype(F32) * factor
    down_updated = down_total + down_term.astype(F32) * factor
    return later_out, earlier_grad, up_updated, down_updated


def solution(mesh):
    return jax.shard_map(
        functools.partial(body, mesh.shape["fs"], mesh.shape["tp"]),
        mesh=mesh,
        in_specs=(
            P(("fs", "tp"), None),
            P(("fs", "tp"), None),
            P(("fs", "tp"), None),
            P("fs", "tp"),
            P("fs", "tp"),
            P("fs", "tp"),
            P("fs", "tp"),
        ),
        out_specs=(P(("fs", "tp"), None), P(("fs", "tp"), None), P("fs", "tp"), P("fs", "tp")),
        check_vma=False,
    )
```

```python
import functools
import math

import jax
import jax.numpy as jnp
from jax import lax
from jax.experimental import pallas as pl
from jax.experimental.pallas import tpu as pltpu
from jax.sharding import PartitionSpec as P

MESH = pl.DeviceIdType.MESH
BF16 = jnp.bfloat16
F32 = jnp.float32


def columns_of(n):
    best = 1
    for x in range(1, n + 1):
        if n % x == 0 and 2 * x * x <= n and (n // x) % 2 == 0:
            best = x
    return best


def ring_to_fs(p, n, x_size):
    if x_size == 1:
        return p
    z_size, wide = n // x_size, x_size - 1
    body = z_size * wide
    z, r = p // wide, p % wide
    x = 1 + jnp.where(z % 2 == 0, r, wide - 1 - r)
    back = z_size - 1 - (p - body)
    return jnp.where(p < body, z * x_size + x, back * x_size)


def fs_to_ring(f, n, x_size):
    if x_size == 1:
        return f
    z_size, wide = n // x_size, x_size - 1
    z, x = f // x_size, f % x_size
    r = jnp.where(z % 2 == 0, x - 1, x_size - 1 - x)
    return jnp.where(x == 0, z_size * wide + z_size - 1 - z, z * wide + r)


def kernel(n, m, parts,
           later_ref, earlier_ref, cot_ref, up_ref, down_ref,
           later_out, earlier_out, up_out, down_out,
           tok, wts, acc, hid, grads, rbuf, part, dbuf, ybuf,
           ty_s, ty_r, td_s, td_r, w_s, w_r, g_s, g_r, od_s, od_r, oy_s, oy_r):
    rows_dev, depth = later_ref.shape
    blk, width = up_ref.shape
    rows = rows_dev * m
    half, y_size = n // 2, m // 2
    aligned = blk % 128 == 0
    wide_q = width // parts
    fs, tp = lax.axis_index("fs"), lax.axis_index("tp")
    x_size = columns_of(n)
    pos = fs_to_ring(fs, n, x_size)
    y, c = tp // 2, tp % 2

    def at_ring(p):
        return ring_to_fs((p + 2 * n) % n, n, x_size)

    right = {"fs": at_ring(pos + 1), "tp": tp}
    left = {"fs": at_ring(pos - 1), "tp": tp}
    mate = {"fs": fs, "tp": y * 2 + 1 - c}
    y_next = {"fs": fs, "tp": ((y + 1) % y_size) * 2 + c}
    y_prev = {"fs": fs, "tp": ((y + y_size - 1) % y_size) * 2 + c}

    barrier = pltpu.get_barrier_semaphore()
    for other in (right, left, mate, y_next, y_prev):
        pl.semaphore_signal(barrier, inc=1, device_id=other, device_id_type=MESH)
    pl.semaphore_wait(barrier, 5)

    def remote(src, dst, send, recv, to):
        return pltpu.make_async_remote_copy(
            src_ref=src, dst_ref=dst, send_sem=send, recv_sem=recv, device_id=to, device_id_type=MESH)

    def trows(a, t):
        return tok.at[a, pl.ds(pl.multiple_of(t * rows_dev, rows_dev), rows_dev), :]

    own_w, own_t = (up_ref, down_ref), (earlier_ref, cot_ref, later_ref)

    arr_of, sign_of = (0, 1, 1, 0), (1, -1, 1, -1)

    def cut(q):
        return pl.ds(q * wide_q, wide_q)

    def w_copy(k, s, q, first=False):
        f = at_ring(pos - sign_of[k] * s)
        there = wts.at[arr_of[k], pl.ds(pl.multiple_of(f * blk, blk), blk), cut(q)]
        src = own_w[arr_of[k]].at[:, cut(q)] if first else there
        return remote(src, there, w_s.at[k, s, q], w_r.at[k, s, q], right if sign_of[k] > 0 else left)

    def ty_copy(a, s, first=False):
        t = ((y + y_size - s) % y_size) * 2 + c
        return remote(own_t[a] if first else trows(a, t), trows(a, t), ty_s.at[a, s], ty_r.at[a, s], y_next)

    def td_copy(a, s, first=False):
        t = ((y + y_size - s) % y_size) * 2 + c
        return remote(own_t[a] if first else trows(a, t), trows(a, t), td_s.at[a, s], td_r.at[a, s], mate)

    every = tuple((k, q) for pair in ((0, 1), (2, 3)) for q in range(parts) for k in pair)
    longs = tuple((k, q) for k, q in every if k < 2)
    for k, q in every:
        w_copy(k, 0, q, True).start()
    for a in range(3):
        if y_size > 1:
            ty_copy(a, 0, True).start()
    for a in range(3):
        td_copy(a, 0, True).start()

    def put(dst, dst_row, src, count):
        step = math.gcd(count, 64)

        @pl.loop(0, count // step)
        def _(i):
            o = pl.multiple_of(i * step, step)
            dst[pl.ds(pl.multiple_of(dst_row + o, step), step), :] = src[pl.ds(o, step), :]

    for a in range(2):
        put(wts.at[a], fs * blk, own_w[a], blk)
    for a in range(3):
        put(tok.at[a], tp * rows_dev, own_t[a], rows_dev)

    tile = math.gcd(wide_q, 256)

    def multiply(a, w, rows_w, clear, q=None):
        first, count = (0, width) if q is None else (q * wide_q, wide_q)

        @pl.loop(0, count // tile)
        def _(j):
            o = pl.ds(pl.multiple_of(first + j * tile, tile), tile)
            got = jnp.dot(tok[a, :, rows_w], wts[w, rows_w, o], preferred_element_type=F32)
            if clear:
                acc[a, :, o] = got
            else:
                acc[a, :, o] += got

    def use(w, f, clear=False, q=None):
        if not aligned:
            return
        o = pl.ds(pl.multiple_of(f * blk, blk), blk)
        for a in ((0, 2) if w == 0 else (1,)):
            multiply(a, w, o, clear, q)

    def forward(s, present, go):
        for k, q in present:
            w_copy(k, s - 1, q).wait_recv()
            if (k, q) in go:
                w_copy(k, s, q).start()

    def use_step(s):
        for k in range(4):
            use(arr_of[k], at_ring(pos - sign_of[k] * s))

    forward(1, every, every if half > 2 else longs)
    for s in range(1, y_size):
        for a in range(3):
            ty_copy(a, s - 1).wait_recv()
            if s < y_size - 1:
                ty_copy(a, s).start()
            td_copy(a, s).start()
    for s in range(y_size):
        for a in range(3):
            td_copy(a, s).wait_recv()
    for w in range(2):
        use(w, fs, True)
    if half > 3:
        @pl.loop(2, half - 1)
        def _(s):
            forward(s, every, every)
            use_step(s - 1)
    if half > 2:
        forward(half - 1, every, longs)
        use_step(half - 2)
    use_step(half - 1)

    step_r = math.gcd(rows, 32)

    def activate(q):
        @pl.loop(0, rows // step_r)
        def _(i):
            o = pl.ds(pl.multiple_of(i * step_r, step_r), step_r)
            relu = jnp.maximum(acc[0, o, cut(q)], 0.0)
            hid[0, o, cut(q)] = (2.0 * relu * acc[1, o, cut(q)]).astype(BF16)
            hid[1, o, cut(q)] = (relu * relu).astype(BF16)

    def term(a, row, size, q=None):
        first, count = (0, width) if q is None else (q * wide_q, wide_q)

        @pl.loop(0, count // tile)
        def _(j):
            o = pl.ds(pl.multiple_of(first + j * tile, tile), tile)
            grads[a, pl.ds(row, size), o] = lax.dot_general(
                tok[a, :, pl.ds(row, size)], hid[a, :, o], (((0,), (0,)), ((), ())),
                preferred_element_type=F32).astype(BF16)

    def block_term(a, p, q=None):
        term(a, pl.multiple_of(at_ring(p) * blk, blk), blk, q)

    def g_copy(k, s, q):
        d = half - (k >= 2) - s
        f = at_ring(pos + sign_of[k] * d)
        src = grads.at[arr_of[k], pl.ds(pl.multiple_of(f * blk, blk), blk), cut(q)]
        return remote(src, rbuf.at[k, s, :, cut(q)], g_s.at[k, s, q], g_r.at[k, s, q],
                      right if sign_of[k] > 0 else left)

    def add_rows(dst, dst_row, src, count, columns=slice(None)):
        step = math.gcd(count, 32)

        @pl.loop(0, count // step)
        def _(i):
            o = pl.multiple_of(i * step, step)
            at = pl.ds(pl.multiple_of(dst_row + o, step), step)
            total = dst[at, columns].astype(F32) + src[pl.ds(o, step), columns].astype(F32)
            dst[at, columns] = total.astype(BF16)

    def g_step(s, which):
        for k, q in which:
            g_copy(k, s - 1, q).wait_recv()
            f = at_ring(pos + sign_of[k] * (half - (k >= 2) - s))
            add_rows(grads.at[arr_of[k]], f * blk, rbuf.at[k, s - 1], blk, cut(q))
            g_copy(k, s, q).start()

    wide = math.gcd(depth, 256)
    for q in range(parts):
        for k in (0, 1):
            w_copy(k, half - 1, q).wait_recv()
            use(arr_of[k], at_ring(pos - sign_of[k] * half), q=q)
        if not aligned:
            full = pl.ds(0, depth)
            for a, w in ((0, 0), (1, 1), (2, 0)):
                multiply(a, w, full, True, q)
        activate(q)
        if not aligned:
            for a in range(2):
                @pl.loop(0, depth // wide)
                def _(i):
                    term(a, pl.multiple_of(i * wide, wide), wide, q)
        for k in (0, 1):
            if aligned:
                block_term(arr_of[k], pos + sign_of[k] * half, q)
            g_copy(k, 0, q).start()
    for k in (2, 3):
        if aligned:
            block_term(arr_of[k], pos + sign_of[k] * (half - 1))
        for q in range(parts):
            g_copy(k, 0, q).start()
    if aligned:
        if half > 1:
            @pl.loop(0, half - 1)
            def _(i):
                d = half - 1 - i
                block_term(0, pos + d)
                block_term(1, pos - d)
        if half > 2:
            @pl.loop(0, half - 2)
            def _(i):
                d = half - 2 - i
                block_term(1, pos + d)
                block_term(0, pos - d)
        for a in range(2):
            block_term(a, pos)

    @pl.loop(0, rows // step_r)
    def _(i):
        o = pl.ds(pl.multiple_of(i * step_r, step_r), step_r)
        relu = jnp.maximum(acc[2, o, :], 0.0)
        hid[2, o, :] = (relu * relu).astype(BF16)

    wide_d = math.gcd(depth, 256)

    def partial(a, h, w):
        @pl.loop(0, depth // wide_d)
        def _(j):
            o = pl.ds(pl.multiple_of(j * wide_d, wide_d), wide_d)
            part[a, :, o] = lax.dot_general(
                hid[h], wts[w, o, :], (((1,), (1,)), ((), ())), preferred_element_type=F32).astype(BF16)

    def prow(yy, cc):
        return pl.multiple_of((yy * 2 + cc) * rows_dev, rows_dev)

    def od_copy(a, yy):
        return remote(part.at[a, pl.ds(prow(yy, 1 - c), rows_dev), :], dbuf.at[a, yy],
                      od_s.at[a, yy], od_r.at[a, yy], mate)

    def oy_copy(a, s):
        t = (y + y_size - 1 - s) % y_size
        return remote(part.at[a, pl.ds(prow(t, c), rows_dev), :], ybuf.at[a, s],
                      oy_s.at[a, s], oy_r.at[a, s], y_next)

    def send_partial(a, h, w):
        partial(a, h, w)
        for yy in range(y_size):
            od_copy(a, yy).start()

    send_partial(0, 0, 0)
    g_step(1, every if half > 2 else longs)
    send_partial(1, 2, 1)
    for a in range(2):
        for yy in range(y_size):
            od_copy(a, yy).wait_recv()
            add_rows(part.at[a], prow(yy, c), dbuf.at[a, yy], rows_dev)
        if y_size > 1:
            oy_copy(a, 0).start()
    if half - 1 > 2:
        @pl.loop(2, half - 1)
        def _(s):
            g_step(s, every)
    for s in range(1, y_size):
        for a in range(2):
            oy_copy(a, s - 1).wait_recv()
            t = (y + y_size - 1 - s) % y_size
            add_rows(part.at[a], prow(t, c), ybuf.at[a, s - 1], rows_dev)
            if s < y_size - 1:
                oy_copy(a, s).start()
    put_own = ((earlier_out, 0), (later_out, 1))
    for out, a in put_own:
        out[...] = part[a, pl.ds(prow(y, c), rows_dev), :]
    if half - 1 >= 2:
        g_step(half - 1, longs)

    ends = [(k, half - 1 - (k >= 2)) for k in range(4)]
    for k, q in tuple((k, q) for k, q in every if k >= 2) + longs:
        g_copy(k, ends[k][1], q).wait_recv()
    step_b = math.gcd(blk, 32)
    for a, out in ((0, up_out), (1, down_out)):
        @pl.loop(0, blk // step_b)
        def _(i):
            lo = pl.multiple_of(i * step_b, step_b)
            o = pl.ds(lo, step_b)
            got = grads[a, pl.ds(pl.multiple_of(fs * blk + lo, step_b), step_b), :].astype(F32)
            for k, s in ends:
                if arr_of[k] == a:
                    got += rbuf[k, s, o, :].astype(F32)
            out[o, :] = got.astype(BF16)

    for k, q in every:
        for s in range(half - (k >= 2)):
            w_copy(k, s, q).wait_send()
            g_copy(k, s, q).wait_send()
    for a in range(3):
        for s in range(y_size):
            if s < y_size - 1:
                ty_copy(a, s).wait_send()
            td_copy(a, s).wait_send()
    for a in range(2):
        for yy in range(y_size):
            od_copy(a, yy).wait_send()
        for s in range(y_size - 1):
            oy_copy(a, s).wait_send()


def plane_kernel(n, chunks, factor,
                 later_ref, earlier_ref, cot_ref, up_ref, down_ref, up_total, down_total,
                 later_out, earlier_out, up_out, down_out,
                 tok, wts, act, hid, grads, gbuf, fin, xbuf, part, dbuf, qa, qb, stage, sums,
                 l_s, o_s, t_s, t_r, wx_s, wz_s, w_r, g_s, g_r, f_s, f_r, d_s, d_r, q_s, q_r, q_l):
    rows_dev, depth = later_ref.shape
    blk, width = up_ref.shape
    z_size, zrows = n // 2, 2 * blk
    wide, cw = width // 2, width // 2 // chunks
    chip_rows = 2 * rows_dev
    fs, tp = lax.axis_index("fs"), lax.axis_index("tp")
    z, x, y, c = fs // 2, fs % 2, tp // 2, tp % 2
    last = z_size - 1
    side = 2 * z // z_size
    span = 2 * blk

    right = {"fs": ((z + 1) % z_size) * 2 + x, "tp": tp}
    left = {"fs": ((z + last) % z_size) * 2 + x, "tp": tp}
    x_next = {"fs": z * 2 + 1 - x, "tp": tp}
    y_next = {"fs": fs, "tp": (1 - y) * 2 + c}
    mate = {"fs": fs, "tp": y * 2 + 1 - c}

    def block_at(xx, yy, cc):
        return ((xx * 2 + yy) * 2 + cc) * rows_dev

    def rows_at(start, count):
        return pl.ds(pl.multiple_of(start, math.gcd(count, 128)), count)

    def columns_at(xx, h):
        return pl.ds(pl.multiple_of(xx * wide + h * cw, cw), cw)

    own_w, own_t = (up_ref, down_ref), (earlier_ref, cot_ref, later_ref)

    def load_w(m, h):
        return pltpu.make_async_copy(
            own_w[m].at[:, columns_at(x, h)], wts.at[m, h, rows_at(fs * blk, blk), :], l_s.at[m * chunks + h])

    def load_t(a):
        return pltpu.make_async_copy(
            own_t[a], tok.at[a, rows_at(block_at(x, y, c), rows_dev), :], l_s.at[2 * chunks + a])

    for m in range(2):
        load_w(m, 0).start()
    load_t(0).start()
    load_t(1).start()
    for m in range(2):
        load_w(m, 1).start()
    load_t(2).start()
    totals = tuple(
        pltpu.make_async_copy(total, sums.at[m], l_s.at[2 * chunks + 3 + m])
        for m, total in enumerate((up_total, down_total)))
    for m in range(2):
        totals[m].start()

    barrier = pltpu.get_barrier_semaphore()
    for other in (right, left, x_next, y_next, mate):
        pl.semaphore_signal(barrier, inc=1, device_id=other, device_id_type=MESH)
    pl.semaphore_wait(barrier, 5)

    def remote(src, dst, send, recv, to):
        return pltpu.make_async_remote_copy(
            src_ref=src, dst_ref=dst, send_sem=send, recv_sem=recv, device_id=to, device_id_type=MESH)

    def piece(m, h, f):
        return wts.at[m, h, rows_at(f * blk, blk), :]

    def wx_copy(m, h):
        return remote(own_w[m].at[:, columns_at(1 - x, h)], piece(m, h, fs), wx_s, w_r.at[m, h, fs], x_next)

    def wz_copy(m, h, f, way):
        return remote(piece(m, h, f), piece(m, h, f), wz_s.at[way, m, h], w_r.at[m, h, f], left if way else right)

    def w_got(m, h, f):
        wz_copy(m, h, f, 0).wait_recv()

    def spread(m, h, f):
        @pl.when(z < last)
        def _():
            wz_copy(m, h, f, 0).start()

        @pl.when(z > 0)
        def _():
            wz_copy(m, h, f, 1).start()

    def spread_at(m, h, f, ends):
        @pl.when((z == 0) | (z == last) if ends else (z > 0) & (z < last))
        def _():
            spread(m, h, f)

    def from_x(h, ms=(0, 1)):
        for m in ms:
            w_got(m, h, z * 2 + 1 - x)
            spread(m, h, z * 2 + 1 - x)

    def from_x_at(h, ms, ends):
        @pl.when((z == 0) | (z == last) if ends else (z > 0) & (z < last))
        def _():
            from_x(h, ms)

    def relay(h, d, columns=(0, 1), ms=(0, 1)):
        for m in ms:
            for p in columns:
                p = (x + p) % 2

                @pl.when((z >= d) & (z < last))
                def _():
                    w_got(m, h, (z - d) * 2 + p)
                    wz_copy(m, h, (z - d) * 2 + p, 0).start()

                @pl.when((z + d < z_size) & (z > 0))
                def _():
                    w_got(m, h, (z + d) * 2 + p)
                    wz_copy(m, h, (z + d) * 2 + p, 1).start()

    def settle(h, m, lo, hi):
        @pl.when((z == 0) | (z == last))
        def _():
            @pl.loop(lo, hi)
            def _(d):
                for p in range(2):
                    w_got(m, h, jnp.where(z == 0, d, last - d) * 2 + p)

    def moves(cut_t):
        return (
            (x, y, 0, rows_dev, x_next),
            (x, y, 0, rows_dev, y_next),
            (1 - x, y, 0, cut_t, y_next),
            (x, 1 - y, cut_t, rows_dev - cut_t, x_next),
            (x, y, 0, rows_dev, mate),
            (1 - x, y, 0, rows_dev, mate),
            (x, 1 - y, 0, rows_dev, mate),
            (1 - x, 1 - y, 0, cut_t, mate),
            (1 - x, 1 - y, cut_t, rows_dev - cut_t, mate),
        )

    cuts = tuple(rows_dev * part // 8 // 16 * 16 for part in (7, 5, 4))

    def facing(i):
        return (1 - side) * (last - i) + side * i

    def t_ref(a, start, count, u):
        return tok.at[a, rows_at(start, count), slice(None) if u is None else rows_at(facing(u) * span, span)]

    def t_got(a, k, u):
        slot = u if k < 4 or a == 1 else k // 7 if a == 2 else 0
        return t_r.at[a, min(k, 4), slot]

    def t_copy(a, k, u):
        xx, yy, lo, count, to = moves(cuts[a])[k]
        there = t_ref(a, block_at(xx, yy, c) + lo, count, u)
        return remote(there, there, t_s.at[a], t_got(a, k, u), to)

    def t_own(a, u):
        for k in (0, 1, 4):
            t_copy(a, k, u).start()

    def t_pass(a, u):
        t_copy(a, 1, u).wait_recv()
        t_copy(a, 3, u).start()
        t_copy(a, 6, u).start()
        t_copy(a, 0, u).wait_recv()
        t_copy(a, 2, u).start()
        t_copy(a, 5, u).start()

    def t_diagonal(a, u):
        t_copy(a, 2, u).wait_recv()
        t_copy(a, 7, u).start()
        t_copy(a, 3, u).wait_recv()
        t_copy(a, 8, u).start()

    def t_mate(a, u=None):
        there = t_ref(a, 0, 4 * rows_dev, u)
        remote(there, there, t_s.at[a], t_got(a, 4, u), mate).wait_recv()

    def t_mate_blocks():
        there = t_ref(2, 0, 3 * rows_dev, None)
        remote(there, there, t_s.at[2], t_got(2, 4, None), mate).wait_recv()

    def t_mate_diagonal():
        there = t_ref(2, 0, rows_dev, None)
        remote(there, there, t_s.at[2], t_got(2, 7, None), mate).wait_recv()

    def earlier_hidden(h):
        @pl.loop(0, 4)
        def _(i):
            o = rows_at(i * chip_rows, chip_rows)
            relu = jnp.maximum(jnp.dot(tok[0, o, :], wts[0, h], preferred_element_type=F32), 0.0)
            act[o, :] = relu
            hid[1, h, o, :] = (relu * relu).astype(BF16)

    def earlier_pre_grad(h):
        @pl.loop(0, 4)
        def _(i):
            o = rows_at(i * chip_rows, chip_rows)
            got = jnp.dot(tok[1, o, :], wts[1, h], preferred_element_type=F32)
            hid[0, h, o, :] = (2.0 * act[o, :] * got).astype(BF16)

    def chip_at(i):
        return (((x + i % 2) % 2) * 2 + (y + i // 2) % 2) * chip_rows

    def later_hidden(h, lo, hi):
        @pl.loop(lo, hi)
        def _(i):
            o = rows_at(chip_at(i), chip_rows)
            relu = jnp.maximum(jnp.dot(tok[2, o, :], wts[0, h], preferred_element_type=F32), 0.0)
            hid[2, h, o, :] = (relu * relu).astype(BF16)

    def term(m, h, d):
        o = rows_at(d * zrows, zrows)
        grads[m, h, o, :] = lax.dot_general(
            tok[m, :, o], hid[m, h], (((0,), (0,)), ((), ())), preferred_element_type=F32).astype(BF16)

    def half_at(d, half):
        return d * zrows + (x + 1 - half) % 2 * blk

    def g_copy(m, h, d, way, half):
        src = grads.at[m, h, rows_at(half_at(d, half), blk), :]
        to = {"fs": ((z + z_size + 1 - 2 * way) % z_size) * 2 + x, "tp": tp}
        slot = d + 1 - way
        return remote(src, gbuf.at[m, h, slot, half], g_s.at[way, m, h], g_r.at[m, h, slot, half], to)

    def term_step(m, h, i):
        d = facing(i)
        term(m, h, d)

        @pl.when(((z == 0) | (z == last)) & (i < last))
        def _():
            for half in range(2):
                g_copy(m, h, d, side, half).start()

    def add_rows(dst, dst_row, src, count, columns=slice(None)):
        step = math.gcd(count, 32)

        @pl.loop(0, count // step)
        def _(i):
            o = pl.multiple_of(i * step, step)
            at = pl.ds(pl.multiple_of(dst_row + o, math.gcd(step, 16)), step)
            dst[at, columns] = (dst[at, columns].astype(F32) + src[pl.ds(o, step), columns].astype(F32)).astype(BF16)

    def reduce_step(h, k, m, near):
        way = side if near else 1 - side
        d = (1 - way) * (last - k) + way * k
        beyond = (1 - 2 * way) * (d - z)
        behind = (1 - way) * z + way * (last - z)

        @pl.when((beyond > 0) & (behind > 0))
        def _():
            for half in range(2):
                g_copy(m, h, d, way, half).wait_recv()
                add_rows(grads.at[m, h], half_at(d, half), gbuf.at[m, h, d + 1 - way, half], blk)
                g_copy(m, h, d, way, half).start()

    outs = (up_out, down_out)

    def f_copy(m, h):
        return remote(fin.at[m, h], xbuf.at[m, h], f_s, f_r.at[m, h], x_next)

    def total(m, h, half, sources):
        step = math.gcd(blk, 32)

        @pl.loop(0, blk // step)
        def _(i):
            o = pl.multiple_of(i * step, step)
            at = pl.ds(o, step)
            got = grads[m, h, pl.ds(pl.multiple_of(half_at(z, half) + o, step), step), :].astype(F32)
            for src in sources:
                got += gbuf[m, h, z + 1 - src, half, at, :].astype(F32)
            if half:
                sums[m, at, columns_at(x, h)] += got * factor
            else:
                fin[m, h, at, :] = got.astype(BF16)

    def store_sum(m, h, xx):
        there = columns_at(xx, h)
        return pltpu.make_async_copy(sums.at[m, :, there], outs[m].at[:, there], o_s.at[m])

    def finish(h, m):
        for half in range(2):
            @pl.when(z > 0)
            def _():
                g_copy(m, h, z, 0, half).wait_recv()

            @pl.when(z < last)
            def _():
                g_copy(m, h, z, 1, half).wait_recv()

            for case, sources in ((z == 0, (1,)), (z == last, (0,)), ((z > 0) & (z < last), (0, 1))):
                @pl.when(case)
                def _():
                    total(m, h, half, sources)

            (store_sum(m, h, x) if half else f_copy(m, h)).start()

    def finish_at(h, m, ends):
        @pl.when((z == 0) | (z == last) if ends else (z > 0) & (z < last))
        def _():
            finish(h, m)

    def finish_x(h, m):
        f_copy(m, h).wait_recv()
        step = math.gcd(blk, 32)

        @pl.loop(0, blk // step)
        def _(i):
            at = pl.ds(pl.multiple_of(i * step, step), step)
            sums[m, at, columns_at(1 - x, h)] += xbuf[m, h, at, :].astype(F32) * factor

        store_sum(m, h, 1 - x).start()

    tile = math.gcd(span, 256)

    def span_at(i):
        return rows_at(((1 - side) * i + side * (last - i)) * span, span)

    def partial(a, k, w, i):
        first = ((1 - side) * i + side * (last - i)) * span

        @pl.loop(0, span // tile)
        def _(j):
            o = rows_at(first + j * tile, tile)
            got = None
            for h in range(chunks):
                one = lax.dot_general(hid[k, h], wts[w, h, o, :], (((1,), (1,)), ((), ())),
                                      preferred_element_type=F32)
                got = one if got is None else got + one
            part[a, :, o] = got.astype(BF16)

        for q in range(4):
            d_copy(a, q, i).start()

    def d_copy(a, q, i):
        return remote(part.at[a, rows_at(q * chip_rows + (1 - c) * rows_dev, rows_dev), span_at(i)],
                      dbuf.at[a, q, :, span_at(i)], d_s.at[a], d_r.at[a, i], mate)

    cuts_q = tuple(rows_dev * share // 8 // 16 * 16 for share in (2, 3))
    hops = (
        (1 - x, y, 0, qa, 0, x_next),
        (1 - x, 1 - y, 0, qa, 1, x_next),
        (x, 1 - y, 1, qb, 0, y_next),
        (1 - x, 1 - y, 1, qb, 1, y_next),
        (x, 1 - y, 0, qa, 2, y_next),
        (1 - x, y, 1, qb, 2, x_next),
    )

    def bounds(a, high):
        return (cuts_q[a], rows_dev - cuts_q[a]) if high else (0, cuts_q[a])

    def q_copy(a, k, i):
        xx, yy, high, buf, slot, to = hops[k]
        lo, count = bounds(a, high)
        return remote(part.at[a, rows_at(block_at(xx, yy, c) + lo, count), span_at(i)],
                      buf.at[a, slot, pl.ds(0, count), span_at(i)], q_s.at[a], q_r.at[a, k // 2, i] if k in (1, 3) else q_l.at[a], to)

    def q_first(a, i):
        there = dbuf.at[a, :, :, span_at(i)]
        remote(there, there, d_s.at[a], d_r.at[a, i], mate).wait_recv()
        for chip in (3, 0, 1, 2):
            start = chip_at(chip)
            add_rows(part.at[a], start + c * rows_dev, dbuf.at[a, start // chip_rows], rows_dev, span_at(i))
            if chip == 3:
                for k in (1, 3):
                    q_copy(a, k, i).start()

    def q_rest(a, i):
        for k in (0, 2):
            q_copy(a, k, i).start()

    def q_second_y(a, i):
        q_copy(a, 1, i).wait_recv()
        add_rows(part.at[a], block_at(x, 1 - y, c), qa.at[a, 1], cuts_q[a], span_at(i))
        q_copy(a, 4, i).start()

    def q_second_x(a, i):
        q_copy(a, 3, i).wait_recv()
        add_rows(part.at[a], block_at(1 - x, y, c) + cuts_q[a], qb.at[a, 1], rows_dev - cuts_q[a], span_at(i))
        q_copy(a, 5, i).start()

    def over(lo, hi, *calls):
        @pl.loop(lo, hi)
        def _(i):
            for call in calls:
                call(i)

    def store_out(a):
        return pltpu.make_async_copy(stage.at[a], (earlier_out, later_out)[a], o_s.at[2 + a])

    def q_last(a):
        there = part.at[a, pl.ds(0, 2 * rows_dev), :]
        remote(there, there, q_s.at[a], q_l.at[a], x_next).wait_recv()
        for high, buf in enumerate((qa, qb)):
            lo, count = bounds(a, high)
            step = math.gcd(count, 16)

            @pl.loop(0, count // step)
            def _(i):
                o = pl.multiple_of(i * step, step)
                at = pl.ds(o, step)
                own = pl.ds(pl.multiple_of(block_at(x, y, c) + lo + o, step), step)
                stage[a, pl.ds(pl.multiple_of(lo + o, step), step), :] = (
                    part[a, own, :].astype(F32) + buf[a, 0, at, :].astype(F32) + buf[a, 2, at, :].astype(F32)
                ).astype(BF16)

        store_out(a).start()

    wx_copy(0, 0).start()
    for m in range(2):
        load_w(m, 0).wait()
        spread(m, 0, fs)
    load_t(0).wait()
    for u in range(z_size):
        t_own(0, u)
    wx_copy(1, 0).start()
    from_x(0, (0,))
    relay(0, 1, (0,), (0,))
    t_pass(0, 0)
    t_pass(0, 1)
    relay(0, 1, (0,), (1,))
    relay(0, 1, (1,), (0,))
    t_pass(0, 2)
    relay(0, 2, (0,), (0,))
    t_pass(0, 3)
    for m in range(2):
        wx_copy(m, 1).start()
    load_t(1).wait()
    t_own(1, 0)
    t_own(1, 1)
    t_diagonal(0, 0)
    t_diagonal(0, 1)
    relay(0, 2, (1,), (0,))
    from_x(0, (1,))
    relay(0, 2, (0,), (1,))
    for m in range(2):
        load_w(m, 1).wait()
        spread_at(m, 1, fs, True)
    t_diagonal(0, 2)
    t_diagonal(0, 3)
    relay(0, 1, (1,), (1,))
    settle(0, 0, 1, z_size)
    t_mate(0)
    earlier_hidden(0)
    t_pass(1, 0)
    t_own(1, 2)
    relay(0, 2, (1,), (1,))
    from_x_at(1, (0, 1), True)
    spread_at(0, 1, fs, False)
    from_x_at(1, (0,), False)
    t_pass(1, 1)
    t_own(1, 3)
    t_diagonal(1, 0)
    t_mate(1, 0)
    term_step(1, 0, 0)
    relay(1, 1, (0,), (0,))
    t_pass(1, 2)
    t_diagonal(1, 1)
    t_mate(1, 1)
    term_step(1, 0, 1)
    relay(1, 1, (1,), (0,))
    spread_at(1, 1, fs, False)
    from_x_at(1, (1,), False)
    t_pass(1, 3)
    load_t(2).wait()
    for u in range(z_size):
        t_own(2, u)
    t_diagonal(1, 2)
    t_mate(1, 2)
    term_step(1, 0, 2)
    reduce_step(0, 0, 1, True)
    t_diagonal(1, 3)
    t_mate(1, 3)
    settle(0, 1, 1, z_size)
    earlier_pre_grad(0)
    t_pass(2, 0)
    relay(1, 2, (0, 1), (0,))
    over(0, z_size, lambda i: term_step(0, 0, i))
    t_pass(2, 1)
    relay(1, 1, (0, 1), (1,))
    reduce_step(0, 1, 1, True)
    term_step(1, 0, last)
    t_pass(2, 2)
    t_diagonal(2, 0)
    t_pass(2, 3)
    t_diagonal(2, 1)
    t_mate_blocks()
    later_hidden(0, 0, 3)
    settle(1, 0, 1, z_size)
    later_hidden(1, 0, 3)
    relay(1, 2, (0, 1), (1,))
    reduce_step(0, 0, 1, False)
    t_diagonal(2, 2)
    t_diagonal(2, 3)
    t_mate_diagonal()
    for h in range(2):
        later_hidden(h, 3, 4)
    reduce_step(0, 0, 0, True)
    settle(1, 1, 1, last)
    partial(1, 2, 1, 0)
    partial(1, 2, 1, 1)
    q_first(1, 0)
    q_rest(1, 0)
    earlier_hidden(1)
    q_first(1, 1)
    q_rest(1, 1)
    term_step(1, 1, 0)
    over(2, last, lambda i: partial(1, 2, 1, i))
    term_step(1, 1, 1)
    q_first(1, 2)
    over(2, z_size, lambda i: term_step(1, 1, i))
    q_second_x(1, 0)
    q_second_y(1, 0)
    for m in range(2):
        totals[m].wait()
    finish_at(0, 1, False)
    reduce_step(0, 1, 0, True)
    settle(1, 1, last, z_size)
    partial(1, 2, 1, last)
    q_second_x(1, 1)
    q_second_y(1, 1)
    reduce_step(0, 0, 0, False)
    earlier_pre_grad(1)
    q_first(1, last)
    q_rest(1, 2)
    over(0, z_size, lambda i: term_step(0, 1, i))
    q_second_x(1, 2)
    q_second_y(1, 2)
    finish_at(0, 1, True)
    reduce_step(1, 0, 1, True)
    partial(0, 0, 0, 0)
    over(1, z_size, lambda i: partial(0, 0, 0, i), lambda i: q_first(0, i - 1))
    reduce_step(1, 1, 1, True)
    q_second_x(1, last)
    q_first(0, last)
    q_rest(1, last)
    q_second_y(1, last)
    over(0, z_size, lambda i: q_rest(0, i))
    finish(0, 0)
    reduce_step(1, 0, 1, False)
    over(0, last, lambda i: q_second_x(0, i))
    finish(1, 1)
    reduce_step(1, 0, 0, True)
    q_second_x(0, last)
    over(0, z_size, lambda i: q_second_y(0, i))
    reduce_step(1, 1, 0, True)
    reduce_step(1, 0, 0, False)
    finish_x(0, 1)
    q_last(1)
    finish(1, 0)
    finish_x(0, 0)
    finish_x(1, 1)
    q_last(0)
    finish_x(1, 0)

    def sent(ref, semaphore):
        remote(ref, ref, semaphore, f_r.at[0, 0], mate).wait_send()

    four = wts.at[0, 0, pl.ds(0, 2 * chunks * blk), :]
    sent(four, wx_s)
    sent(four, f_s)
    for m in range(2):
        pltpu.make_async_copy(outs[m], outs[m], o_s.at[m]).wait()
        for h in range(chunks):
            for way in range(2):
                for hops_left in range(1, z_size):
                    @pl.when((last - z if way == 0 else z) == hops_left)
                    def _():
                        sent(wts.at[m, h, pl.ds(0, (z_size - hops_left) * zrows), :], wz_s.at[way, m, h])
                        sent(grads.at[m, h, pl.ds(0, hops_left * zrows), :], g_s.at[way, m, h])
    for a in range(3):
        sent(tok.at[a, pl.ds(0, 7 * rows_dev), :], t_s.at[a])
    for a in range(2):
        store_out(a).wait()
        sent(part.at[a, pl.ds(0, 4 * rows_dev), :], d_s.at[a])
        sent(part.at[a, pl.ds(0, 3 * rows_dev), :], q_s.at[a])


def plane_call(n, factor, *args):
    rows_dev, depth = args[0].shape
    blk, width = args[3].shape
    z_size, chunks, rows = n // 2, 2, rows_dev * 8
    cw = width // 2 // chunks
    low, high = rows_dev * 3 // 8 // 16 * 16, rows_dev - rows_dev * 2 // 8 // 16 * 16
    dma = pltpu.SemaphoreType.DMA
    hbm = pl.BlockSpec(memory_space=pltpu.HBM)
    return pl.pallas_call(
        functools.partial(plane_kernel, n, chunks, factor),
        out_shape=(
            jax.ShapeDtypeStruct((rows_dev, depth), BF16),
            jax.ShapeDtypeStruct((rows_dev, depth), BF16),
            jax.ShapeDtypeStruct((blk, width), F32),
            jax.ShapeDtypeStruct((blk, width), F32),
        ),
        in_specs=[hbm] * 7,
        out_specs=(hbm,) * 4,
        scratch_shapes=[
            pltpu.VMEM((3, rows, depth), BF16),
            pltpu.VMEM((2, chunks, depth, cw), BF16),
            pltpu.VMEM((rows, cw), F32),
            pltpu.VMEM((3, chunks, rows, cw), BF16),
            pltpu.VMEM((2, chunks, depth, cw), BF16),
            pltpu.VMEM((2, chunks, z_size + 1, 2, blk, cw), BF16),
            pltpu.VMEM((2, chunks, blk, cw), BF16),
            pltpu.VMEM((2, chunks, blk, cw), BF16),
            pltpu.VMEM((2, rows, depth), BF16),
            pltpu.VMEM((2, 4, rows_dev, depth), BF16),
            pltpu.VMEM((2, 3, low, depth), BF16),
            pltpu.VMEM((2, 3, high, depth), BF16),
            pltpu.VMEM((2, rows_dev, depth), BF16),
            pltpu.VMEM((2, blk, width), F32),
            dma((2 * chunks + 5,)), dma((4,)), dma((3,)), dma((3, 5, z_size)), dma, dma((2, 2, chunks)), dma((2, chunks, n)),
            dma((2, 2, chunks)), dma((2, chunks, z_size + 1, 2)), dma, dma((2, chunks)),
            dma((2,)), dma((2, z_size)), dma((2,)), dma((2, 2, z_size)), dma((2,)),
        ],
        compiler_params=pltpu.CompilerParams(
            collective_id=0, has_side_effects=True, vmem_limit_bytes=67043328
        ),
        name="feed_forward_planes",
    )(*args)


def hand_on_kernel(*refs):
    count = (len(refs) - 2) // 3
    ins, outs, held, in_s, out_s = refs[:count], refs[count:2 * count], refs[2 * count:-2], refs[-2], refs[-1]
    loads, stores = [], []
    for a, (src, kept, dst) in enumerate(zip(ins, held, outs)):
        half = src.shape[0] // 2
        for i in range(2):
            o = pl.ds(i * half, half)
            loads.append(pltpu.make_async_copy(src.at[o, :], kept.at[o, :], in_s.at[a, i]))
            stores.append(pltpu.make_async_copy(kept.at[o, :], dst.at[o, :], out_s.at[a]))
    order = sorted(range(2 * count), key=lambda i: -i)
    for i in order:
        loads[i].start()
    for i in order:
        loads[i].wait()
        stores[i].start()
    for a, (kept, dst) in enumerate(zip(held, outs)):
        pltpu.make_async_copy(kept, dst, out_s.at[a]).wait()


def hand_on(*arrays):
    count = len(arrays)
    hbm = pl.BlockSpec(memory_space=pltpu.HBM)
    return pl.pallas_call(
        hand_on_kernel,
        out_shape=tuple(jax.ShapeDtypeStruct(a.shape, a.dtype) for a in arrays),
        in_specs=[hbm] * count,
        out_specs=(hbm,) * count,
        scratch_shapes=[*(pltpu.VMEM(a.shape, a.dtype) for a in arrays),
                        pltpu.SemaphoreType.DMA((count, 2)), pltpu.SemaphoreType.DMA((count,))],
        compiler_params=pltpu.CompilerParams(vmem_limit_bytes=67043328),
        name="feed_forward_results",
    )(*arrays)


def ring_call(n, m, *args):
    rows_dev, depth = args[0].shape
    blk, width = args[3].shape
    rows, half, y_size = rows_dev * m, n // 2, m // 2
    dma = pltpu.SemaphoreType.DMA
    vmem = pl.BlockSpec(memory_space=pltpu.VMEM)
    sums = max(y_size - 1, 1)
    parts = 2 if width % 256 == 0 else 1
    return pl.pallas_call(
        functools.partial(kernel, n, m, parts),
        out_shape=(
            jax.ShapeDtypeStruct((rows_dev, depth), BF16),
            jax.ShapeDtypeStruct((rows_dev, depth), BF16),
            jax.ShapeDtypeStruct((blk, width), BF16),
            jax.ShapeDtypeStruct((blk, width), BF16),
        ),
        in_specs=[vmem] * 5,
        out_specs=(vmem,) * 4,
        scratch_shapes=[
            pltpu.VMEM((3, rows, depth), BF16),
            pltpu.VMEM((2, depth, width), BF16),
            pltpu.VMEM((3, rows, width), F32),
            pltpu.VMEM((3, rows, width), BF16),
            pltpu.VMEM((2, depth, width), BF16),
            pltpu.VMEM((4, half, blk, width), BF16),
            pltpu.VMEM((2, rows, depth), BF16),
            pltpu.VMEM((2, y_size, rows_dev, depth), BF16),
            pltpu.VMEM((2, sums, rows_dev, depth), BF16),
            dma((3, y_size)), dma((3, y_size)), dma((3, y_size)), dma((3, y_size)),
            *[dma((4, half, parts))] * 4,
            dma((2, y_size)), dma((2, y_size)), dma((2, sums)), dma((2, sums)),
        ],
        compiler_params=pltpu.CompilerParams(
            collective_id=0, has_side_effects=True, vmem_limit_bytes=67043328
        ),
        name="feed_forward_step",
    )(*args)


def body(n, m, later_rows, earlier_rows, cotangent, up_weight, down_weight, up_total, down_total):
    rows = later_rows.shape[0] * m
    factor = 1.0 / math.sqrt(rows * n)
    width = up_weight.shape[1]
    planar = columns_of(n) == 2 and n == 8 and m == 4 and width % 1024 == 0 and rows % 512 == 0
    planes = (later_rows, earlier_rows, cotangent, up_weight, down_weight)
    if planar:
        return tuple(hand_on(*plane_call(n, factor, *planes, up_total, down_total)))
    later_out, earlier_grad, up_term, down_term = ring_call(n, m, *planes)
    up_updated = up_total + up_term.astype(F32) * factor
    down_updated = down_total + down_term.astype(F32) * factor
    return later_out, earlier_grad, up_updated, down_updated


def solution(mesh):
    return jax.shard_map(
        functools.partial(body, mesh.shape["fs"], mesh.shape["tp"]),
        mesh=mesh,
        in_specs=(
            P(("fs", "tp"), None),
            P(("fs", "tp"), None),
            P(("fs", "tp"), None),
            P("fs", "tp"),
            P("fs", "tp"),
            P("fs", "tp"),
            P("fs", "tp"),
        ),
        out_specs=(P(("fs", "tp"), None), P(("fs", "tp"), None), P("fs", "tp"), P("fs", "tp")),
        check_vma=False,
    )
```

```python
import functools
import math

import jax
import jax.numpy as jnp
from jax import lax
from jax.experimental import pallas as pl
from jax.experimental.pallas import tpu as pltpu
from jax.sharding import PartitionSpec as P

MESH = pl.DeviceIdType.MESH
BF16 = jnp.bfloat16
F32 = jnp.float32


def columns_of(n):
    best = 1
    for x in range(1, n + 1):
        if n % x == 0 and 2 * x * x <= n and (n // x) % 2 == 0:
            best = x
    return best


def ring_to_fs(p, n, x_size):
    if x_size == 1:
        return p
    z_size, wide = n // x_size, x_size - 1
    body = z_size * wide
    z, r = p // wide, p % wide
    x = 1 + jnp.where(z % 2 == 0, r, wide - 1 - r)
    back = z_size - 1 - (p - body)
    return jnp.where(p < body, z * x_size + x, back * x_size)


def fs_to_ring(f, n, x_size):
    if x_size == 1:
        return f
    z_size, wide = n // x_size, x_size - 1
    z, x = f // x_size, f % x_size
    r = jnp.where(z % 2 == 0, x - 1, x_size - 1 - x)
    return jnp.where(x == 0, z_size * wide + z_size - 1 - z, z * wide + r)


def kernel(n, m, parts,
           later_ref, earlier_ref, cot_ref, up_ref, down_ref,
           later_out, earlier_out, up_out, down_out,
           tok, wts, acc, hid, grads, rbuf, part, dbuf, ybuf,
           ty_s, ty_r, td_s, td_r, w_s, w_r, g_s, g_r, od_s, od_r, oy_s, oy_r):
    rows_dev, depth = later_ref.shape
    blk, width = up_ref.shape
    rows = rows_dev * m
    half, y_size = n // 2, m // 2
    aligned = blk % 128 == 0
    wide_q = width // parts
    fs, tp = lax.axis_index("fs"), lax.axis_index("tp")
    x_size = columns_of(n)
    pos = fs_to_ring(fs, n, x_size)
    y, c = tp // 2, tp % 2

    def at_ring(p):
        return ring_to_fs((p + 2 * n) % n, n, x_size)

    right = {"fs": at_ring(pos + 1), "tp": tp}
    left = {"fs": at_ring(pos - 1), "tp": tp}
    mate = {"fs": fs, "tp": y * 2 + 1 - c}
    y_next = {"fs": fs, "tp": ((y + 1) % y_size) * 2 + c}
    y_prev = {"fs": fs, "tp": ((y + y_size - 1) % y_size) * 2 + c}

    barrier = pltpu.get_barrier_semaphore()
    for other in (right, left, mate, y_next, y_prev):
        pl.semaphore_signal(barrier, inc=1, device_id=other, device_id_type=MESH)
    pl.semaphore_wait(barrier, 5)

    def remote(src, dst, send, recv, to):
        return pltpu.make_async_remote_copy(
            src_ref=src, dst_ref=dst, send_sem=send, recv_sem=recv, device_id=to, device_id_type=MESH)

    def trows(a, t):
        return tok.at[a, pl.ds(pl.multiple_of(t * rows_dev, rows_dev), rows_dev), :]

    own_w, own_t = (up_ref, down_ref), (earlier_ref, cot_ref, later_ref)

    arr_of, sign_of = (0, 1, 1, 0), (1, -1, 1, -1)

    def cut(q):
        return pl.ds(q * wide_q, wide_q)

    def w_copy(k, s, q, first=False):
        f = at_ring(pos - sign_of[k] * s)
        there = wts.at[arr_of[k], pl.ds(pl.multiple_of(f * blk, blk), blk), cut(q)]
        src = own_w[arr_of[k]].at[:, cut(q)] if first else there
        return remote(src, there, w_s.at[k, s, q], w_r.at[k, s, q], right if sign_of[k] > 0 else left)

    def ty_copy(a, s, first=False):
        t = ((y + y_size - s) % y_size) * 2 + c
        return remote(own_t[a] if first else trows(a, t), trows(a, t), ty_s.at[a, s], ty_r.at[a, s], y_next)

    def td_copy(a, s, first=False):
        t = ((y + y_size - s) % y_size) * 2 + c
        return remote(own_t[a] if first else trows(a, t), trows(a, t), td_s.at[a, s], td_r.at[a, s], mate)

    every = tuple((k, q) for pair in ((0, 1), (2, 3)) for q in range(parts) for k in pair)
    longs = tuple((k, q) for k, q in every if k < 2)
    for k, q in every:
        w_copy(k, 0, q, True).start()
    for a in range(3):
        if y_size > 1:
            ty_copy(a, 0, True).start()
    for a in range(3):
        td_copy(a, 0, True).start()

    def put(dst, dst_row, src, count):
        step = math.gcd(count, 64)

        @pl.loop(0, count // step)
        def _(i):
            o = pl.multiple_of(i * step, step)
            dst[pl.ds(pl.multiple_of(dst_row + o, step), step), :] = src[pl.ds(o, step), :]

    for a in range(2):
        put(wts.at[a], fs * blk, own_w[a], blk)
    for a in range(3):
        put(tok.at[a], tp * rows_dev, own_t[a], rows_dev)

    tile = math.gcd(wide_q, 256)

    def multiply(a, w, rows_w, clear, q=None):
        first, count = (0, width) if q is None else (q * wide_q, wide_q)

        @pl.loop(0, count // tile)
        def _(j):
            o = pl.ds(pl.multiple_of(first + j * tile, tile), tile)
            got = jnp.dot(tok[a, :, rows_w], wts[w, rows_w, o], preferred_element_type=F32)
            if clear:
                acc[a, :, o] = got
            else:
                acc[a, :, o] += got

    def use(w, f, clear=False, q=None):
        if not aligned:
            return
        o = pl.ds(pl.multiple_of(f * blk, blk), blk)
        for a in ((0, 2) if w == 0 else (1,)):
            multiply(a, w, o, clear, q)

    def forward(s, present, go):
        for k, q in present:
            w_copy(k, s - 1, q).wait_recv()
            if (k, q) in go:
                w_copy(k, s, q).start()

    def use_step(s):
        for k in range(4):
            use(arr_of[k], at_ring(pos - sign_of[k] * s))

    forward(1, every, every if half > 2 else longs)
    for s in range(1, y_size):
        for a in range(3):
            ty_copy(a, s - 1).wait_recv()
            if s < y_size - 1:
                ty_copy(a, s).start()
            td_copy(a, s).start()
    for s in range(y_size):
        for a in range(3):
            td_copy(a, s).wait_recv()
    for w in range(2):
        use(w, fs, True)
    if half > 3:
        @pl.loop(2, half - 1)
        def _(s):
            forward(s, every, every)
            use_step(s - 1)
    if half > 2:
        forward(half - 1, every, longs)
        use_step(half - 2)
    use_step(half - 1)

    step_r = math.gcd(rows, 32)

    def activate(q):
        @pl.loop(0, rows // step_r)
        def _(i):
            o = pl.ds(pl.multiple_of(i * step_r, step_r), step_r)
            relu = jnp.maximum(acc[0, o, cut(q)], 0.0)
            hid[0, o, cut(q)] = (2.0 * relu * acc[1, o, cut(q)]).astype(BF16)
            hid[1, o, cut(q)] = (relu * relu).astype(BF16)

    def term(a, row, size, q=None):
        first, count = (0, width) if q is None else (q * wide_q, wide_q)

        @pl.loop(0, count // tile)
        def _(j):
            o = pl.ds(pl.multiple_of(first + j * tile, tile), tile)
            grads[a, pl.ds(row, size), o] = lax.dot_general(
                tok[a, :, pl.ds(row, size)], hid[a, :, o], (((0,), (0,)), ((), ())),
                preferred_element_type=F32).astype(BF16)

    def block_term(a, p, q=None):
        term(a, pl.multiple_of(at_ring(p) * blk, blk), blk, q)

    def g_copy(k, s, q):
        d = half - (k >= 2) - s
        f = at_ring(pos + sign_of[k] * d)
        src = grads.at[arr_of[k], pl.ds(pl.multiple_of(f * blk, blk), blk), cut(q)]
        return remote(src, rbuf.at[k, s, :, cut(q)], g_s.at[k, s, q], g_r.at[k, s, q],
                      right if sign_of[k] > 0 else left)

    def add_rows(dst, dst_row, src, count, columns=slice(None)):
        step = math.gcd(count, 32)

        @pl.loop(0, count // step)
        def _(i):
            o = pl.multiple_of(i * step, step)
            at = pl.ds(pl.multiple_of(dst_row + o, step), step)
            total = dst[at, columns].astype(F32) + src[pl.ds(o, step), columns].astype(F32)
            dst[at, columns] = total.astype(BF16)

    def g_step(s, which):
        for k, q in which:
            g_copy(k, s - 1, q).wait_recv()
            f = at_ring(pos + sign_of[k] * (half - (k >= 2) - s))
            add_rows(grads.at[arr_of[k]], f * blk, rbuf.at[k, s - 1], blk, cut(q))
            g_copy(k, s, q).start()

    wide = math.gcd(depth, 256)
    for q in range(parts):
        for k in (0, 1):
            w_copy(k, half - 1, q).wait_recv()
            use(arr_of[k], at_ring(pos - sign_of[k] * half), q=q)
        if not aligned:
            full = pl.ds(0, depth)
            for a, w in ((0, 0), (1, 1), (2, 0)):
                multiply(a, w, full, True, q)
        activate(q)
        if not aligned:
            for a in range(2):
                @pl.loop(0, depth // wide)
                def _(i):
                    term(a, pl.multiple_of(i * wide, wide), wide, q)
        for k in (0, 1):
            if aligned:
                block_term(arr_of[k], pos + sign_of[k] * half, q)
            g_copy(k, 0, q).start()
    for k in (2, 3):
        if aligned:
            block_term(arr_of[k], pos + sign_of[k] * (half - 1))
        for q in range(parts):
            g_copy(k, 0, q).start()
    if aligned:
        if half > 1:
            @pl.loop(0, half - 1)
            def _(i):
                d = half - 1 - i
                block_term(0, pos + d)
                block_term(1, pos - d)
        if half > 2:
            @pl.loop(0, half - 2)
            def _(i):
                d = half - 2 - i
                block_term(1, pos + d)
                block_term(0, pos - d)
        for a in range(2):
            block_term(a, pos)

    @pl.loop(0, rows // step_r)
    def _(i):
        o = pl.ds(pl.multiple_of(i * step_r, step_r), step_r)
        relu = jnp.maximum(acc[2, o, :], 0.0)
        hid[2, o, :] = (relu * relu).astype(BF16)

    wide_d = math.gcd(depth, 256)

    def partial(a, h, w):
        @pl.loop(0, depth // wide_d)
        def _(j):
            o = pl.ds(pl.multiple_of(j * wide_d, wide_d), wide_d)
            part[a, :, o] = lax.dot_general(
                hid[h], wts[w, o, :], (((1,), (1,)), ((), ())), preferred_element_type=F32).astype(BF16)

    def prow(yy, cc):
        return pl.multiple_of((yy * 2 + cc) * rows_dev, rows_dev)

    def od_copy(a, yy):
        return remote(part.at[a, pl.ds(prow(yy, 1 - c), rows_dev), :], dbuf.at[a, yy],
                      od_s.at[a, yy], od_r.at[a, yy], mate)

    def oy_copy(a, s):
        t = (y + y_size - 1 - s) % y_size
        return remote(part.at[a, pl.ds(prow(t, c), rows_dev), :], ybuf.at[a, s],
                      oy_s.at[a, s], oy_r.at[a, s], y_next)

    def send_partial(a, h, w):
        partial(a, h, w)
        for yy in range(y_size):
            od_copy(a, yy).start()

    send_partial(0, 0, 0)
    g_step(1, every if half > 2 else longs)
    send_partial(1, 2, 1)
    for a in range(2):
        for yy in range(y_size):
            od_copy(a, yy).wait_recv()
            add_rows(part.at[a], prow(yy, c), dbuf.at[a, yy], rows_dev)
        if y_size > 1:
            oy_copy(a, 0).start()
    if half - 1 > 2:
        @pl.loop(2, half - 1)
        def _(s):
            g_step(s, every)
    for s in range(1, y_size):
        for a in range(2):
            oy_copy(a, s - 1).wait_recv()
            t = (y + y_size - 1 - s) % y_size
            add_rows(part.at[a], prow(t, c), ybuf.at[a, s - 1], rows_dev)
            if s < y_size - 1:
                oy_copy(a, s).start()
    put_own = ((earlier_out, 0), (later_out, 1))
    for out, a in put_own:
        out[...] = part[a, pl.ds(prow(y, c), rows_dev), :]
    if half - 1 >= 2:
        g_step(half - 1, longs)

    ends = [(k, half - 1 - (k >= 2)) for k in range(4)]
    for k, q in tuple((k, q) for k, q in every if k >= 2) + longs:
        g_copy(k, ends[k][1], q).wait_recv()
    step_b = math.gcd(blk, 32)
    for a, out in ((0, up_out), (1, down_out)):
        @pl.loop(0, blk // step_b)
        def _(i):
            lo = pl.multiple_of(i * step_b, step_b)
            o = pl.ds(lo, step_b)
            got = grads[a, pl.ds(pl.multiple_of(fs * blk + lo, step_b), step_b), :].astype(F32)
            for k, s in ends:
                if arr_of[k] == a:
                    got += rbuf[k, s, o, :].astype(F32)
            out[o, :] = got.astype(BF16)

    for k, q in every:
        for s in range(half - (k >= 2)):
            w_copy(k, s, q).wait_send()
            g_copy(k, s, q).wait_send()
    for a in range(3):
        for s in range(y_size):
            if s < y_size - 1:
                ty_copy(a, s).wait_send()
            td_copy(a, s).wait_send()
    for a in range(2):
        for yy in range(y_size):
            od_copy(a, yy).wait_send()
        for s in range(y_size - 1):
            oy_copy(a, s).wait_send()


def plane_kernel(n, chunks, factor,
                 later_ref, earlier_ref, cot_ref, up_ref, down_ref, up_total, down_total,
                 later_out, earlier_out, up_out, down_out,
                 tok, wts, act, hid, grads, gbuf, fin, xbuf, part, dbuf, qa, qb, stage, sums,
                 l_s, o_s, t_s, t_r, wx_s, wz_s, w_r, g_s, g_r, f_s, f_r, d_s, d_r, q_s, q_r, q_l):
    rows_dev, depth = later_ref.shape
    blk, width = up_ref.shape
    z_size, zrows = n // 2, 2 * blk
    wide, cw = width // 2, width // 2 // chunks
    chip_rows = 2 * rows_dev
    fs, tp = lax.axis_index("fs"), lax.axis_index("tp")
    z, x, y, c = fs // 2, fs % 2, tp // 2, tp % 2
    last = z_size - 1
    side = 2 * z // z_size
    span = 2 * blk

    right = {"fs": ((z + 1) % z_size) * 2 + x, "tp": tp}
    left = {"fs": ((z + last) % z_size) * 2 + x, "tp": tp}
    x_next = {"fs": z * 2 + 1 - x, "tp": tp}
    y_next = {"fs": fs, "tp": (1 - y) * 2 + c}
    mate = {"fs": fs, "tp": y * 2 + 1 - c}

    def block_at(xx, yy, cc):
        return ((xx * 2 + yy) * 2 + cc) * rows_dev

    def rows_at(start, count):
        return pl.ds(pl.multiple_of(start, math.gcd(count, 128)), count)

    def columns_at(xx, h):
        return pl.ds(pl.multiple_of(xx * wide + h * cw, cw), cw)

    own_w, own_t = (up_ref, down_ref), (earlier_ref, cot_ref, later_ref)

    def load_w(m, h):
        return pltpu.make_async_copy(
            own_w[m].at[:, columns_at(x, h)], wts.at[m, h, rows_at(fs * blk, blk), :], l_s.at[m * chunks + h])

    def load_t(a):
        return pltpu.make_async_copy(
            own_t[a], tok.at[a, rows_at(block_at(x, y, c), rows_dev), :], l_s.at[2 * chunks + a])

    for m in range(2):
        load_w(m, 0).start()
    load_t(0).start()
    load_t(1).start()
    for m in range(2):
        load_w(m, 1).start()
    load_t(2).start()
    totals = tuple(
        pltpu.make_async_copy(total, sums.at[m], l_s.at[2 * chunks + 3 + m])
        for m, total in enumerate((up_total, down_total)))
    for m in range(2):
        totals[m].start()

    barrier = pltpu.get_barrier_semaphore()
    for other in (right, left, x_next, y_next, mate):
        pl.semaphore_signal(barrier, inc=1, device_id=other, device_id_type=MESH)
    pl.semaphore_wait(barrier, 5)

    def remote(src, dst, send, recv, to):
        return pltpu.make_async_remote_copy(
            src_ref=src, dst_ref=dst, send_sem=send, recv_sem=recv, device_id=to, device_id_type=MESH)

    def piece(m, h, f):
        return wts.at[m, h, rows_at(f * blk, blk), :]

    def wx_copy(m, h):
        return remote(own_w[m].at[:, columns_at(1 - x, h)], piece(m, h, fs), wx_s, w_r.at[m, h, fs], x_next)

    def wz_copy(m, h, f, way):
        return remote(piece(m, h, f), piece(m, h, f), wz_s.at[way, m, h], w_r.at[m, h, f], left if way else right)

    def w_got(m, h, f):
        wz_copy(m, h, f, 0).wait_recv()

    def spread(m, h, f):
        @pl.when(z < last)
        def _():
            wz_copy(m, h, f, 0).start()

        @pl.when(z > 0)
        def _():
            wz_copy(m, h, f, 1).start()

    def spread_at(m, h, f, ends):
        @pl.when((z == 0) | (z == last) if ends else (z > 0) & (z < last))
        def _():
            spread(m, h, f)

    def from_x(h, ms=(0, 1)):
        for m in ms:
            w_got(m, h, z * 2 + 1 - x)
            spread(m, h, z * 2 + 1 - x)

    def from_x_at(h, ms, ends):
        @pl.when((z == 0) | (z == last) if ends else (z > 0) & (z < last))
        def _():
            from_x(h, ms)

    def relay(h, d, columns=(0, 1), ms=(0, 1)):
        for m in ms:
            for p in columns:
                p = (x + p) % 2

                @pl.when((z >= d) & (z < last))
                def _():
                    w_got(m, h, (z - d) * 2 + p)
                    wz_copy(m, h, (z - d) * 2 + p, 0).start()

                @pl.when((z + d < z_size) & (z > 0))
                def _():
                    w_got(m, h, (z + d) * 2 + p)
                    wz_copy(m, h, (z + d) * 2 + p, 1).start()

    def settle(h, m, lo, hi):
        @pl.when((z == 0) | (z == last))
        def _():
            @pl.loop(lo, hi)
            def _(d):
                for p in range(2):
                    w_got(m, h, jnp.where(z == 0, d, last - d) * 2 + p)

    def moves(cut_t):
        return (
            (x, y, 0, rows_dev, x_next),
            (x, y, 0, rows_dev, y_next),
            (1 - x, y, 0, cut_t, y_next),
            (x, 1 - y, cut_t, rows_dev - cut_t, x_next),
            (x, y, 0, rows_dev, mate),
            (1 - x, y, 0, rows_dev, mate),
            (x, 1 - y, 0, rows_dev, mate),
            (1 - x, 1 - y, 0, cut_t, mate),
            (1 - x, 1 - y, cut_t, rows_dev - cut_t, mate),
        )

    cuts = tuple(rows_dev * part // 8 // 16 * 16 for part in (7, 5, 4))

    def facing(i):
        return (1 - side) * (last - i) + side * i

    def t_ref(a, start, count, u):
        return tok.at[a, rows_at(start, count), slice(None) if u is None else rows_at(facing(u) * span, span)]

    def t_got(a, k, u):
        slot = u if k < 4 or a == 1 else k // 7 if a == 2 else 0
        return t_r.at[a, min(k, 4), slot]

    def t_copy(a, k, u):
        xx, yy, lo, count, to = moves(cuts[a])[k]
        there = t_ref(a, block_at(xx, yy, c) + lo, count, u)
        return remote(there, there, t_s.at[a], t_got(a, k, u), to)

    def t_own(a, u):
        for k in (0, 1, 4):
            t_copy(a, k, u).start()

    def t_pass(a, u):
        t_copy(a, 1, u).wait_recv()
        t_copy(a, 3, u).start()
        t_copy(a, 6, u).start()
        t_copy(a, 0, u).wait_recv()
        t_copy(a, 2, u).start()
        t_copy(a, 5, u).start()

    def t_diagonal(a, u):
        t_copy(a, 2, u).wait_recv()
        t_copy(a, 7, u).start()
        t_copy(a, 3, u).wait_recv()
        t_copy(a, 8, u).start()

    def t_mate(a, u=None):
        there = t_ref(a, 0, 4 * rows_dev, u)
        remote(there, there, t_s.at[a], t_got(a, 4, u), mate).wait_recv()

    def t_mate_blocks():
        there = t_ref(2, 0, 3 * rows_dev, None)
        remote(there, there, t_s.at[2], t_got(2, 4, None), mate).wait_recv()

    def t_mate_diagonal():
        there = t_ref(2, 0, rows_dev, None)
        remote(there, there, t_s.at[2], t_got(2, 7, None), mate).wait_recv()

    def earlier_hidden(h):
        @pl.loop(0, 4)
        def _(i):
            o = rows_at(i * chip_rows, chip_rows)
            relu = jnp.maximum(jnp.dot(tok[0, o, :], wts[0, h], preferred_element_type=F32), 0.0)
            act[o, :] = relu
            hid[1, h, o, :] = (relu * relu).astype(BF16)

    def earlier_pre_grad(h):
        @pl.loop(0, 4)
        def _(i):
            o = rows_at(i * chip_rows, chip_rows)
            got = jnp.dot(tok[1, o, :], wts[1, h], preferred_element_type=F32)
            hid[0, h, o, :] = (2.0 * act[o, :] * got).astype(BF16)

    def chip_at(i):
        return (((x + i % 2) % 2) * 2 + (y + i // 2) % 2) * chip_rows

    def later_hidden(h, lo, hi):
        @pl.loop(lo, hi)
        def _(i):
            o = rows_at(chip_at(i), chip_rows)
            relu = jnp.maximum(jnp.dot(tok[2, o, :], wts[0, h], preferred_element_type=F32), 0.0)
            hid[2, h, o, :] = (relu * relu).astype(BF16)

    def term(m, h, d):
        o = rows_at(d * zrows, zrows)
        grads[m, h, o, :] = lax.dot_general(
            tok[m, :, o], hid[m, h], (((0,), (0,)), ((), ())), preferred_element_type=F32).astype(BF16)

    def half_at(d, half):
        return d * zrows + (x + 1 - half) % 2 * blk

    def g_copy(m, h, d, way, half):
        src = grads.at[m, h, rows_at(half_at(d, half), blk), :]
        to = {"fs": ((z + z_size + 1 - 2 * way) % z_size) * 2 + x, "tp": tp}
        slot = d + 1 - way
        return remote(src, gbuf.at[m, h, slot, half], g_s.at[way, m, h], g_r.at[m, h, slot, half], to)

    def term_step(m, h, i):
        d = facing(i)
        term(m, h, d)

        @pl.when(((z == 0) | (z == last)) & (i < last))
        def _():
            for half in range(2):
                g_copy(m, h, d, side, half).start()

    def add_rows(dst, dst_row, src, count, columns=slice(None)):
        step = math.gcd(count, 32)

        @pl.loop(0, count // step)
        def _(i):
            o = pl.multiple_of(i * step, step)
            at = pl.ds(pl.multiple_of(dst_row + o, math.gcd(step, 16)), step)
            dst[at, columns] = (dst[at, columns].astype(F32) + src[pl.ds(o, step), columns].astype(F32)).astype(BF16)

    def reduce_step(h, k, m, near):
        way = side if near else 1 - side
        d = (1 - way) * (last - k) + way * k
        beyond = (1 - 2 * way) * (d - z)
        behind = (1 - way) * z + way * (last - z)

        @pl.when((beyond > 0) & (behind > 0))
        def _():
            for half in range(2):
                g_copy(m, h, d, way, half).wait_recv()
                add_rows(grads.at[m, h], half_at(d, half), gbuf.at[m, h, d + 1 - way, half], blk)
                g_copy(m, h, d, way, half).start()

    outs = (up_out, down_out)

    def f_copy(m, h):
        return remote(fin.at[m, h], xbuf.at[m, h], f_s, f_r.at[m, h], x_next)

    def total(m, h, half, sources):
        step = math.gcd(blk, 32)

        @pl.loop(0, blk // step)
        def _(i):
            o = pl.multiple_of(i * step, step)
            at = pl.ds(o, step)
            got = grads[m, h, pl.ds(pl.multiple_of(half_at(z, half) + o, step), step), :].astype(F32)
            for src in sources:
                got += gbuf[m, h, z + 1 - src, half, at, :].astype(F32)
            if half:
                sums[m, at, columns_at(x, h)] += got * factor
            else:
                fin[m, h, at, :] = got.astype(BF16)

    def store_sum(m, h, xx):
        there = columns_at(xx, h)
        return pltpu.make_async_copy(sums.at[m, :, there], outs[m].at[:, there], o_s.at[m])

    def finish(h, m):
        for half in range(2):
            @pl.when(z > 0)
            def _():
                g_copy(m, h, z, 0, half).wait_recv()

            @pl.when(z < last)
            def _():
                g_copy(m, h, z, 1, half).wait_recv()

            for case, sources in ((z == 0, (1,)), (z == last, (0,)), ((z > 0) & (z < last), (0, 1))):
                @pl.when(case)
                def _():
                    total(m, h, half, sources)

            (store_sum(m, h, x) if half else f_copy(m, h)).start()

    def finish_at(h, m, ends):
        @pl.when((z == 0) | (z == last) if ends else (z > 0) & (z < last))
        def _():
            finish(h, m)

    def finish_x(h, m):
        f_copy(m, h).wait_recv()
        step = math.gcd(blk, 32)

        @pl.loop(0, blk // step)
        def _(i):
            at = pl.ds(pl.multiple_of(i * step, step), step)
            sums[m, at, columns_at(1 - x, h)] += xbuf[m, h, at, :].astype(F32) * factor

        store_sum(m, h, 1 - x).start()

    tile = math.gcd(span, 256)

    def span_at(i):
        return rows_at(((1 - side) * i + side * (last - i)) * span, span)

    def partial(a, k, w, i):
        first = ((1 - side) * i + side * (last - i)) * span

        @pl.loop(0, span // tile)
        def _(j):
            o = rows_at(first + j * tile, tile)
            got = None
            for h in range(chunks):
                one = lax.dot_general(hid[k, h], wts[w, h, o, :], (((1,), (1,)), ((), ())),
                                      preferred_element_type=F32)
                got = one if got is None else got + one
            part[a, :, o] = got.astype(BF16)

        for q in range(4):
            d_copy(a, q, i).start()

    def d_copy(a, q, i):
        return remote(part.at[a, rows_at(q * chip_rows + (1 - c) * rows_dev, rows_dev), span_at(i)],
                      dbuf.at[a, q, :, span_at(i)], d_s.at[a], d_r.at[a, i], mate)

    cuts_q = tuple(rows_dev * share // 8 // 16 * 16 for share in (2, 3))
    hops = (
        (1 - x, y, 0, qa, 0, x_next),
        (1 - x, 1 - y, 0, qa, 1, x_next),
        (x, 1 - y, 1, qb, 0, y_next),
        (1 - x, 1 - y, 1, qb, 1, y_next),
        (x, 1 - y, 0, qa, 2, y_next),
        (1 - x, y, 1, qb, 2, x_next),
    )

    def bounds(a, high):
        return (cuts_q[a], rows_dev - cuts_q[a]) if high else (0, cuts_q[a])

    def q_copy(a, k, i):
        xx, yy, high, buf, slot, to = hops[k]
        lo, count = bounds(a, high)
        return remote(part.at[a, rows_at(block_at(xx, yy, c) + lo, count), span_at(i)],
                      buf.at[a, slot, pl.ds(0, count), span_at(i)], q_s.at[a], q_r.at[a, k // 2, i] if k in (1, 3) else q_l.at[a], to)

    def q_first(a, i):
        there = dbuf.at[a, :, :, span_at(i)]
        remote(there, there, d_s.at[a], d_r.at[a, i], mate).wait_recv()
        for q in range(4):
            add_rows(part.at[a], q * chip_rows + c * rows_dev, dbuf.at[a, q], rows_dev, span_at(i))
        for k in (1, 3):
            q_copy(a, k, i).start()

    def q_rest(a, i):
        for k in (0, 2):
            q_copy(a, k, i).start()

    def q_second_y(a, i):
        q_copy(a, 1, i).wait_recv()
        add_rows(part.at[a], block_at(x, 1 - y, c), qa.at[a, 1], cuts_q[a], span_at(i))
        q_copy(a, 4, i).start()

    def q_second_x(a, i):
        q_copy(a, 3, i).wait_recv()
        add_rows(part.at[a], block_at(1 - x, y, c) + cuts_q[a], qb.at[a, 1], rows_dev - cuts_q[a], span_at(i))
        q_copy(a, 5, i).start()

    def over(lo, hi, *calls):
        @pl.loop(lo, hi)
        def _(i):
            for call in calls:
                call(i)

    def store_out(a):
        return pltpu.make_async_copy(stage.at[a], (earlier_out, later_out)[a], o_s.at[2 + a])

    def q_last(a):
        there = part.at[a, pl.ds(0, 2 * rows_dev), :]
        remote(there, there, q_s.at[a], q_l.at[a], x_next).wait_recv()
        for high, buf in enumerate((qa, qb)):
            lo, count = bounds(a, high)
            step = math.gcd(count, 16)

            @pl.loop(0, count // step)
            def _(i):
                o = pl.multiple_of(i * step, step)
                at = pl.ds(o, step)
                own = pl.ds(pl.multiple_of(block_at(x, y, c) + lo + o, step), step)
                stage[a, pl.ds(pl.multiple_of(lo + o, step), step), :] = (
                    part[a, own, :].astype(F32) + buf[a, 0, at, :].astype(F32) + buf[a, 2, at, :].astype(F32)
                ).astype(BF16)

        store_out(a).start()

    wx_copy(0, 0).start()
    for m in range(2):
        load_w(m, 0).wait()
        spread(m, 0, fs)
    load_t(0).wait()
    for u in range(z_size):
        t_own(0, u)
    wx_copy(1, 0).start()
    from_x(0, (0,))
    relay(0, 1, (0,), (0,))
    t_pass(0, 0)
    t_pass(0, 1)
    relay(0, 1, (0,), (1,))
    relay(0, 1, (1,), (0,))
    t_pass(0, 2)
    relay(0, 2, (0,), (0,))
    t_pass(0, 3)
    for m in range(2):
        wx_copy(m, 1).start()
    load_t(1).wait()
    t_own(1, 0)
    t_own(1, 1)
    t_diagonal(0, 0)
    t_diagonal(0, 1)
    relay(0, 2, (1,), (0,))
    from_x(0, (1,))
    relay(0, 2, (0,), (1,))
    for m in range(2):
        load_w(m, 1).wait()
        spread_at(m, 1, fs, True)
    t_diagonal(0, 2)
    t_diagonal(0, 3)
    relay(0, 1, (1,), (1,))
    settle(0, 0, 1, z_size)
    t_mate(0)
    from_x_at(1, (0, 1), True)
    earlier_hidden(0)
    t_pass(1, 0)
    t_own(1, 2)
    relay(0, 2, (1,), (1,))
    spread_at(0, 1, fs, False)
    from_x_at(1, (0,), False)
    t_pass(1, 1)
    t_own(1, 3)
    t_diagonal(1, 0)
    t_mate(1, 0)
    term_step(1, 0, 0)
    relay(1, 1, (0,), (0,))
    t_pass(1, 2)
    t_diagonal(1, 1)
    t_mate(1, 1)
    term_step(1, 0, 1)
    relay(1, 1, (1,), (0,))
    spread_at(1, 1, fs, False)
    from_x_at(1, (1,), False)
    t_pass(1, 3)
    load_t(2).wait()
    for u in range(z_size):
        t_own(2, u)
    t_diagonal(1, 2)
    t_mate(1, 2)
    term_step(1, 0, 2)
    reduce_step(0, 0, 1, True)
    t_diagonal(1, 3)
    t_mate(1, 3)
    settle(0, 1, 1, z_size)
    earlier_pre_grad(0)
    t_pass(2, 0)
    relay(1, 2, (0, 1), (0,))
    over(0, z_size, lambda i: term_step(0, 0, i))
    t_pass(2, 1)
    relay(1, 1, (0, 1), (1,))
    reduce_step(0, 1, 1, True)
    term_step(1, 0, last)
    t_pass(2, 2)
    t_diagonal(2, 0)
    t_pass(2, 3)
    t_diagonal(2, 1)
    t_mate_blocks()
    later_hidden(0, 0, 3)
    settle(1, 0, 1, z_size)
    later_hidden(1, 0, 3)
    relay(1, 2, (0, 1), (1,))
    reduce_step(0, 0, 1, False)
    t_diagonal(2, 2)
    t_diagonal(2, 3)
    t_mate_diagonal()
    for h in range(2):
        later_hidden(h, 3, 4)
    reduce_step(0, 0, 0, True)
    settle(1, 1, 1, last)
    partial(1, 2, 1, 0)
    partial(1, 2, 1, 1)
    q_first(1, 0)
    q_rest(1, 0)
    earlier_hidden(1)
    q_first(1, 1)
    q_rest(1, 1)
    term_step(1, 1, 0)
    over(2, last, lambda i: partial(1, 2, 1, i))
    term_step(1, 1, 1)
    q_first(1, 2)
    over(2, z_size, lambda i: term_step(1, 1, i))
    q_second_x(1, 0)
    for m in range(2):
        totals[m].wait()
    finish_at(0, 1, False)
    reduce_step(0, 1, 0, True)
    settle(1, 1, last, z_size)
    partial(1, 2, 1, last)
    q_second_x(1, 1)
    reduce_step(0, 0, 0, False)
    earlier_pre_grad(1)
    q_first(1, last)
    q_rest(1, 2)
    over(0, z_size, lambda i: term_step(0, 1, i))
    q_second_x(1, 2)
    finish_at(0, 1, True)
    reduce_step(1, 0, 1, True)
    partial(0, 0, 0, 0)
    over(1, z_size, lambda i: partial(0, 0, 0, i), lambda i: q_first(0, i - 1))
    reduce_step(1, 1, 1, True)
    q_second_x(1, last)
    q_first(0, last)
    q_rest(1, last)
    over(0, z_size, lambda i: q_second_y(1, i))
    over(0, z_size, lambda i: q_rest(0, i))
    finish(0, 0)
    reduce_step(1, 0, 1, False)
    over(0, last, lambda i: q_second_x(0, i))
    finish(1, 1)
    reduce_step(1, 0, 0, True)
    q_second_x(0, last)
    over(0, z_size, lambda i: q_second_y(0, i))
    reduce_step(1, 1, 0, True)
    reduce_step(1, 0, 0, False)
    finish_x(0, 1)
    q_last(1)
    finish(1, 0)
    finish_x(0, 0)
    finish_x(1, 1)
    q_last(0)
    finish_x(1, 0)

    def sent(ref, semaphore):
        remote(ref, ref, semaphore, f_r.at[0, 0], mate).wait_send()

    four = wts.at[0, 0, pl.ds(0, 2 * chunks * blk), :]
    sent(four, wx_s)
    sent(four, f_s)
    for m in range(2):
        pltpu.make_async_copy(outs[m], outs[m], o_s.at[m]).wait()
        for h in range(chunks):
            for way in range(2):
                for hops_left in range(1, z_size):
                    @pl.when((last - z if way == 0 else z) == hops_left)
                    def _():
                        sent(wts.at[m, h, pl.ds(0, (z_size - hops_left) * zrows), :], wz_s.at[way, m, h])
                        sent(grads.at[m, h, pl.ds(0, hops_left * zrows), :], g_s.at[way, m, h])
    for a in range(3):
        sent(tok.at[a, pl.ds(0, 7 * rows_dev), :], t_s.at[a])
    for a in range(2):
        store_out(a).wait()
        sent(part.at[a, pl.ds(0, 4 * rows_dev), :], d_s.at[a])
        sent(part.at[a, pl.ds(0, 3 * rows_dev), :], q_s.at[a])


def plane_call(n, factor, *args):
    rows_dev, depth = args[0].shape
    blk, width = args[3].shape
    z_size, chunks, rows = n // 2, 2, rows_dev * 8
    cw = width // 2 // chunks
    low, high = rows_dev * 3 // 8 // 16 * 16, rows_dev - rows_dev * 2 // 8 // 16 * 16
    dma = pltpu.SemaphoreType.DMA
    hbm = pl.BlockSpec(memory_space=pltpu.HBM)
    return pl.pallas_call(
        functools.partial(plane_kernel, n, chunks, factor),
        out_shape=(
            jax.ShapeDtypeStruct((rows_dev, depth), BF16),
            jax.ShapeDtypeStruct((rows_dev, depth), BF16),
            jax.ShapeDtypeStruct((blk, width), F32),
            jax.ShapeDtypeStruct((blk, width), F32),
        ),
        in_specs=[hbm] * 7,
        out_specs=(hbm,) * 4,
        scratch_shapes=[
            pltpu.VMEM((3, rows, depth), BF16),
            pltpu.VMEM((2, chunks, depth, cw), BF16),
            pltpu.VMEM((rows, cw), F32),
            pltpu.VMEM((3, chunks, rows, cw), BF16),
            pltpu.VMEM((2, chunks, depth, cw), BF16),
            pltpu.VMEM((2, chunks, z_size + 1, 2, blk, cw), BF16),
            pltpu.VMEM((2, chunks, blk, cw), BF16),
            pltpu.VMEM((2, chunks, blk, cw), BF16),
            pltpu.VMEM((2, rows, depth), BF16),
            pltpu.VMEM((2, 4, rows_dev, depth), BF16),
            pltpu.VMEM((2, 3, low, depth), BF16),
            pltpu.VMEM((2, 3, high, depth), BF16),
            pltpu.VMEM((2, rows_dev, depth), BF16),
            pltpu.VMEM((2, blk, width), F32),
            dma((2 * chunks + 5,)), dma((4,)), dma((3,)), dma((3, 5, z_size)), dma, dma((2, 2, chunks)), dma((2, chunks, n)),
            dma((2, 2, chunks)), dma((2, chunks, z_size + 1, 2)), dma, dma((2, chunks)),
            dma((2,)), dma((2, z_size)), dma((2,)), dma((2, 2, z_size)), dma((2,)),
        ],
        compiler_params=pltpu.CompilerParams(
            collective_id=0, has_side_effects=True, vmem_limit_bytes=67043328
        ),
        name="feed_forward_planes",
    )(*args)


def hand_on_kernel(*refs):
    count = (len(refs) - 2) // 3
    ins, outs, held, in_s, out_s = refs[:count], refs[count:2 * count], refs[2 * count:-2], refs[-2], refs[-1]
    loads, stores = [], []
    for a, (src, kept, dst) in enumerate(zip(ins, held, outs)):
        half = src.shape[0] // 2
        for i in range(2):
            o = pl.ds(i * half, half)
            loads.append(pltpu.make_async_copy(src.at[o, :], kept.at[o, :], in_s.at[a, i]))
            stores.append(pltpu.make_async_copy(kept.at[o, :], dst.at[o, :], out_s.at[a]))
    for load in loads:
        load.start()
    for load, store in zip(loads, stores):
        load.wait()
        store.start()
    for a, (kept, dst) in enumerate(zip(held, outs)):
        pltpu.make_async_copy(kept, dst, out_s.at[a]).wait()


def hand_on(*arrays):
    count = len(arrays)
    hbm = pl.BlockSpec(memory_space=pltpu.HBM)
    return pl.pallas_call(
        hand_on_kernel,
        out_shape=tuple(jax.ShapeDtypeStruct(a.shape, a.dtype) for a in arrays),
        in_specs=[hbm] * count,
        out_specs=(hbm,) * count,
        scratch_shapes=[*(pltpu.VMEM(a.shape, a.dtype) for a in arrays),
                        pltpu.SemaphoreType.DMA((count, 2)), pltpu.SemaphoreType.DMA((count,))],
        compiler_params=pltpu.CompilerParams(vmem_limit_bytes=67043328),
        name="feed_forward_results",
    )(*arrays)


def ring_call(n, m, *args):
    rows_dev, depth = args[0].shape
    blk, width = args[3].shape
    rows, half, y_size = rows_dev * m, n // 2, m // 2
    dma = pltpu.SemaphoreType.DMA
    vmem = pl.BlockSpec(memory_space=pltpu.VMEM)
    sums = max(y_size - 1, 1)
    parts = 2 if width % 256 == 0 else 1
    return pl.pallas_call(
        functools.partial(kernel, n, m, parts),
        out_shape=(
            jax.ShapeDtypeStruct((rows_dev, depth), BF16),
            jax.ShapeDtypeStruct((rows_dev, depth), BF16),
            jax.ShapeDtypeStruct((blk, width), BF16),
            jax.ShapeDtypeStruct((blk, width), BF16),
        ),
        in_specs=[vmem] * 5,
        out_specs=(vmem,) * 4,
        scratch_shapes=[
            pltpu.VMEM((3, rows, depth), BF16),
            pltpu.VMEM((2, depth, width), BF16),
            pltpu.VMEM((3, rows, width), F32),
            pltpu.VMEM((3, rows, width), BF16),
            pltpu.VMEM((2, depth, width), BF16),
            pltpu.VMEM((4, half, blk, width), BF16),
            pltpu.VMEM((2, rows, depth), BF16),
            pltpu.VMEM((2, y_size, rows_dev, depth), BF16),
            pltpu.VMEM((2, sums, rows_dev, depth), BF16),
            dma((3, y_size)), dma((3, y_size)), dma((3, y_size)), dma((3, y_size)),
            *[dma((4, half, parts))] * 4,
            dma((2, y_size)), dma((2, y_size)), dma((2, sums)), dma((2, sums)),
        ],
        compiler_params=pltpu.CompilerParams(
            collective_id=0, has_side_effects=True, vmem_limit_bytes=67043328
        ),
        name="feed_forward_step",
    )(*args)


def body(n, m, later_rows, earlier_rows, cotangent, up_weight, down_weight, up_total, down_total):
    rows = later_rows.shape[0] * m
    factor = 1.0 / math.sqrt(rows * n)
    width = up_weight.shape[1]
    planar = columns_of(n) == 2 and n == 8 and m == 4 and width % 1024 == 0 and rows % 512 == 0
    planes = (later_rows, earlier_rows, cotangent, up_weight, down_weight)
    if planar:
        return tuple(hand_on(*plane_call(n, factor, *planes, up_total, down_total)))
    later_out, earlier_grad, up_term, down_term = ring_call(n, m, *planes)
    up_updated = up_total + up_term.astype(F32) * factor
    down_updated = down_total + down_term.astype(F32) * factor
    return later_out, earlier_grad, up_updated, down_updated


def solution(mesh):
    return jax.shard_map(
        functools.partial(body, mesh.shape["fs"], mesh.shape["tp"]),
        mesh=mesh,
        in_specs=(
            P(("fs", "tp"), None),
            P(("fs", "tp"), None),
            P(("fs", "tp"), None),
            P("fs", "tp"),
            P("fs", "tp"),
            P("fs", "tp"),
            P("fs", "tp"),
        ),
        out_specs=(P(("fs", "tp"), None), P(("fs", "tp"), None), P("fs", "tp"), P("fs", "tp")),
        check_vma=False,
    )
```
